32 devices in a mesh: grp: 2 (over x), ep: 16 (over z, y, core).
Axes of the slice: x: 2, y: 2, z: 4, core: 2. Of those that a mesh axis runs over, the one named last changes fastest.
Arguments:
- queries: bfloat16 [32, 8, 128], P(('grp', 'ep')), parts along dimension 0, may hold values from -400 to 400
- fresh_token_key: bfloat16 [32, 2, 128], P(('grp', 'ep')), parts along dimension 0, may hold values from -6 to 6
- value_new: bfloat16 [32, 2, 128], P(('grp', 'ep')), parts along dimension 0, may hold values from -6 to 6
- forget_logit: float32 [32, 8], P(('grp', 'ep')), parts along dimension 0, may hold values from -8 to 8
- cache_keys: bfloat16 [32, 2, 4096, 128], P(('grp', 'ep')), parts along dimension 0, may hold values from -12 to 12
- cache_values: bfloat16 [32, 2, 4096, 128], P(('grp', 'ep')), parts along dimension 0, may hold values from -6 to 6
- cache_cumlog: float32 [32, 8, 4096], P(('grp', 'ep')), parts along dimension 0, may hold values from -572 to 0
- lengths: int32 [32], P(('grp', 'ep')), parts along dimension 0, may hold values from 1024 to 4096
- residual: bfloat16 [32, 2048], P('grp', 'ep'), parts along dimension 0, may hold values from -6 to 6
- out_weight: bfloat16 [1024, 2048], P(None, 'ep'), may hold values from -0.1875 to 0.1875
- norm_gain: float32 [2048], replicated, may hold values from 0.1 to 1.9
- expert_gate: bfloat16 [16, 704, 2048], P('ep'), may hold values from -0.125 to 0.125
- expert_up: bfloat16 [16, 704, 2048], P('ep'), may hold values from -0.125 to 0.125
- expert_down: bfloat16 [16, 704, 2048], P('ep'), may hold values from -0.21875 to 0.21875
- shared_gate: bfloat16 [1408, 2048], P('ep'), may hold values from -0.125 to 0.125
- shared_up: bfloat16 [1408, 2048], P('ep'), may hold values from -0.125 to 0.125
- shared_down: bfloat16 [1408, 2048], P(None, 'ep'), may hold values from -0.15625 to 0.15625
- routes: int32 [32, 6], P('grp'), parts along dimension 0, may hold values from 0 to 15, all different within a row; in each aligned block of 16 rows (0 to 15, 16 to 31, ...) at most 12 rows name the same one
- route_scores: float32 [32, 6], P('grp'), parts along dimension 0, may hold values from 0.05 to 1
Outputs:
- updated: bfloat16 [32, 2048], P('grp', 'ep'), parts along dimension 0
The draws below stay inside these ranges and needn't reach their ends.
There are 2 independent parts, one for each index of `grp`. The reference program is written for one: setup_inputs(seed, part) draws one part's arguments, and reference() takes and returns one part's arrays. A program takes and returns all parts, laid end to end along the dimension named above; an argument that names none is the same for every part. Nothing has to cross between parts.
Inputs may be any that keep to these rules, and one draw needn't show every extreme that they name: `routes`: each row names 6 different experts; no expert is named by more than 12 rows of a part, a bound that some block reaches.
All inputs are finite; a program needn't handle non-finite values.
Results may differ from the reference program's by a relative error of at most 0.0068.
Values may be sent and summed in bfloat16 or wider, within the bound.
No kernel may reach another device: no remote copies, remote signals or barrier semaphores. Data moves between devices by JAX's collectives and lax.ppermute only.
A program may use at most 64 MiB of HBM per device.

```python
import math
import jax
import jax.numpy as jnp
import numpy as np
from jax import lax

D = 2048
QUERY_HEADS = 8
HD = 128
KVH = 2
FF = 704
SHARED_FF = 1408
TOP_K = 6
CACHE_POSITIONS = 4096
SEQUENCE_TOTAL = 16
EXPERTS = 16
CAP = 12
QW = 1024


def draw_queries(key, part):
    sampled = jnp.clip(jax.random.normal(jax.random.fold_in(key, 511), (SEQUENCE_TOTAL, QUERY_HEADS, HD), jnp.float32), -6.0, 6.0)
    return sampled.astype(jnp.bfloat16)


def draw_cache_keys(key, part):
    sampled = jnp.clip(jax.random.normal(jax.random.fold_in(key, 521), (SEQUENCE_TOTAL, KVH, CACHE_POSITIONS, HD), jnp.float32), -6.0, 6.0)
    return sampled.astype(jnp.bfloat16)


def draw_cache_cumlog(key, part):
    slow_share = 0.5
    slow_heads = jax.random.uniform(jax.random.fold_in(key, 531), (SEQUENCE_TOTAL, QUERY_HEADS), jnp.float32) < slow_share
    seq_factor = 2.0 ** jax.random.uniform(jax.random.fold_in(key, 532), (SEQUENCE_TOTAL, 1, 1), jnp.float32, -1.0, 1.0)
    decay_rate = jnp.where(slow_heads, 1.0 / CACHE_POSITIONS, 1.0 / 40.0)[:, :, None] * seq_factor
    jitter_strength = jax.random.uniform(jax.random.fold_in(key, 533), (SEQUENCE_TOTAL, QUERY_HEADS, CACHE_POSITIONS), jnp.float32, 0.2, 1.8)
    cluster_positions = jax.random.uniform(jax.random.fold_in(key, 534), (SEQUENCE_TOTAL, 1, CACHE_POSITIONS), jnp.float32) < 4.0 / CACHE_POSITIONS
    cluster_length = jnp.log(jax.random.uniform(jax.random.fold_in(key, 535), (SEQUENCE_TOTAL, QUERY_HEADS, CACHE_POSITIONS), jnp.float32, 0.5, 0.8))
    step_log_gate = -decay_rate * jitter_strength + jnp.where(cluster_positions, cluster_length, 0.0)
    return jnp.cumsum(step_log_gate, axis=2)


def set_ends(result, stream_key, smallest, high):
    extent = result.shape
    index_at = [jax.random.randint(jax.random.fold_in(stream_key, axis), (), 0, extent[axis]) for axis in range(len(extent))]
    result = result.at[tuple(index_at)].set(smallest)
    longest = extent.index(max(extent))
    index_at[longest] = (index_at[longest] + 1) % extent[longest]
    return result.at[tuple(index_at)].set(high)


def block_scale(rng, shape, split, smallest, high):
    def one(dim, parts):
        steps = jax.random.uniform(jax.random.fold_in(jax.random.fold_in(rng, 6), dim), (parts,), jnp.float32, smallest / len(split), high / len(split))
        return jnp.repeat(jnp.exp(steps), shape[dim] // parts).reshape((-1,) + (1,) * (len(shape) - dim - 1))

    loudness = one(*split[0])
    for cut in split[1:]:
        loudness = loudness * one(*cut)
    return loudness


def deal_out(key, own, number, rows, amount, top, bound, skew):
    sequence = jax.random.permutation(key, amount)
    crowded, usual = shares(amount, rows * top, bound, skew, True), shares(amount, rows * top, bound, skew, False)
    places = jnp.arange(amount)

    def named(tallies, turn):
        used = int((tallies > 0).sum())
        fixed = max(1, used // 4)
        passed = fixed + (places - fixed + turn * (used - fixed)) % max(1, amount - fixed)
        return jnp.zeros((amount,), jnp.int32).at[sequence[jnp.where(places < fixed, places, passed)]].set(jnp.asarray(tallies, jnp.int32))

    tallies = jnp.where(number % 4 == 0, named(crowded, number // 4), named(usual, number - number // 4 - 1))
    mixed = jax.random.permutation(jax.random.fold_in(own, 3), amount)
    source_of, receiver = mixed[0:amount // 2 * 2:2], mixed[1:amount // 2 * 2:2]
    slack = jnp.minimum(tallies[source_of] - 1, bound - tallies[receiver]) // 2
    slack = jnp.where((source_of == sequence[0]) | (receiver == sequence[0]) | (tallies[receiver] == 0), 0, jnp.maximum(slack, 0))
    passed = jax.random.randint(jax.random.fold_in(own, 4), (amount // 2,), 0, 1 << 20) % (slack + 1)
    tallies = tallies.at[source_of].add(-passed).at[receiver].add(passed)
    labels = jnp.searchsorted(jnp.cumsum(tallies), jnp.arange(rows * top), side="right").astype(jnp.int32)
    table = labels.reshape(top, rows).T
    table = table[jax.random.permutation(jax.random.fold_in(own, 1), rows)]
    turn = jax.random.randint(jax.random.fold_in(own, 2), (rows, 1), 0, top)
    return jnp.take_along_axis(table, (jnp.arange(top)[None, :] + turn) % top, axis=1)


def shares(number_of, total, reach, skew, full):
    weights = [(1 << 20) // math.isqrt(grade ** skew) + 1 for grade in range(1, number_of + 1)]
    largest = reach if full else min(reach, max(-(-total // number_of), total * weights[0] // sum(weights)))
    least = 1 if total - largest >= number_of - 1 else 0
    counts, surplus = [largest] + [least] * (number_of - 1), total - largest - least * (number_of - 1)
    while surplus > 0:
        movable = [i for i in range(1, number_of) if counts[i] < largest] or [i for i in range(1, number_of) if counts[i] < reach]
        mass, remaining = sum([weights[i] for i in movable]), surplus
        for i in movable:
            more = min(reach - counts[i], max(1, remaining * weights[i] // mass), surplus)
            counts[i] = counts[i] + more
            surplus = surplus - more
    return np.array(counts)


def gaussian(rng, dims, width, most, split=(), held_as=jnp.bfloat16):
    array = jax.random.normal(rng, dims, jnp.float32) * width
    if len(split) > 0:
        array = block_scale(rng, dims, split, -0.22, 0.18) * array
    return jnp.clip(array, min=-most, max=most).astype(held_as)


def setup_inputs(seed: int = 0, part: int = 0) -> dict:
    splits = jax.random.split(jax.random.key(seed), 20)
    own_keys = jax.random.split(jax.random.fold_in(splits[19], part), 20)
    queries = draw_queries(jax.random.fold_in(jax.random.fold_in(splits[19], part), 71), part)
    fresh_token_key = gaussian(own_keys[1], (SEQUENCE_TOTAL, KVH, HD), 1.0, 6.0, ((0, 16),))
    value_new = gaussian(own_keys[2], (SEQUENCE_TOTAL, KVH, HD), 1.0, 6.0, ((0, 16),))
    forget_logit = gaussian(own_keys[3], (SEQUENCE_TOTAL, QUERY_HEADS), 2.0, 8.0, ((0, 16),), jnp.float32)
    cache_keys = draw_cache_keys(jax.random.fold_in(jax.random.fold_in(splits[19], part), 71), part)
    cache_values = gaussian(own_keys[5], (SEQUENCE_TOTAL, KVH, CACHE_POSITIONS, HD), 1.0, 6.0, ((0, 16),))
    cache_cumlog = draw_cache_cumlog(jax.random.fold_in(jax.random.fold_in(splits[19], part), 71), part)
    lengths = set_ends(jax.random.randint(own_keys[7], (SEQUENCE_TOTAL,), CACHE_POSITIONS // 4, CACHE_POSITIONS + 1), jax.random.fold_in(own_keys[7], 1), CACHE_POSITIONS // 4, CACHE_POSITIONS).astype(jnp.int32)
    residual = gaussian(own_keys[8], (SEQUENCE_TOTAL, D), 1.0, 6.0, ((1, 16),))
    out_weight = gaussian(splits[9], (QW, D), QW ** -0.5, 0.1875, ((1, 16),))
    norm_gain = jnp.clip(1.0 + 0.18 * jax.random.normal(splits[10], (D,), jnp.float32), 0.1, 1.9)
    expert_gate = gaussian(splits[11], (EXPERTS, FF, D), D ** -0.5, 0.125, ((0, 16),))
    expert_up = gaussian(splits[12], (EXPERTS, FF, D), D ** -0.5, 0.125, ((0, 16),))
    expert_down = gaussian(splits[13], (EXPERTS, FF, D), FF ** -0.5, 0.21875, ((0, 16),))
    shared_gate = gaussian(splits[14], (SHARED_FF, D), D ** -0.5, 0.125, ((0, 16),))
    shared_up = gaussian(splits[15], (SHARED_FF, D), D ** -0.5, 0.125, ((0, 16),))
    shared_down = gaussian(splits[16], (SHARED_FF, D), SHARED_FF ** -0.5, 0.15625, ((1, 16),))
    routes_keys = jax.random.split(jax.random.fold_in(own_keys[17], 1), SEQUENCE_TOTAL // SEQUENCE_TOTAL)
    routes_turns = jax.random.permutation(jax.random.fold_in(own_keys[17], 3), SEQUENCE_TOTAL // SEQUENCE_TOTAL)
    routes = jax.vmap(lambda own, number: deal_out(jax.random.fold_in(own_keys[17], 2), own, number, SEQUENCE_TOTAL, EXPERTS, TOP_K, CAP, 2))(routes_keys, routes_turns).reshape((SEQUENCE_TOTAL, TOP_K))
    route_scores = jnp.clip(jax.random.uniform(own_keys[18], (SEQUENCE_TOTAL, TOP_K), jnp.float32, 0.05, 1.0), 0.05, 1.0)
    return dict(queries=queries, fresh_token_key=fresh_token_key, value_new=value_new, forget_logit=forget_logit, cache_keys=cache_keys, cache_values=cache_values, cache_cumlog=cache_cumlog, lengths=lengths, residual=residual, out_weight=out_weight, norm_gain=norm_gain, expert_gate=expert_gate, expert_up=expert_up, expert_down=expert_down, shared_gate=shared_gate, shared_up=shared_up, shared_down=shared_down, routes=routes, route_scores=route_scores)


norm_eps = 1e-06
routed_scale = 2.5
contract_last = (((1,), (1,)), ((), ()))

def expert_hidden(row_block, gate_matrix, up_matrix):
    gate_part = lax.dot_general(row_block, gate_matrix, contract_last, preferred_element_type=jnp.float32)
    up_part = lax.dot_general(row_block, up_matrix, contract_last, preferred_element_type=jnp.float32)
    return (jax.nn.silu(gate_part) * up_part).astype(jnp.bfloat16)

def attend_one(packed):
    queries, fresh_token_key, value_new, forget_logit, cache_keys, cache_values, cache_cumlog, length = packed
    head_count, head_size = queries.shape
    key_heads, cache_span, _ = cache_keys.shape
    groups = head_count // key_heads
    inv_root = head_size ** (-0.5)
    grouped_heads = queries.astype(jnp.float32).reshape(key_heads, groups, head_size)
    scores = jnp.einsum('kgd,kpd->kgp', grouped_heads, cache_keys.astype(jnp.float32)).reshape(head_count, cache_span) * inv_root
    positions = jnp.arange(cache_span, dtype=jnp.int32)[None, :]
    latest = lax.optimization_barrier(jnp.sum(jnp.where(positions == length - 1, cache_cumlog, jnp.zeros_like(cache_cumlog)), axis=1))
    log_gate = jax.nn.log_sigmoid(forget_logit)
    scores = scores + (latest + log_gate)[:, None] - cache_cumlog
    visible = positions < length
    scores = jnp.where(visible, scores, -jnp.inf)
    own_score = jnp.einsum('kgd,kd->kg', grouped_heads, fresh_token_key.astype(jnp.float32)).reshape(head_count) * inv_root
    top_score = jnp.maximum(lax.optimization_barrier(jnp.max(scores, axis=1)), own_score)
    weights = jnp.where(visible, jnp.exp(scores - top_score[:, None]), jnp.zeros_like(scores))
    own_weight = jnp.exp(own_score - top_score)
    denominator = lax.optimization_barrier(jnp.sum(weights, axis=1)) + own_weight
    rounded = lax.optimization_barrier(weights.astype(jnp.bfloat16)).astype(jnp.float32)
    own_rounded = lax.optimization_barrier(own_weight.astype(jnp.bfloat16)).astype(jnp.float32)
    weighted = jnp.einsum('kgp,kpd->kgd', rounded.reshape(key_heads, groups, cache_span), cache_values.astype(jnp.float32)).reshape(head_count, head_size)
    own_value = jnp.repeat(value_new.astype(jnp.float32), groups, axis=0)
    numerator = weighted + own_rounded[:, None] * own_value
    return (numerator / denominator[:, None]).astype(jnp.bfloat16).reshape(head_count * head_size)

def reference(queries, fresh_token_key, value_new, forget_logit, cache_keys, cache_values, cache_cumlog, lengths, residual, out_weight, norm_gain, expert_gate, expert_up, expert_down, shared_gate, shared_up, shared_down, routes, route_scores):
    attended = lax.map(attend_one, (queries, fresh_token_key, value_new, forget_logit, cache_keys, cache_values, cache_cumlog, lengths))
    mixed = jnp.dot(attended, out_weight, preferred_element_type=jnp.float32)
    stream = (residual.astype(jnp.float32) + mixed).astype(jnp.bfloat16)
    rows_wide = stream.astype(jnp.float32)
    inv_rms = lax.rsqrt(lax.optimization_barrier(jnp.mean(rows_wide * rows_wide, axis=1, keepdims=True)) + norm_eps)
    normed = (rows_wide * inv_rms * norm_gain).astype(jnp.bfloat16)
    gate_weights = route_scores / lax.optimization_barrier(jnp.sum(route_scores, axis=1, keepdims=True)) * routed_scale
    slot_ids = jnp.arange(CAP, dtype=jnp.int32)[:, None]

    def one_expert(totals, packed):
        expert_id, gate_matrix, up_matrix, down_matrix = packed
        expert_hits = routes == expert_id
        is_member = lax.optimization_barrier(jnp.sum(expert_hits.astype(jnp.int32), axis=1)).astype(jnp.int32)
        token_share = lax.optimization_barrier(jnp.sum(jnp.where(expert_hits, gate_weights, jnp.zeros_like(gate_weights)), axis=1))
        slot_rank = (jnp.cumsum(is_member) - 1).astype(jnp.int32)
        selector = (is_member[None, :] == 1) & (slot_rank[None, :] == slot_ids)
        picked = jnp.dot(selector.astype(jnp.bfloat16), normed, preferred_element_type=jnp.float32).astype(jnp.bfloat16)
        hidden = expert_hidden(picked, gate_matrix, up_matrix)
        expert_out = jnp.dot(hidden, down_matrix, preferred_element_type=jnp.float32).astype(jnp.bfloat16)
        slot_share = jnp.dot(selector.astype(jnp.float32), token_share, precision=lax.Precision.HIGHEST)
        contribution = jnp.dot(selector.astype(jnp.float32).T, expert_out.astype(jnp.float32) * slot_share[:, None], precision=lax.Precision.HIGHEST)
        return (totals + contribution, None)
    routed, _ = lax.scan(one_expert, jnp.zeros(stream.shape, jnp.float32), (jnp.arange(EXPERTS, dtype=jnp.int32), expert_gate, expert_up, expert_down))
    shared_mid = expert_hidden(normed, shared_gate, shared_up)
    shared = jnp.dot(shared_mid, shared_down, preferred_element_type=jnp.float32)
    return (stream.astype(jnp.float32) + routed + shared).astype(jnp.bfloat16)
```

```python
import jax
import jax.numpy as jnp
from jax import lax
from jax.experimental import pallas as pl
from jax.experimental.pallas import tpu as pltpu
from jax.sharding import PartitionSpec as P

CAP = 12


norm_eps = 1e-06
routed_scale = 2.5
contract_last = (((1,), (1,)), ((), ()))


def expert_hidden(row_block, gate_matrix, up_matrix):
    gate_part = lax.dot_general(
        row_block, gate_matrix, contract_last, preferred_element_type=jnp.float32
    )
    up_part = lax.dot_general(
        row_block, up_matrix, contract_last, preferred_element_type=jnp.float32
    )
    return (jax.nn.silu(gate_part) * up_part).astype(jnp.bfloat16)


def attention(
    queries,
    fresh_token_key,
    value_new,
    forget_logit,
    cache_keys,
    cache_values,
    cache_cumlog,
    lengths,
):
    batch_rows, head_count, head_size = queries.shape
    key_heads = cache_keys.shape[1]
    cache_span = cache_keys.shape[2]
    groups = head_count // key_heads
    inv_root = head_size ** (-0.5)
    grouped_heads = queries.reshape(batch_rows, key_heads, groups, head_size)
    scores = (
        jnp.einsum(
            "bkgd,bkpd->bkgp", grouped_heads, cache_keys, preferred_element_type=jnp.float32
        ).reshape(batch_rows, head_count, cache_span)
        * inv_root
    )
    positions = lax.broadcasted_iota(jnp.int32, (1, 1, cache_span), 2)
    last_pos = (lengths - 1)[:, None, None]
    latest = jnp.sum(jnp.where(positions == last_pos, cache_cumlog, 0.0), axis=2)
    log_gate = jax.nn.log_sigmoid(forget_logit)
    scores = scores + (latest + log_gate)[:, :, None] - cache_cumlog
    visible = positions < lengths[:, None, None]
    scores = jnp.where(visible, scores, -jnp.inf)
    own_score = (
        jnp.einsum(
            "tiuh,tih->tiu", grouped_heads, fresh_token_key, preferred_element_type=jnp.float32
        ).reshape(batch_rows, head_count)
        * inv_root
    )
    top_score = jnp.maximum(jnp.max(scores, axis=2), own_score)
    weights = jnp.where(visible, jnp.exp(scores - top_score[:, :, None]), 0.0)
    own_weight = jnp.exp(own_score - top_score)
    denominator = jnp.sum(weights, axis=2) + own_weight
    weighted = jnp.einsum(
        "bkgp,bkpd->bkgd",
        weights.astype(jnp.bfloat16).reshape(batch_rows, key_heads, groups, cache_span),
        cache_values,
        preferred_element_type=jnp.float32,
    )
    own_rounded = lax.optimization_barrier(own_weight.astype(jnp.bfloat16)).astype(jnp.float32)
    own_value = jnp.repeat(value_new, groups, axis=1).astype(jnp.float32)
    numerator = (
        weighted.reshape(batch_rows, head_count, head_size) + own_rounded[:, :, None] * own_value
    )
    return (
        (numerator / denominator[:, :, None])
        .astype(jnp.bfloat16)
        .reshape(batch_rows, head_count * head_size)
    )


def plain_device(
    queries,
    fresh_token_key,
    value_new,
    forget_logit,
    cache_keys,
    cache_values,
    cache_cumlog,
    lengths,
    residual,
    out_weight,
    norm_gain,
    expert_gate,
    expert_up,
    expert_down,
    shared_gate,
    shared_up,
    shared_down,
    routes,
    route_scores,
):
    attended = attention(
        queries,
        fresh_token_key,
        value_new,
        forget_logit,
        cache_keys,
        cache_values,
        cache_cumlog,
        lengths,
    )
    mixed = jnp.dot(
        lax.all_gather(attended, "ep", axis=0, tiled=True),
        out_weight,
        preferred_element_type=jnp.float32,
    )
    stream = (residual.astype(jnp.float32) + mixed).astype(jnp.bfloat16)
    full_rows = lax.all_gather(stream, "ep", axis=1, tiled=True)
    rows_wide = full_rows.astype(jnp.float32)
    inv_rms = lax.rsqrt(jnp.mean(rows_wide * rows_wide, axis=1, keepdims=True) + norm_eps)
    normed = (rows_wide * inv_rms * norm_gain).astype(jnp.bfloat16)
    gate_weights = route_scores / jnp.sum(route_scores, axis=1, keepdims=True) * routed_scale
    shared_mid = expert_hidden(normed, shared_gate, shared_up)
    my_expert = lax.axis_index("ep")
    expert_hits = routes == my_expert
    is_member = jnp.sum(expert_hits.astype(jnp.int32), axis=1)
    slot_rank = jnp.cumsum(is_member) - 1
    slot_ids = lax.broadcasted_iota(jnp.int32, (CAP, 1), 0)
    selector = (is_member[None, :] == 1) & (slot_rank[None, :] == slot_ids)
    picked = jnp.dot(
        selector.astype(jnp.bfloat16), normed, preferred_element_type=jnp.float32
    ).astype(jnp.bfloat16)
    hidden = expert_hidden(picked, expert_gate[0], expert_up[0])
    expert_out = jnp.dot(hidden, expert_down[0], preferred_element_type=jnp.float32).astype(
        jnp.bfloat16
    )
    received = lax.all_to_all(expert_out[None], "ep", split_axis=2, concat_axis=0, tiled=True)
    expert_count = received.shape[0]
    expert_ids = lax.broadcasted_iota(jnp.int32, (1, 1, expert_count), 2)
    all_hits = routes[:, :, None] == expert_ids
    membership = jnp.sum(all_hits.astype(jnp.int32), axis=1)
    share_all = jnp.sum(jnp.where(all_hits, gate_weights[:, :, None], 0.0), axis=1)
    rank_all = jnp.cumsum(membership, axis=0) - 1
    slot_grid = lax.broadcasted_iota(jnp.int32, (1, 1, CAP), 2)
    slot_mask = (membership[:, :, None] == 1) & (rank_all[:, :, None] == slot_grid)
    combiner = jnp.where(slot_mask, share_all[:, :, None], 0.0).reshape(
        routes.shape[0], expert_count * CAP
    )
    flat_slots = received.reshape(expert_count * CAP, received.shape[2]).astype(jnp.float32)
    routed_part = jnp.dot(combiner, flat_slots, precision=lax.Precision.HIGHEST)
    shared_part = jnp.dot(
        lax.all_gather(shared_mid, "ep", axis=1, tiled=True),
        shared_down,
        preferred_element_type=jnp.float32,
    )
    return (stream.astype(jnp.float32) + routed_part + shared_part).astype(jnp.bfloat16)


VMEM = pltpu.VMEM
chunk_count = 4


def in_vmem():
    return pl.BlockSpec(memory_space=VMEM)


def params(mib):
    return pltpu.CompilerParams(vmem_limit_bytes=mib * 1024 * 1024)


def attention_kernel(
    lengths_ref,
    queries_ref,
    fresh_ref,
    value_new_ref,
    forget_ref,
    keys_hbm,
    values_hbm,
    cumlog_hbm,
    out_ref,
    keys,
    values,
    cumlog,
    sems,
):
    heads, size = queries_ref.shape
    key_heads, span, _ = keys.shape
    groups = heads // key_heads
    step = span // chunk_count
    inv_root = size ** (-0.5)
    cumlog_copy = pltpu.make_async_copy(cumlog_hbm.at[0], cumlog, sems.at[2 * chunk_count])
    cumlog_copy.start()

    def copies(source, target, first):
        return [
            pltpu.make_async_copy(
                source.at[0, :, pl.ds(c * step, step), :],
                target.at[:, pl.ds(c * step, step), :],
                sems.at[first + c],
            )
            for c in range(chunk_count)
        ]

    key_copies = copies(keys_hbm, keys, 0)
    value_copies = copies(values_hbm, values, chunk_count)
    for copy in key_copies + value_copies:
        copy.start()

    length = lengths_ref[0]
    queries = queries_ref[...]
    head_rows = lax.broadcasted_iota(jnp.int32, (heads, 1), 0)
    wide = jnp.concatenate(
        [jnp.where(head_rows // groups == k, queries, jnp.zeros_like(queries)) for k in range(key_heads)],
        axis=1,
    )

    def per_head(ref):
        rows = ref[...].astype(jnp.float32)
        total = jnp.zeros((heads, size), jnp.float32)
        for k in range(key_heads):
            total = jnp.where(head_rows // groups == k, rows[k : k + 1, :], total)
        return total

    own_score = (
        jnp.sum(queries.astype(jnp.float32) * per_head(fresh_ref), axis=1, keepdims=True) * inv_root
    )
    logit_row = jnp.broadcast_to(forget_ref[...], (heads, heads))
    diagonal = lax.broadcasted_iota(jnp.int32, (heads, heads), 1) == head_rows
    logit = jnp.sum(jnp.where(diagonal, logit_row, 0.0), axis=1, keepdims=True)
    log_gate = jnp.minimum(logit, 0.0) - jnp.log1p(jnp.exp(-jnp.abs(logit)))
    cumlog_copy.wait()
    positions = lax.broadcasted_iota(jnp.int32, (heads, span), 1)
    latest = jnp.sum(
        jnp.where(positions == length - 1, cumlog[...], 0.0), axis=1, keepdims=True
    )
    offset = latest + log_gate
    scores = []
    for c in range(chunk_count):
        key_copies[c].wait()
        block = jnp.concatenate(
            [keys[k, c * step : (c + 1) * step, :] for k in range(key_heads)], axis=1
        )
        raw = lax.dot_general(wide, block, contract_last, preferred_element_type=jnp.float32)
        raw = raw * inv_root + offset - cumlog[:, c * step : (c + 1) * step]
        visible = positions[:, c * step : (c + 1) * step] < length
        scores.append(jnp.where(visible, raw, -jnp.inf))
    top = own_score
    for part in scores:
        top = jnp.maximum(top, jnp.max(part, axis=1, keepdims=True))
    own_weight = jnp.exp(own_score - top)
    denominator = own_weight
    total = jnp.zeros((heads, key_heads * size), jnp.float32)
    for c in range(chunk_count):
        weights = jnp.exp(scores[c] - top)
        denominator = denominator + jnp.sum(weights, axis=1, keepdims=True)
        value_copies[c].wait()
        block = jnp.concatenate(
            [values[k, c * step : (c + 1) * step, :] for k in range(key_heads)], axis=1
        )
        total = total + jnp.dot(
            weights.astype(jnp.bfloat16), block, preferred_element_type=jnp.float32
        )
    mine = own_weight.astype(jnp.bfloat16).astype(jnp.float32) * per_head(value_new_ref)
    for k in range(key_heads):
        mine = mine + jnp.where(
            head_rows // groups == k, total[:, k * size : (k + 1) * size], 0.0
        )
    attended = (mine / denominator).astype(jnp.bfloat16)
    for peer in range(out_ref.shape[0]):
        out_ref[peer] = attended


def projection_kernel(rows_ref, weight_ref, residual_ref, out_ref):
    tokens, heads, size = rows_ref.shape
    stacked = rows_ref[...].reshape(tokens * heads, size)
    which = lax.broadcasted_iota(jnp.int32, (tokens * heads, 1), 0) % heads
    wide = jnp.concatenate(
        [jnp.where(which == h, stacked, jnp.zeros_like(stacked)) for h in range(heads)], axis=1
    )
    product = jnp.dot(wide, weight_ref[...], preferred_element_type=jnp.float32)
    mixed = jnp.sum(product.reshape(tokens, heads, product.shape[1]), axis=1)
    stream = (residual_ref[...].astype(jnp.float32) + mixed).astype(jnp.bfloat16)
    for peer in range(out_ref.shape[0]):
        out_ref[peer] = stream


def silu_product(gate, up):
    return gate / (1.0 + jnp.exp(-gate)) * up


def expert_kernel(
    expert_ref,
    blocks_ref,
    gain_ref,
    routes_ref,
    scores_ref,
    gate_ref,
    up_ref,
    down_ref,
    shared_gate_ref,
    shared_up_ref,
    out_ref,
):
    peers, tokens, width = blocks_ref.shape
    wide = [blocks_ref[p].astype(jnp.float32) for p in range(peers)]
    squares = wide[0] * wide[0]
    for block in wide[1:]:
        squares = squares + block * block
    mean = jnp.sum(squares, axis=1, keepdims=True) / (peers * width)
    inv_rms = lax.rsqrt(mean + norm_eps)
    normed = jnp.concatenate(
        [
            (wide[p] * inv_rms * gain_ref[p : p + 1, :]).astype(jnp.bfloat16)
            for p in range(peers)
        ],
        axis=1,
    )
    scores = scores_ref[...]
    shares = scores / jnp.sum(scores, axis=0, keepdims=True) * routed_scale
    share = jnp.sum(
        jnp.where(routes_ref[...] == expert_ref[0], shares, 0.0), axis=0, keepdims=True
    )

    def against(matrix):
        return lax.dot_general(matrix, normed, contract_last, preferred_element_type=jnp.float32)

    shared_hidden = silu_product(against(shared_gate_ref[...]), against(shared_up_ref[...])).astype(
        jnp.bfloat16
    )
    units = shared_hidden.shape[0]
    spread = (
        lax.broadcasted_iota(jnp.int32, (units, width), 0)
        == lax.broadcasted_iota(jnp.int32, (units, width), 1)
    ).astype(jnp.bfloat16)
    contract_first = (((0,), (0,)), ((), ()))
    shared_rows = lax.dot_general(
        shared_hidden, spread, contract_first, preferred_element_type=jnp.float32
    ).astype(jnp.bfloat16)
    hidden = (silu_product(against(gate_ref[...]), against(up_ref[...])) * share).astype(
        jnp.bfloat16
    )
    result = lax.dot_general(
        hidden, down_ref[...], contract_first, preferred_element_type=jnp.float32
    ).astype(jnp.bfloat16)
    for p in range(peers):
        out_ref[p, :tokens, :] = result[:, p * width : (p + 1) * width]
        out_ref[p, tokens:, :] = shared_rows


def combine_kernel(received_ref, stream_ref, down_ref, out_ref):
    peers, double, width = received_ref.shape
    tokens = double // 2
    units = down_ref.shape[0] // peers
    total = stream_ref[0].astype(jnp.float32)
    for p in range(peers):
        total = total + received_ref[p, :tokens, :].astype(jnp.float32)
    for p in range(peers):
        total = total + jnp.dot(
            received_ref[p, tokens:, :][:, :units],
            down_ref[p * units : (p + 1) * units, :],
            preferred_element_type=jnp.float32,
        )
    out_ref[...] = total.astype(jnp.bfloat16)


def exchange(blocks):
    return lax.all_to_all(blocks, "ep", split_axis=0, concat_axis=0, tiled=True)


def kernel_device(
    queries,
    fresh_token_key,
    value_new,
    forget_logit,
    cache_keys,
    cache_values,
    cache_cumlog,
    lengths,
    residual,
    out_weight,
    norm_gain,
    expert_gate,
    expert_up,
    expert_down,
    shared_gate,
    shared_up,
    shared_down,
    routes,
    route_scores,
):
    peers = lax.axis_size("ep")
    _, heads, size = queries.shape
    _, key_heads, span, _ = cache_keys.shape
    tokens, width = residual.shape
    bf16 = jnp.bfloat16
    spread = pl.pallas_call(
        attention_kernel,
        out_shape=jax.ShapeDtypeStruct((peers, heads, size), bf16),
        in_specs=[pl.BlockSpec(memory_space=pltpu.SMEM)]
        + [in_vmem()] * 4
        + [pl.BlockSpec(memory_space=pl.ANY)] * 3,
        out_specs=in_vmem(),
        scratch_shapes=[
            VMEM((key_heads, span, size), bf16),
            VMEM((key_heads, span, size), bf16),
            VMEM((heads, span), jnp.float32),
            pltpu.SemaphoreType.DMA((2 * chunk_count + 1,)),
        ],
        compiler_params=params(12),
        name="attention",
    )(
        lengths,
        queries[0],
        fresh_token_key[0],
        value_new[0],
        forget_logit,
        cache_keys,
        cache_values,
        cache_cumlog,
    )
    rows = exchange(spread)
    stream = pl.pallas_call(
        projection_kernel,
        out_shape=jax.ShapeDtypeStruct((peers, tokens, width), bf16),
        in_specs=[in_vmem()] * 3,
        out_specs=in_vmem(),
        compiler_params=params(4),
        name="projection",
    )(rows, out_weight, residual)
    blocks = exchange(stream)
    expert = lax.axis_index("ep").reshape(1)
    outgoing = pl.pallas_call(
        expert_kernel,
        out_shape=jax.ShapeDtypeStruct((peers, 2 * tokens, width), bf16),
        in_specs=[pl.BlockSpec(memory_space=pltpu.SMEM)] + [in_vmem()] * 9,
        out_specs=in_vmem(),
        compiler_params=params(16),
        name="experts",
    )(
        expert,
        blocks,
        norm_gain.reshape(peers, width),
        routes.T,
        route_scores.T,
        expert_gate[0],
        expert_up[0],
        expert_down[0],
        shared_gate,
        shared_up,
    )
    received = exchange(outgoing)
    return pl.pallas_call(
        combine_kernel,
        out_shape=jax.ShapeDtypeStruct((tokens, width), bf16),
        in_specs=[in_vmem()] * 3,
        out_specs=in_vmem(),
        compiler_params=params(4),
        name="combine",
    )(received, stream, shared_down)


def on_device(*arrays):
    residual, expert_gate, shared_gate = arrays[8], arrays[11], arrays[14]
    queries, cache_keys = arrays[0], arrays[4]
    fits = (
        residual.shape[1] % 128 == 0
        and residual.shape[0] % 16 == 0
        and shared_gate.shape[0] % 8 == 0
        and shared_gate.shape[0] <= residual.shape[1]
        and expert_gate.shape[0] == 1
        and queries.shape[0] == 1
        and cache_keys.shape[2] % (128 * chunk_count) == 0
    )
    return kernel_device(*arrays) if fits else plain_device(*arrays)


def solution(mesh):
    placed = (
        P(("grp", "ep"), None, None),
        P(("grp", "ep"), None, None),
        P(("grp", "ep"), None, None),
        P(("grp", "ep"), None),
        P(("grp", "ep"), None, None, None),
        P(("grp", "ep"), None, None, None),
        P(("grp", "ep"), None, None),
        P(("grp", "ep")),
        P("grp", "ep"),
        P(None, "ep"),
        P(),
        P("ep", None, None),
        P("ep", None, None),
        P("ep", None, None),
        P("ep", None),
        P("ep", None),
        P(None, "ep"),
        P("grp", None),
        P("grp", None),
    )
    return jax.shard_map(
        on_device, mesh=mesh, in_specs=placed, out_specs=P("grp", "ep"), check_vma=False
    )
```

```python
import jax
import jax.numpy as jnp
from jax import lax
from jax.experimental import pallas as pl
from jax.experimental.pallas import tpu as pltpu
from jax.sharding import PartitionSpec as P

CAP = 12


norm_eps = 1e-06
routed_scale = 2.5
contract_last = (((1,), (1,)), ((), ()))


def expert_hidden(row_block, gate_matrix, up_matrix):
    gate_part = lax.dot_general(
        row_block, gate_matrix, contract_last, preferred_element_type=jnp.float32
    )
    up_part = lax.dot_general(
        row_block, up_matrix, contract_last, preferred_element_type=jnp.float32
    )
    return (jax.nn.silu(gate_part) * up_part).astype(jnp.bfloat16)


def attention(
    queries,
    fresh_token_key,
    value_new,
    forget_logit,
    cache_keys,
    cache_values,
    cache_cumlog,
    lengths,
):
    batch_rows, head_count, head_size = queries.shape
    key_heads = cache_keys.shape[1]
    cache_span = cache_keys.shape[2]
    groups = head_count // key_heads
    inv_root = head_size ** (-0.5)
    grouped_heads = queries.reshape(batch_rows, key_heads, groups, head_size)
    scores = (
        jnp.einsum(
            "bkgd,bkpd->bkgp", grouped_heads, cache_keys, preferred_element_type=jnp.float32
        ).reshape(batch_rows, head_count, cache_span)
        * inv_root
    )
    positions = lax.broadcasted_iota(jnp.int32, (1, 1, cache_span), 2)
    last_pos = (lengths - 1)[:, None, None]
    latest = jnp.sum(jnp.where(positions == last_pos, cache_cumlog, 0.0), axis=2)
    log_gate = jax.nn.log_sigmoid(forget_logit)
    scores = scores + (latest + log_gate)[:, :, None] - cache_cumlog
    visible = positions < lengths[:, None, None]
    scores = jnp.where(visible, scores, -jnp.inf)
    own_score = (
        jnp.einsum(
            "tiuh,tih->tiu", grouped_heads, fresh_token_key, preferred_element_type=jnp.float32
        ).reshape(batch_rows, head_count)
        * inv_root
    )
    top_score = jnp.maximum(jnp.max(scores, axis=2), own_score)
    weights = jnp.where(visible, jnp.exp(scores - top_score[:, :, None]), 0.0)
    own_weight = jnp.exp(own_score - top_score)
    denominator = jnp.sum(weights, axis=2) + own_weight
    weighted = jnp.einsum(
        "bkgp,bkpd->bkgd",
        weights.astype(jnp.bfloat16).reshape(batch_rows, key_heads, groups, cache_span),
        cache_values,
        preferred_element_type=jnp.float32,
    )
    own_rounded = lax.optimization_barrier(own_weight.astype(jnp.bfloat16)).astype(jnp.float32)
    own_value = jnp.repeat(value_new, groups, axis=1).astype(jnp.float32)
    numerator = (
        weighted.reshape(batch_rows, head_count, head_size) + own_rounded[:, :, None] * own_value
    )
    return (
        (numerator / denominator[:, :, None])
        .astype(jnp.bfloat16)
        .reshape(batch_rows, head_count * head_size)
    )


def plain_device(
    queries,
    fresh_token_key,
    value_new,
    forget_logit,
    cache_keys,
    cache_values,
    cache_cumlog,
    lengths,
    residual,
    out_weight,
    norm_gain,
    expert_gate,
    expert_up,
    expert_down,
    shared_gate,
    shared_up,
    shared_down,
    routes,
    route_scores,
):
    attended = attention(
        queries,
        fresh_token_key,
        value_new,
        forget_logit,
        cache_keys,
        cache_values,
        cache_cumlog,
        lengths,
    )
    mixed = jnp.dot(
        lax.all_gather(attended, "ep", axis=0, tiled=True),
        out_weight,
        preferred_element_type=jnp.float32,
    )
    stream = (residual.astype(jnp.float32) + mixed).astype(jnp.bfloat16)
    full_rows = lax.all_gather(stream, "ep", axis=1, tiled=True)
    rows_wide = full_rows.astype(jnp.float32)
    inv_rms = lax.rsqrt(jnp.mean(rows_wide * rows_wide, axis=1, keepdims=True) + norm_eps)
    normed = (rows_wide * inv_rms * norm_gain).astype(jnp.bfloat16)
    gate_weights = route_scores / jnp.sum(route_scores, axis=1, keepdims=True) * routed_scale
    shared_mid = expert_hidden(normed, shared_gate, shared_up)
    my_expert = lax.axis_index("ep")
    expert_hits = routes == my_expert
    is_member = jnp.sum(expert_hits.astype(jnp.int32), axis=1)
    slot_rank = jnp.cumsum(is_member) - 1
    slot_ids = lax.broadcasted_iota(jnp.int32, (CAP, 1), 0)
    selector = (is_member[None, :] == 1) & (slot_rank[None, :] == slot_ids)
    picked = jnp.dot(
        selector.astype(jnp.bfloat16), normed, preferred_element_type=jnp.float32
    ).astype(jnp.bfloat16)
    hidden = expert_hidden(picked, expert_gate[0], expert_up[0])
    expert_out = jnp.dot(hidden, expert_down[0], preferred_element_type=jnp.float32).astype(
        jnp.bfloat16
    )
    received = lax.all_to_all(expert_out[None], "ep", split_axis=2, concat_axis=0, tiled=True)
    expert_count = received.shape[0]
    expert_ids = lax.broadcasted_iota(jnp.int32, (1, 1, expert_count), 2)
    all_hits = routes[:, :, None] == expert_ids
    membership = jnp.sum(all_hits.astype(jnp.int32), axis=1)
    share_all = jnp.sum(jnp.where(all_hits, gate_weights[:, :, None], 0.0), axis=1)
    rank_all = jnp.cumsum(membership, axis=0) - 1
    slot_grid = lax.broadcasted_iota(jnp.int32, (1, 1, CAP), 2)
    slot_mask = (membership[:, :, None] == 1) & (rank_all[:, :, None] == slot_grid)
    combiner = jnp.where(slot_mask, share_all[:, :, None], 0.0).reshape(
        routes.shape[0], expert_count * CAP
    )
    flat_slots = received.reshape(expert_count * CAP, received.shape[2]).astype(jnp.float32)
    routed_part = jnp.dot(combiner, flat_slots, precision=lax.Precision.HIGHEST)
    shared_part = jnp.dot(
        lax.all_gather(shared_mid, "ep", axis=1, tiled=True),
        shared_down,
        preferred_element_type=jnp.float32,
    )
    return (stream.astype(jnp.float32) + routed_part + shared_part).astype(jnp.bfloat16)


VMEM = pltpu.VMEM
chunk_count = 4


def in_vmem():
    return pl.BlockSpec(memory_space=VMEM)


def in_hbm():
    return pl.BlockSpec(memory_space=pltpu.HBM)


def held_in_hbm(*arrays):
    return [pltpu.with_memory_space_constraint(a, pltpu.HBM) for a in arrays]


def params(mib):
    return pltpu.CompilerParams(vmem_limit_bytes=mib * 1024 * 1024)


def attention_kernel(
    lengths_ref,
    queries_hbm,
    fresh_hbm,
    value_new_hbm,
    forget_hbm,
    keys_hbm,
    values_hbm,
    cumlog_hbm,
    out_ref,
    queries_ref,
    fresh_ref,
    value_new_ref,
    forget_ref,
    keys,
    values,
    cumlog,
    sems,
):
    heads, size = queries_ref.shape
    key_heads, span, _ = keys.shape
    groups = heads // key_heads
    step = span // chunk_count
    inv_root = size ** (-0.5)
    small_copies = [
        pltpu.make_async_copy(source, target, sems.at[2 * chunk_count + i])
        for i, (source, target) in enumerate(
            (
                (queries_hbm.at[0], queries_ref),
                (fresh_hbm.at[0], fresh_ref),
                (forget_hbm, forget_ref),
                (value_new_hbm.at[0], value_new_ref),
                (cumlog_hbm.at[0], cumlog),
            )
        )
    ]
    for copy in small_copies:
        copy.start()

    def copies(source, target, first):
        return [
            pltpu.make_async_copy(
                source.at[0, :, pl.ds(c * step, step), :],
                target.at[:, pl.ds(c * step, step), :],
                sems.at[first + c],
            )
            for c in range(chunk_count)
        ]

    key_copies = copies(keys_hbm, keys, 0)
    value_copies = copies(values_hbm, values, chunk_count)
    for copy in key_copies + value_copies:
        copy.start()

    length = lengths_ref[0]
    for copy in small_copies[:-1]:
        copy.wait()
    queries = queries_ref[...]
    head_rows = lax.broadcasted_iota(jnp.int32, (heads, 1), 0)
    wide = jnp.concatenate(
        [jnp.where(head_rows // groups == k, queries, jnp.zeros_like(queries)) for k in range(key_heads)],
        axis=1,
    )

    def per_head(ref):
        rows = ref[...].astype(jnp.float32)
        total = jnp.zeros((heads, size), jnp.float32)
        for k in range(key_heads):
            total = jnp.where(head_rows // groups == k, rows[k : k + 1, :], total)
        return total

    own_score = (
        jnp.sum(queries.astype(jnp.float32) * per_head(fresh_ref), axis=1, keepdims=True) * inv_root
    )
    logit_row = jnp.broadcast_to(forget_ref[...], (heads, heads))
    diagonal = lax.broadcasted_iota(jnp.int32, (heads, heads), 1) == head_rows
    logit = jnp.sum(jnp.where(diagonal, logit_row, 0.0), axis=1, keepdims=True)
    log_gate = jnp.minimum(logit, 0.0) - jnp.log1p(jnp.exp(-jnp.abs(logit)))
    small_copies[-1].wait()
    positions = lax.broadcasted_iota(jnp.int32, (heads, span), 1)
    latest = jnp.sum(
        jnp.where(positions == length - 1, cumlog[...], 0.0), axis=1, keepdims=True
    )
    offset = latest + log_gate
    scores = []
    for c in range(chunk_count):
        key_copies[c].wait()
        block = jnp.concatenate(
            [keys[k, c * step : (c + 1) * step, :] for k in range(key_heads)], axis=1
        )
        raw = lax.dot_general(wide, block, contract_last, preferred_element_type=jnp.float32)
        raw = raw * inv_root + offset - cumlog[:, c * step : (c + 1) * step]
        visible = positions[:, c * step : (c + 1) * step] < length
        scores.append(jnp.where(visible, raw, -jnp.inf))
    top = own_score
    for part in scores:
        top = jnp.maximum(top, jnp.max(part, axis=1, keepdims=True))
    own_weight = jnp.exp(own_score - top)
    denominator = own_weight
    total = jnp.zeros((heads, key_heads * size), jnp.float32)
    for c in range(chunk_count):
        weights = jnp.exp(scores[c] - top)
        denominator = denominator + jnp.sum(weights, axis=1, keepdims=True)
        value_copies[c].wait()
        block = jnp.concatenate(
            [values[k, c * step : (c + 1) * step, :] for k in range(key_heads)], axis=1
        )
        total = total + jnp.dot(
            weights.astype(jnp.bfloat16), block, preferred_element_type=jnp.float32
        )
    mine = own_weight.astype(jnp.bfloat16).astype(jnp.float32) * per_head(value_new_ref)
    for k in range(key_heads):
        mine = mine + jnp.where(
            head_rows // groups == k, total[:, k * size : (k + 1) * size], 0.0
        )
    attended = (mine / denominator).astype(jnp.bfloat16)
    for peer in range(out_ref.shape[0]):
        out_ref[peer] = attended


def projection_kernel(rows_ref, weight_ref, residual_ref, out_ref):
    tokens, heads, size = rows_ref.shape
    stacked = rows_ref[...].reshape(tokens * heads, size)
    which = lax.broadcasted_iota(jnp.int32, (tokens * heads, 1), 0) % heads
    wide = jnp.concatenate(
        [jnp.where(which == h, stacked, jnp.zeros_like(stacked)) for h in range(heads)], axis=1
    )
    product = jnp.dot(wide, weight_ref[...], preferred_element_type=jnp.float32)
    mixed = jnp.sum(product.reshape(tokens, heads, product.shape[1]), axis=1)
    stream = (residual_ref[...].astype(jnp.float32) + mixed).astype(jnp.bfloat16)
    for peer in range(out_ref.shape[0]):
        out_ref[peer] = stream


def silu_product(gate, up):
    return gate / (1.0 + jnp.exp(-gate)) * up


def expert_kernel(
    blocks_ref,
    gain_ref,
    routes_ref,
    scores_ref,
    gate_ref,
    up_ref,
    down_ref,
    shared_gate_ref,
    shared_up_ref,
    out_ref,
):
    peers, tokens, width = blocks_ref.shape
    wide = [blocks_ref[p].astype(jnp.float32) for p in range(peers)]
    squares = wide[0] * wide[0]
    for block in wide[1:]:
        squares = squares + block * block
    mean = jnp.sum(squares, axis=1, keepdims=True) / (peers * width)
    inv_rms = lax.rsqrt(mean + norm_eps)
    normed = jnp.concatenate(
        [
            (wide[p] * inv_rms * gain_ref[p : p + 1, :]).astype(jnp.bfloat16)
            for p in range(peers)
        ],
        axis=1,
    )
    scores = scores_ref[...]
    shares = scores / jnp.sum(scores, axis=0, keepdims=True) * routed_scale
    share = jnp.sum(
        jnp.where(routes_ref[...] == lax.axis_index("ep"), shares, 0.0), axis=0, keepdims=True
    )

    def against(matrix):
        return lax.dot_general(matrix, normed, contract_last, preferred_element_type=jnp.float32)

    shared_hidden = silu_product(against(shared_gate_ref[...]), against(shared_up_ref[...])).astype(
        jnp.bfloat16
    )
    units = shared_hidden.shape[0]
    spread = (
        lax.broadcasted_iota(jnp.int32, (units, width), 0)
        == lax.broadcasted_iota(jnp.int32, (units, width), 1)
    ).astype(jnp.bfloat16)
    contract_first = (((0,), (0,)), ((), ()))
    shared_rows = lax.dot_general(
        shared_hidden, spread, contract_first, preferred_element_type=jnp.float32
    ).astype(jnp.bfloat16)
    hidden = (silu_product(against(gate_ref[...]), against(up_ref[...])) * share).astype(
        jnp.bfloat16
    )
    result = lax.dot_general(
        hidden, down_ref[...], contract_first, preferred_element_type=jnp.float32
    ).astype(jnp.bfloat16)
    for p in range(peers):
        out_ref[p, :tokens, :] = result[:, p * width : (p + 1) * width]
        out_ref[p, tokens:, :] = shared_rows


def combine_kernel(received_ref, stream_ref, down_ref, out_ref):
    peers, double, width = received_ref.shape
    tokens = double // 2
    units = down_ref.shape[0] // peers
    total = stream_ref[0].astype(jnp.float32)
    for p in range(peers):
        total = total + received_ref[p, :tokens, :].astype(jnp.float32)
    for p in range(peers):
        total = total + jnp.dot(
            received_ref[p, tokens:, :][:, :units],
            down_ref[p * units : (p + 1) * units, :],
            preferred_element_type=jnp.float32,
        )
    out_ref[...] = total.astype(jnp.bfloat16)


def exchange(blocks):
    return lax.all_to_all(blocks, "ep", split_axis=0, concat_axis=0, tiled=True)


def kernel_device(
    queries,
    fresh_token_key,
    value_new,
    forget_logit,
    cache_keys,
    cache_values,
    cache_cumlog,
    lengths,
    residual,
    out_weight,
    norm_gain,
    expert_gate,
    expert_up,
    expert_down,
    shared_gate,
    shared_up,
    shared_down,
    routes,
    route_scores,
):
    peers = lax.axis_size("ep")
    _, heads, size = queries.shape
    _, key_heads, span, _ = cache_keys.shape
    tokens, width = residual.shape
    bf16 = jnp.bfloat16
    spread = pl.pallas_call(
        attention_kernel,
        out_shape=VMEM((peers, heads, size), bf16),
        in_specs=[pl.BlockSpec(memory_space=pltpu.SMEM)] + [in_hbm()] * 7,
        out_specs=in_vmem(),
        scratch_shapes=[
            VMEM((heads, size), bf16),
            VMEM((key_heads, size), bf16),
            VMEM((key_heads, size), bf16),
            VMEM((1, heads), jnp.float32),
            VMEM((key_heads, span, size), bf16),
            VMEM((key_heads, span, size), bf16),
            VMEM((heads, span), jnp.float32),
            pltpu.SemaphoreType.DMA((2 * chunk_count + 5,)),
        ],
        compiler_params=params(12),
        name="attention",
    )(
        lengths,
        *held_in_hbm(
            queries,
            fresh_token_key,
            value_new,
            forget_logit,
            cache_keys,
            cache_values,
            cache_cumlog,
        ),
    )
    rows = exchange(spread)
    stream = pl.pallas_call(
        projection_kernel,
        out_shape=VMEM((peers, tokens, width), bf16),
        in_specs=[in_vmem()] * 3,
        out_specs=in_vmem(),
        compiler_params=params(4),
        cost_estimate=pl.CostEstimate(flops=100000000000, bytes_accessed=0, transcendentals=0),
        name="projection",
    )(rows, out_weight, residual)
    blocks = exchange(stream)
    outgoing = pl.pallas_call(
        expert_kernel,
        out_shape=VMEM((peers, 2 * tokens, width), bf16),
        in_specs=[in_vmem()] * 9,
        out_specs=in_vmem(),
        compiler_params=params(16),
        name="experts",
    )(
        blocks,
        norm_gain.reshape(peers, width),
        routes.T,
        route_scores.T,
        *(
            pltpu.with_memory_space_constraint(a, VMEM)
            for a in (expert_gate[0], expert_up[0], expert_down[0], shared_gate, shared_up)
        ),
    )
    received = exchange(outgoing)
    return pl.pallas_call(
        combine_kernel,
        out_shape=jax.ShapeDtypeStruct((tokens, width), bf16),
        in_specs=[in_vmem()] * 3,
        out_specs=in_vmem(),
        compiler_params=params(4),
        name="combine",
    )(received, stream, shared_down)


def on_device(*arrays):
    residual, expert_gate, shared_gate = arrays[8], arrays[11], arrays[14]
    queries, cache_keys = arrays[0], arrays[4]
    fits = (
        residual.shape[1] % 128 == 0
        and residual.shape[0] % 16 == 0
        and shared_gate.shape[0] % 8 == 0
        and shared_gate.shape[0] <= residual.shape[1]
        and expert_gate.shape[0] == 1
        and queries.shape[0] == 1
        and cache_keys.shape[2] % (128 * chunk_count) == 0
    )
    return kernel_device(*arrays) if fits else plain_device(*arrays)


def solution(mesh):
    placed = (
        P(("grp", "ep"), None, None),
        P(("grp", "ep"), None, None),
        P(("grp", "ep"), None, None),
        P(("grp", "ep"), None),
        P(("grp", "ep"), None, None, None),
        P(("grp", "ep"), None, None, None),
        P(("grp", "ep"), None, None),
        P(("grp", "ep")),
        P("grp", "ep"),
        P(None, "ep"),
        P(),
        P("ep", None, None),
        P("ep", None, None),
        P("ep", None, None),
        P("ep", None),
        P("ep", None),
        P(None, "ep"),
        P("grp", None),
        P("grp", None),
    )
    return jax.shard_map(
        on_device, mesh=mesh, in_specs=placed, out_specs=P("grp", "ep"), check_vma=False
    )
```

```python
import jax
import jax.numpy as jnp
from jax import lax
from jax.experimental import pallas as pl
from jax.experimental.pallas import tpu as pltpu
from jax.sharding import PartitionSpec as P

CAP = 12


norm_eps = 1e-06
routed_scale = 2.5
contract_last = (((1,), (1,)), ((), ()))


def expert_hidden(row_block, gate_matrix, up_matrix):
    gate_part = lax.dot_general(
        row_block, gate_matrix, contract_last, preferred_element_type=jnp.float32
    )
    up_part = lax.dot_general(
        row_block, up_matrix, contract_last, preferred_element_type=jnp.float32
    )
    return (jax.nn.silu(gate_part) * up_part).astype(jnp.bfloat16)


def attention(
    queries,
    fresh_token_key,
    value_new,
    forget_logit,
    cache_keys,
    cache_values,
    cache_cumlog,
    lengths,
):
    batch_rows, head_count, head_size = queries.shape
    key_heads = cache_keys.shape[1]
    cache_span = cache_keys.shape[2]
    groups = head_count // key_heads
    inv_root = head_size ** (-0.5)
    grouped_heads = queries.reshape(batch_rows, key_heads, groups, head_size)
    scores = (
        jnp.einsum(
            "bkgd,bkpd->bkgp", grouped_heads, cache_keys, preferred_element_type=jnp.float32
        ).reshape(batch_rows, head_count, cache_span)
        * inv_root
    )
    positions = lax.broadcasted_iota(jnp.int32, (1, 1, cache_span), 2)
    last_pos = (lengths - 1)[:, None, None]
    latest = jnp.sum(jnp.where(positions == last_pos, cache_cumlog, 0.0), axis=2)
    log_gate = jax.nn.log_sigmoid(forget_logit)
    scores = scores + (latest + log_gate)[:, :, None] - cache_cumlog
    visible = positions < lengths[:, None, None]
    scores = jnp.where(visible, scores, -jnp.inf)
    own_score = (
        jnp.einsum(
            "tiuh,tih->tiu", grouped_heads, fresh_token_key, preferred_element_type=jnp.float32
        ).reshape(batch_rows, head_count)
        * inv_root
    )
    top_score = jnp.maximum(jnp.max(scores, axis=2), own_score)
    weights = jnp.where(visible, jnp.exp(scores - top_score[:, :, None]), 0.0)
    own_weight = jnp.exp(own_score - top_score)
    denominator = jnp.sum(weights, axis=2) + own_weight
    weighted = jnp.einsum(
        "bkgp,bkpd->bkgd",
        weights.astype(jnp.bfloat16).reshape(batch_rows, key_heads, groups, cache_span),
        cache_values,
        preferred_element_type=jnp.float32,
    )
    own_rounded = lax.optimization_barrier(own_weight.astype(jnp.bfloat16)).astype(jnp.float32)
    own_value = jnp.repeat(value_new, groups, axis=1).astype(jnp.float32)
    numerator = (
        weighted.reshape(batch_rows, head_count, head_size) + own_rounded[:, :, None] * own_value
    )
    return (
        (numerator / denominator[:, :, None])
        .astype(jnp.bfloat16)
        .reshape(batch_rows, head_count * head_size)
    )


def plain_device(
    queries,
    fresh_token_key,
    value_new,
    forget_logit,
    cache_keys,
    cache_values,
    cache_cumlog,
    lengths,
    residual,
    out_weight,
    norm_gain,
    expert_gate,
    expert_up,
    expert_down,
    shared_gate,
    shared_up,
    shared_down,
    routes,
    route_scores,
):
    attended = attention(
        queries,
        fresh_token_key,
        value_new,
        forget_logit,
        cache_keys,
        cache_values,
        cache_cumlog,
        lengths,
    )
    mixed = jnp.dot(
        lax.all_gather(attended, "ep", axis=0, tiled=True),
        out_weight,
        preferred_element_type=jnp.float32,
    )
    stream = (residual.astype(jnp.float32) + mixed).astype(jnp.bfloat16)
    full_rows = lax.all_gather(stream, "ep", axis=1, tiled=True)
    rows_wide = full_rows.astype(jnp.float32)
    inv_rms = lax.rsqrt(jnp.mean(rows_wide * rows_wide, axis=1, keepdims=True) + norm_eps)
    normed = (rows_wide * inv_rms * norm_gain).astype(jnp.bfloat16)
    gate_weights = route_scores / jnp.sum(route_scores, axis=1, keepdims=True) * routed_scale
    shared_mid = expert_hidden(normed, shared_gate, shared_up)
    my_expert = lax.axis_index("ep")
    expert_hits = routes == my_expert
    is_member = jnp.sum(expert_hits.astype(jnp.int32), axis=1)
    slot_rank = jnp.cumsum(is_member) - 1
    slot_ids = lax.broadcasted_iota(jnp.int32, (CAP, 1), 0)
    selector = (is_member[None, :] == 1) & (slot_rank[None, :] == slot_ids)
    picked = jnp.dot(
        selector.astype(jnp.bfloat16), normed, preferred_element_type=jnp.float32
    ).astype(jnp.bfloat16)
    hidden = expert_hidden(picked, expert_gate[0], expert_up[0])
    expert_out = jnp.dot(hidden, expert_down[0], preferred_element_type=jnp.float32).astype(
        jnp.bfloat16
    )
    received = lax.all_to_all(expert_out[None], "ep", split_axis=2, concat_axis=0, tiled=True)
    expert_count = received.shape[0]
    expert_ids = lax.broadcasted_iota(jnp.int32, (1, 1, expert_count), 2)
    all_hits = routes[:, :, None] == expert_ids
    membership = jnp.sum(all_hits.astype(jnp.int32), axis=1)
    share_all = jnp.sum(jnp.where(all_hits, gate_weights[:, :, None], 0.0), axis=1)
    rank_all = jnp.cumsum(membership, axis=0) - 1
    slot_grid = lax.broadcasted_iota(jnp.int32, (1, 1, CAP), 2)
    slot_mask = (membership[:, :, None] == 1) & (rank_all[:, :, None] == slot_grid)
    combiner = jnp.where(slot_mask, share_all[:, :, None], 0.0).reshape(
        routes.shape[0], expert_count * CAP
    )
    flat_slots = received.reshape(expert_count * CAP, received.shape[2]).astype(jnp.float32)
    routed_part = jnp.dot(combiner, flat_slots, precision=lax.Precision.HIGHEST)
    shared_part = jnp.dot(
        lax.all_gather(shared_mid, "ep", axis=1, tiled=True),
        shared_down,
        preferred_element_type=jnp.float32,
    )
    return (stream.astype(jnp.float32) + routed_part + shared_part).astype(jnp.bfloat16)


VMEM = pltpu.VMEM
key_cuts = (0, 1, 4)
value_cuts = (0, 4)


def in_vmem():
    return pl.BlockSpec(memory_space=VMEM)


def in_hbm():
    return pl.BlockSpec(memory_space=pltpu.HBM)


def held_in_hbm(*arrays):
    return [pltpu.with_memory_space_constraint(a, pltpu.HBM) for a in arrays]


def params(mib):
    return pltpu.CompilerParams(vmem_limit_bytes=mib * 1024 * 1024)


def attention_kernel(
    lengths_ref,
    queries_hbm,
    fresh_hbm,
    value_new_hbm,
    forget_hbm,
    keys_hbm,
    values_hbm,
    cumlog_hbm,
    out_ref,
    queries_ref,
    fresh_ref,
    value_new_ref,
    forget_ref,
    keys,
    values,
    scores,
    sems,
):
    heads, size = queries_ref.shape
    key_heads, span, _ = keys.shape
    groups = heads // key_heads
    inv_root = size ** (-0.5)
    first = len(key_cuts) + len(value_cuts) - 2
    small_copies = [
        pltpu.make_async_copy(source, target, sems.at[first + i])
        for i, (source, target) in enumerate(
            (
                (cumlog_hbm.at[0], scores),
                (queries_hbm.at[0], queries_ref),
                (fresh_hbm.at[0], fresh_ref),
                (forget_hbm, forget_ref),
                (value_new_hbm.at[0], value_new_ref),
            )
        )
    ]

    def pieces(cuts):
        edges = [span * cut // cuts[-1] for cut in cuts]
        return list(zip(edges[:-1], edges[1:]))

    def copies(source, target, cuts, first):
        return [
            pltpu.make_async_copy(
                source.at[0, :, pl.ds(low, high - low), :],
                target.at[:, pl.ds(low, high - low), :],
                sems.at[first + i],
            )
            for i, (low, high) in enumerate(pieces(cuts))
        ]

    key_copies = copies(keys_hbm, keys, key_cuts, 0)
    value_copies = copies(values_hbm, values, value_cuts, len(key_cuts) - 1)
    for copy in small_copies + key_copies + value_copies:
        copy.start()

    def side_by_side(ref, low, high):
        return jnp.concatenate([ref[k, low:high, :] for k in range(key_heads)], axis=1)

    head_rows = lax.broadcasted_iota(jnp.int32, (heads, 1), 0)

    def per_head(ref):
        rows = ref[...].astype(jnp.float32)
        total = jnp.zeros((heads, size), jnp.float32)
        for k in range(key_heads):
            total = jnp.where(head_rows // groups == k, rows[k : k + 1, :], total)
        return total

    for copy in small_copies:
        copy.wait()
    length = lengths_ref[0]
    queries = queries_ref[...]
    wide = jnp.concatenate(
        [
            jnp.where(head_rows // groups == k, queries, jnp.zeros_like(queries))
            for k in range(key_heads)
        ],
        axis=1,
    )
    own_score = (
        jnp.sum(queries.astype(jnp.float32) * per_head(fresh_ref), axis=1, keepdims=True) * inv_root
    )
    logit_row = jnp.broadcast_to(forget_ref[...], (heads, heads))
    diagonal = lax.broadcasted_iota(jnp.int32, (heads, heads), 1) == head_rows
    logit = jnp.sum(jnp.where(diagonal, logit_row, 0.0), axis=1, keepdims=True)
    log_gate = jnp.minimum(logit, 0.0) - jnp.log1p(jnp.exp(-jnp.abs(logit)))
    positions = lax.broadcasted_iota(jnp.int32, (heads, span), 1)
    cumlog = scores[...]
    latest = jnp.sum(jnp.where(positions == length - 1, cumlog, 0.0), axis=1, keepdims=True)
    scores[...] = jnp.where(positions < length, latest + log_gate - cumlog, -jnp.inf)
    top = own_score
    for copy, (low, high) in zip(key_copies, pieces(key_cuts)):
        copy.wait()
        raw = lax.dot_general(
            wide,
            side_by_side(keys, low, high),
            contract_last,
            preferred_element_type=jnp.float32,
        )
        part = raw * inv_root + scores[:, low:high]
        scores[:, low:high] = part
        top = jnp.maximum(top, jnp.max(part, axis=1, keepdims=True))
    weights = jnp.exp(scores[...] - top)
    own_weight = jnp.exp(own_score - top)
    denominator = own_weight + jnp.sum(weights, axis=1, keepdims=True)
    weights = weights.astype(jnp.bfloat16)
    mine = own_weight.astype(jnp.bfloat16).astype(jnp.float32) * per_head(value_new_ref)
    total = jnp.zeros((heads, key_heads * size), jnp.float32)
    for copy, (low, high) in zip(value_copies, pieces(value_cuts)):
        copy.wait()
        total = total + jnp.dot(
            weights[:, low:high],
            side_by_side(values, low, high),
            preferred_element_type=jnp.float32,
        )
    for k in range(key_heads):
        mine = mine + jnp.where(
            head_rows // groups == k, total[:, k * size : (k + 1) * size], 0.0
        )
    attended = (mine / denominator).astype(jnp.bfloat16)
    for peer in range(out_ref.shape[0]):
        out_ref[peer] = attended


def attend(queries, fresh_token_key, value_new, forget_logit, cache_keys, cache_values, cache_cumlog, lengths):
    peers = lax.axis_size("ep")
    _, heads, size = queries.shape
    _, key_heads, span, _ = cache_keys.shape
    bf16 = jnp.bfloat16
    return pl.pallas_call(
        attention_kernel,
        out_shape=VMEM((peers, heads, size), bf16),
        in_specs=[pl.BlockSpec(memory_space=pltpu.SMEM)] + [in_hbm()] * 7,
        out_specs=in_vmem(),
        scratch_shapes=[
            VMEM((heads, size), bf16),
            VMEM((key_heads, size), bf16),
            VMEM((key_heads, size), bf16),
            VMEM((1, heads), jnp.float32),
            VMEM((key_heads, span, size), bf16),
            VMEM((key_heads, span, size), bf16),
            VMEM((heads, span), jnp.float32),
            pltpu.SemaphoreType.DMA((len(key_cuts) + len(value_cuts) + 3,)),
        ],
        compiler_params=params(12),
        name="attention",
    )(
        lengths,
        *held_in_hbm(
            queries,
            fresh_token_key,
            value_new,
            forget_logit,
            cache_keys,
            cache_values,
            cache_cumlog,
        ),
    )


def projection_kernel(rows_ref, weight_ref, residual_ref, out_ref):
    tokens, heads, size = rows_ref.shape
    stacked = rows_ref[...].reshape(tokens * heads, size)
    which = lax.broadcasted_iota(jnp.int32, (tokens * heads, 1), 0) % heads
    wide = jnp.concatenate(
        [jnp.where(which == h, stacked, jnp.zeros_like(stacked)) for h in range(heads)], axis=1
    )
    product = jnp.dot(wide, weight_ref[...], preferred_element_type=jnp.float32)
    mixed = jnp.sum(product.reshape(tokens, heads, product.shape[1]), axis=1)
    stream = (residual_ref[...].astype(jnp.float32) + mixed).astype(jnp.bfloat16)
    for peer in range(out_ref.shape[0]):
        out_ref[peer] = stream


def silu_product(gate, up):
    return gate / (1.0 + jnp.exp(-gate)) * up


def expert_kernel(
    blocks_ref,
    gain_ref,
    routes_ref,
    scores_ref,
    gate_ref,
    up_ref,
    down_ref,
    shared_gate_ref,
    shared_up_ref,
    out_ref,
):
    peers, tokens, width = blocks_ref.shape
    wide = [blocks_ref[p].astype(jnp.float32) for p in range(peers)]
    squares = wide[0] * wide[0]
    for block in wide[1:]:
        squares = squares + block * block
    mean = jnp.sum(squares, axis=1, keepdims=True) / (peers * width)
    inv_rms = lax.rsqrt(mean + norm_eps)
    normed = jnp.concatenate(
        [
            (wide[p] * inv_rms * gain_ref[p : p + 1, :]).astype(jnp.bfloat16)
            for p in range(peers)
        ],
        axis=1,
    )
    scores = scores_ref[...]
    shares = scores / jnp.sum(scores, axis=0, keepdims=True) * routed_scale
    share = jnp.sum(
        jnp.where(routes_ref[...] == lax.axis_index("ep"), shares, 0.0), axis=0, keepdims=True
    )

    def against(matrix):
        return lax.dot_general(matrix, normed, contract_last, preferred_element_type=jnp.float32)

    hidden = (silu_product(against(gate_ref[...]), against(up_ref[...])) * share).astype(
        jnp.bfloat16
    )
    shared_hidden = silu_product(against(shared_gate_ref[...]), against(shared_up_ref[...])).astype(
        jnp.bfloat16
    )
    units = shared_hidden.shape[0]
    spread = (
        lax.broadcasted_iota(jnp.int32, (units, width), 0)
        == lax.broadcasted_iota(jnp.int32, (units, width), 1)
    ).astype(jnp.bfloat16)
    contract_first = (((0,), (0,)), ((), ()))
    shared_rows = lax.dot_general(
        shared_hidden, spread, contract_first, preferred_element_type=jnp.float32
    ).astype(jnp.bfloat16)
    result = lax.dot_general(
        hidden, down_ref[...], contract_first, preferred_element_type=jnp.float32
    ).astype(jnp.bfloat16)
    for p in range(peers):
        out_ref[p, :tokens, :] = result[:, p * width : (p + 1) * width]
        out_ref[p, tokens:, :] = shared_rows


def run_experts(
    blocks,
    norm_gain,
    routes,
    route_scores,
    expert_gate,
    expert_up,
    expert_down,
    shared_gate,
    shared_up,
):
    peers, tokens, width = blocks.shape
    bf16 = jnp.bfloat16
    return pl.pallas_call(
        expert_kernel,
        out_shape=VMEM((peers, 2 * tokens, width), bf16),
        in_specs=[in_vmem()] * 9,
        out_specs=in_vmem(),
        compiler_params=params(16),
        name="experts",
    )(
        blocks,
        norm_gain.reshape(peers, width),
        routes.T,
        route_scores.T,
        *(
            pltpu.with_memory_space_constraint(a, VMEM)
            for a in (expert_gate[0], expert_up[0], expert_down[0], shared_gate, shared_up)
        ),
    )


def combine_kernel(received_ref, stream_ref, down_ref, out_ref):
    peers, double, width = received_ref.shape
    tokens = double // 2
    units = down_ref.shape[0] // peers
    total = stream_ref[0].astype(jnp.float32)
    for p in range(peers):
        total = total + received_ref[p, :tokens, :].astype(jnp.float32)
    for p in range(peers):
        total = total + jnp.dot(
            received_ref[p, tokens:, :][:, :units],
            down_ref[p * units : (p + 1) * units, :],
            preferred_element_type=jnp.float32,
        )
    out_ref[...] = total.astype(jnp.bfloat16)


def combine(received, stream, shared_down):
    tokens, width = stream.shape[1:]
    bf16 = jnp.bfloat16
    return pl.pallas_call(
        combine_kernel,
        out_shape=jax.ShapeDtypeStruct((tokens, width), bf16),
        in_specs=[in_vmem()] * 3,
        out_specs=in_vmem(),
        compiler_params=params(4),
        name="combine",
    )(received, stream, shared_down)


def exchange(blocks):
    return lax.all_to_all(blocks, "ep", split_axis=0, concat_axis=0, tiled=True)


def kernel_device(
    queries,
    fresh_token_key,
    value_new,
    forget_logit,
    cache_keys,
    cache_values,
    cache_cumlog,
    lengths,
    residual,
    out_weight,
    norm_gain,
    expert_gate,
    expert_up,
    expert_down,
    shared_gate,
    shared_up,
    shared_down,
    routes,
    route_scores,
):
    peers = lax.axis_size("ep")
    _, heads, size = queries.shape
    _, key_heads, span, _ = cache_keys.shape
    tokens, width = residual.shape
    bf16 = jnp.bfloat16
    spread = attend(
        queries,
        fresh_token_key,
        value_new,
        forget_logit,
        cache_keys,
        cache_values,
        cache_cumlog,
        lengths,
    )
    rows = exchange(spread)
    stream = pl.pallas_call(
        projection_kernel,
        out_shape=VMEM((peers, tokens, width), bf16),
        in_specs=[in_vmem()] * 3,
        out_specs=in_vmem(),
        compiler_params=params(4),
        cost_estimate=pl.CostEstimate(flops=100000000000, bytes_accessed=0, transcendentals=0),
        name="projection",
    )(rows, out_weight, residual)
    blocks = exchange(stream)
    outgoing = run_experts(
        blocks,
        norm_gain,
        routes,
        route_scores,
        expert_gate,
        expert_up,
        expert_down,
        shared_gate,
        shared_up,
    )
    received = exchange(outgoing)
    return combine(received, stream, shared_down)


def on_device(*arrays):
    residual, expert_gate, shared_gate = arrays[8], arrays[11], arrays[14]
    queries, cache_keys = arrays[0], arrays[4]
    fits = (
        residual.shape[1] % 128 == 0
        and residual.shape[0] % 16 == 0
        and shared_gate.shape[0] % 8 == 0
        and shared_gate.shape[0] <= residual.shape[1]
        and expert_gate.shape[0] == 1
        and queries.shape[0] == 1
        and cache_keys.shape[2] % 2048 == 0
    )
    return kernel_device(*arrays) if fits else plain_device(*arrays)


def solution(mesh):
    placed = (
        P(("grp", "ep"), None, None),
        P(("grp", "ep"), None, None),
        P(("grp", "ep"), None, None),
        P(("grp", "ep"), None),
        P(("grp", "ep"), None, None, None),
        P(("grp", "ep"), None, None, None),
        P(("grp", "ep"), None, None),
        P(("grp", "ep")),
        P("grp", "ep"),
        P(None, "ep"),
        P(),
        P("ep", None, None),
        P("ep", None, None),
        P("ep", None, None),
        P("ep", None),
        P("ep", None),
        P(None, "ep"),
        P("grp", None),
        P("grp", None),
    )
    return jax.shard_map(
        on_device, mesh=mesh, in_specs=placed, out_specs=P("grp", "ep"), check_vma=False
    )
```

```python
import jax
import jax.numpy as jnp
from jax import lax
from jax.experimental import pallas as pl
from jax.experimental.pallas import tpu as pltpu
from jax.sharding import PartitionSpec as P

CAP = 12


norm_eps = 1e-06
routed_scale = 2.5
contract_last = (((1,), (1,)), ((), ()))


def expert_hidden(row_block, gate_matrix, up_matrix):
    gate_part = lax.dot_general(
        row_block, gate_matrix, contract_last, preferred_element_type=jnp.float32
    )
    up_part = lax.dot_general(
        row_block, up_matrix, contract_last, preferred_element_type=jnp.float32
    )
    return (jax.nn.silu(gate_part) * up_part).astype(jnp.bfloat16)


def attention(
    queries,
    fresh_token_key,
    value_new,
    forget_logit,
    cache_keys,
    cache_values,
    cache_cumlog,
    lengths,
):
    batch_rows, head_count, head_size = queries.shape
    key_heads = cache_keys.shape[1]
    cache_span = cache_keys.shape[2]
    groups = head_count // key_heads
    inv_root = head_size ** (-0.5)
    grouped_heads = queries.reshape(batch_rows, key_heads, groups, head_size)
    scores = (
        jnp.einsum(
            "bkgd,bkpd->bkgp", grouped_heads, cache_keys, preferred_element_type=jnp.float32
        ).reshape(batch_rows, head_count, cache_span)
        * inv_root
    )
    positions = lax.broadcasted_iota(jnp.int32, (1, 1, cache_span), 2)
    last_pos = (lengths - 1)[:, None, None]
    latest = jnp.sum(jnp.where(positions == last_pos, cache_cumlog, 0.0), axis=2)
    log_gate = jax.nn.log_sigmoid(forget_logit)
    scores = scores + (latest + log_gate)[:, :, None] - cache_cumlog
    visible = positions < lengths[:, None, None]
    scores = jnp.where(visible, scores, -jnp.inf)
    own_score = (
        jnp.einsum(
            "tiuh,tih->tiu", grouped_heads, fresh_token_key, preferred_element_type=jnp.float32
        ).reshape(batch_rows, head_count)
        * inv_root
    )
    top_score = jnp.maximum(jnp.max(scores, axis=2), own_score)
    weights = jnp.where(visible, jnp.exp(scores - top_score[:, :, None]), 0.0)
    own_weight = jnp.exp(own_score - top_score)
    denominator = jnp.sum(weights, axis=2) + own_weight
    weighted = jnp.einsum(
        "bkgp,bkpd->bkgd",
        weights.astype(jnp.bfloat16).reshape(batch_rows, key_heads, groups, cache_span),
        cache_values,
        preferred_element_type=jnp.float32,
    )
    own_rounded = lax.optimization_barrier(own_weight.astype(jnp.bfloat16)).astype(jnp.float32)
    own_value = jnp.repeat(value_new, groups, axis=1).astype(jnp.float32)
    numerator = (
        weighted.reshape(batch_rows, head_count, head_size) + own_rounded[:, :, None] * own_value
    )
    return (
        (numerator / denominator[:, :, None])
        .astype(jnp.bfloat16)
        .reshape(batch_rows, head_count * head_size)
    )


def plain_device(
    queries,
    fresh_token_key,
    value_new,
    forget_logit,
    cache_keys,
    cache_values,
    cache_cumlog,
    lengths,
    residual,
    out_weight,
    norm_gain,
    expert_gate,
    expert_up,
    expert_down,
    shared_gate,
    shared_up,
    shared_down,
    routes,
    route_scores,
):
    attended = attention(
        queries,
        fresh_token_key,
        value_new,
        forget_logit,
        cache_keys,
        cache_values,
        cache_cumlog,
        lengths,
    )
    mixed = jnp.dot(
        lax.all_gather(attended, "ep", axis=0, tiled=True),
        out_weight,
        preferred_element_type=jnp.float32,
    )
    stream = (residual.astype(jnp.float32) + mixed).astype(jnp.bfloat16)
    full_rows = lax.all_gather(stream, "ep", axis=1, tiled=True)
    rows_wide = full_rows.astype(jnp.float32)
    inv_rms = lax.rsqrt(jnp.mean(rows_wide * rows_wide, axis=1, keepdims=True) + norm_eps)
    normed = (rows_wide * inv_rms * norm_gain).astype(jnp.bfloat16)
    gate_weights = route_scores / jnp.sum(route_scores, axis=1, keepdims=True) * routed_scale
    shared_mid = expert_hidden(normed, shared_gate, shared_up)
    my_expert = lax.axis_index("ep")
    expert_hits = routes == my_expert
    is_member = jnp.sum(expert_hits.astype(jnp.int32), axis=1)
    slot_rank = jnp.cumsum(is_member) - 1
    slot_ids = lax.broadcasted_iota(jnp.int32, (CAP, 1), 0)
    selector = (is_member[None, :] == 1) & (slot_rank[None, :] == slot_ids)
    picked = jnp.dot(
        selector.astype(jnp.bfloat16), normed, preferred_element_type=jnp.float32
    ).astype(jnp.bfloat16)
    hidden = expert_hidden(picked, expert_gate[0], expert_up[0])
    expert_out = jnp.dot(hidden, expert_down[0], preferred_element_type=jnp.float32).astype(
        jnp.bfloat16
    )
    received = lax.all_to_all(expert_out[None], "ep", split_axis=2, concat_axis=0, tiled=True)
    expert_count = received.shape[0]
    expert_ids = lax.broadcasted_iota(jnp.int32, (1, 1, expert_count), 2)
    all_hits = routes[:, :, None] == expert_ids
    membership = jnp.sum(all_hits.astype(jnp.int32), axis=1)
    share_all = jnp.sum(jnp.where(all_hits, gate_weights[:, :, None], 0.0), axis=1)
    rank_all = jnp.cumsum(membership, axis=0) - 1
    slot_grid = lax.broadcasted_iota(jnp.int32, (1, 1, CAP), 2)
    slot_mask = (membership[:, :, None] == 1) & (rank_all[:, :, None] == slot_grid)
    combiner = jnp.where(slot_mask, share_all[:, :, None], 0.0).reshape(
        routes.shape[0], expert_count * CAP
    )
    flat_slots = received.reshape(expert_count * CAP, received.shape[2]).astype(jnp.float32)
    routed_part = jnp.dot(combiner, flat_slots, precision=lax.Precision.HIGHEST)
    shared_part = jnp.dot(
        lax.all_gather(shared_mid, "ep", axis=1, tiled=True),
        shared_down,
        preferred_element_type=jnp.float32,
    )
    return (stream.astype(jnp.float32) + routed_part + shared_part).astype(jnp.bfloat16)


VMEM = pltpu.VMEM
cuts = (0, 1, 4, 8)
ahead = 2


def in_vmem():
    return pl.BlockSpec(memory_space=VMEM)


def in_hbm():
    return pl.BlockSpec(memory_space=pltpu.HBM)


def held_in_hbm(*arrays):
    return [pltpu.with_memory_space_constraint(a, pltpu.HBM) for a in arrays]


def params(mib):
    return pltpu.CompilerParams(vmem_limit_bytes=mib * 1024 * 1024)


def attention_kernel(
    lengths_ref,
    queries_hbm,
    fresh_hbm,
    value_new_hbm,
    forget_hbm,
    keys_hbm,
    values_hbm,
    cumlog_hbm,
    out_ref,
    queries_ref,
    fresh_ref,
    value_new_ref,
    forget_ref,
    keys,
    values,
    scores,
    sems,
):
    heads, size = queries_ref.shape
    key_heads, span, _ = keys.shape
    groups = heads // key_heads
    inv_root = size ** (-0.5)
    first = 2 * len(cuts) - 2
    small_copies = [
        pltpu.make_async_copy(source, target, sems.at[first + i])
        for i, (source, target) in enumerate(
            (
                (cumlog_hbm.at[0], scores),
                (queries_hbm.at[0], queries_ref),
                (fresh_hbm.at[0], fresh_ref),
                (forget_hbm, forget_ref),
                (value_new_hbm.at[0], value_new_ref),
            )
        )
    ]

    def pieces(cuts):
        edges = [span * cut // cuts[-1] for cut in cuts]
        return list(zip(edges[:-1], edges[1:]))

    def copies(source, target, cuts, first):
        return [
            pltpu.make_async_copy(
                source.at[0, :, pl.ds(low, high - low), :],
                target.at[:, pl.ds(low, high - low), :],
                sems.at[first + i],
            )
            for i, (low, high) in enumerate(pieces(cuts))
        ]

    key_copies = copies(keys_hbm, keys, cuts, 0)
    value_copies = copies(values_hbm, values, cuts, len(cuts) - 1)
    for copy in small_copies + key_copies + value_copies:
        copy.start()

    def side_by_side(ref, low, high):
        return jnp.concatenate([ref[k, low:high, :] for k in range(key_heads)], axis=1)

    head_rows = lax.broadcasted_iota(jnp.int32, (heads, 1), 0)

    def per_head(ref):
        rows = ref[...].astype(jnp.float32)
        total = jnp.zeros((heads, size), jnp.float32)
        for k in range(key_heads):
            total = jnp.where(head_rows // groups == k, rows[k : k + 1, :], total)
        return total

    for copy in small_copies:
        copy.wait()
    length = lengths_ref[0]
    queries = queries_ref[...]
    wide = jnp.concatenate(
        [
            jnp.where(head_rows // groups == k, queries, jnp.zeros_like(queries))
            for k in range(key_heads)
        ],
        axis=1,
    )
    own_score = (
        jnp.sum(queries.astype(jnp.float32) * per_head(fresh_ref), axis=1, keepdims=True) * inv_root
    )
    logit_row = jnp.broadcast_to(forget_ref[...], (heads, heads))
    diagonal = lax.broadcasted_iota(jnp.int32, (heads, heads), 1) == head_rows
    logit = jnp.sum(jnp.where(diagonal, logit_row, 0.0), axis=1, keepdims=True)
    log_gate = jnp.minimum(logit, 0.0) - jnp.log1p(jnp.exp(-jnp.abs(logit)))
    positions = lax.broadcasted_iota(jnp.int32, (heads, span), 1)
    cumlog = scores[...]
    latest = jnp.sum(jnp.where(positions == length - 1, cumlog, 0.0), axis=1, keepdims=True)
    scores[...] = jnp.where(positions < length, latest + log_gate - cumlog, -jnp.inf)
    parts = pieces(cuts)

    def score(i):
        low, high = parts[i]
        raw = lax.dot_general(
            wide,
            side_by_side(keys, low, high),
            contract_last,
            preferred_element_type=jnp.float32,
        )
        return raw * inv_root + scores[:, low:high]

    def attend_to(weights, i):
        low, high = parts[i]
        return jnp.dot(weights, side_by_side(values, low, high), preferred_element_type=jnp.float32)

    count = len(parts)
    ready = [None] * count
    def fold(state, i):
        top, total, denominator = state
        new_top = jnp.maximum(top, jnp.max(ready[i], axis=1, keepdims=True))
        weights = jnp.exp(ready[i] - new_top)
        added = jnp.sum(weights, axis=1, keepdims=True)
        value_copies[i].wait()
        product = attend_to(weights.astype(jnp.bfloat16), i)
        if total is None:
            return new_top, product, added
        shrink = jnp.exp(top - new_top)
        return new_top, total * shrink + product, denominator * shrink + added

    state = own_score, None, None
    for i in range(count):
        key_copies[i].wait()
        ready[i] = score(i)
        if i >= ahead:
            state = fold(state, i - ahead)
    for i in range(max(count - ahead, 0), count):
        state = fold(state, i)
    top, total, denominator = state
    own_weight = jnp.exp(own_score - top)
    denominator = denominator + own_weight
    mine = own_weight.astype(jnp.bfloat16).astype(jnp.float32) * per_head(value_new_ref)
    for k in range(key_heads):
        mine = mine + jnp.where(
            head_rows // groups == k, total[:, k * size : (k + 1) * size], 0.0
        )
    attended = (mine / denominator).astype(jnp.bfloat16)
    for peer in range(out_ref.shape[0]):
        out_ref[peer] = attended


def attend(queries, fresh_token_key, value_new, forget_logit, cache_keys, cache_values, cache_cumlog, lengths):
    peers = lax.axis_size("ep")
    _, heads, size = queries.shape
    _, key_heads, span, _ = cache_keys.shape
    bf16 = jnp.bfloat16
    return pl.pallas_call(
        attention_kernel,
        out_shape=VMEM((peers, heads, size), bf16),
        in_specs=[pl.BlockSpec(memory_space=pltpu.SMEM)] + [in_hbm()] * 7,
        out_specs=in_vmem(),
        scratch_shapes=[
            VMEM((heads, size), bf16),
            VMEM((key_heads, size), bf16),
            VMEM((key_heads, size), bf16),
            VMEM((1, heads), jnp.float32),
            VMEM((key_heads, span, size), bf16),
            VMEM((key_heads, span, size), bf16),
            VMEM((heads, span), jnp.float32),
            pltpu.SemaphoreType.DMA((2 * len(cuts) + 3,)),
        ],
        compiler_params=params(12),
        name="attention",
    )(
        lengths,
        *held_in_hbm(
            queries,
            fresh_token_key,
            value_new,
            forget_logit,
            cache_keys,
            cache_values,
            cache_cumlog,
        ),
    )


def projection_kernel(rows_ref, weight_ref, residual_ref, out_ref):
    tokens, heads, size = rows_ref.shape
    stacked = rows_ref[...].reshape(tokens * heads, size)
    which = lax.broadcasted_iota(jnp.int32, (tokens * heads, 1), 0) % heads
    wide = jnp.concatenate(
        [jnp.where(which == h, stacked, jnp.zeros_like(stacked)) for h in range(heads)], axis=1
    )
    product = jnp.dot(wide, weight_ref[...], preferred_element_type=jnp.float32)
    mixed = jnp.sum(product.reshape(tokens, heads, product.shape[1]), axis=1)
    stream = (residual_ref[...].astype(jnp.float32) + mixed).astype(jnp.bfloat16)
    for peer in range(out_ref.shape[0]):
        out_ref[peer] = stream


def silu_product(gate, up):
    return gate / (1.0 + jnp.exp(-gate)) * up


def expert_kernel(
    blocks_ref,
    gain_ref,
    routes_ref,
    scores_ref,
    gate_ref,
    up_ref,
    down_ref,
    shared_gate_ref,
    shared_up_ref,
    out_ref,
):
    peers, tokens, width = blocks_ref.shape
    wide = [blocks_ref[p].astype(jnp.float32) for p in range(peers)]
    squares = wide[0] * wide[0]
    for block in wide[1:]:
        squares = squares + block * block
    mean = jnp.sum(squares, axis=1, keepdims=True) / (peers * width)
    inv_rms = lax.rsqrt(mean + norm_eps)
    normed = jnp.concatenate(
        [
            (wide[p] * inv_rms * gain_ref[p : p + 1, :]).astype(jnp.bfloat16)
            for p in range(peers)
        ],
        axis=1,
    )
    scores = scores_ref[...]
    shares = scores / jnp.sum(scores, axis=0, keepdims=True) * routed_scale
    share = jnp.sum(
        jnp.where(routes_ref[...] == lax.axis_index("ep"), shares, 0.0), axis=0, keepdims=True
    )

    def against(matrix):
        return lax.dot_general(matrix, normed, contract_last, preferred_element_type=jnp.float32)

    units = shared_gate_ref.shape[0]
    spread = (
        lax.broadcasted_iota(jnp.int32, (units, width), 0)
        == lax.broadcasted_iota(jnp.int32, (units, width), 1)
    ).astype(jnp.bfloat16)
    contract_first = (((0,), (0,)), ((), ()))
    halves = (against(gate_ref[...]), against(up_ref[...]))
    shared_halves = (against(shared_gate_ref[...]), against(shared_up_ref[...]))
    hidden = (silu_product(*halves) * share).astype(jnp.bfloat16)
    result = lax.dot_general(
        hidden, down_ref[...], contract_first, preferred_element_type=jnp.float32
    ).astype(jnp.bfloat16)
    shared_hidden = silu_product(*shared_halves).astype(jnp.bfloat16)
    shared_rows = lax.dot_general(
        shared_hidden, spread, contract_first, preferred_element_type=jnp.float32
    ).astype(jnp.bfloat16)
    for p in range(peers):
        out_ref[p, :tokens, :] = result[:, p * width : (p + 1) * width]
        out_ref[p, tokens:, :] = shared_rows


def run_experts(
    blocks,
    norm_gain,
    routes,
    route_scores,
    expert_gate,
    expert_up,
    expert_down,
    shared_gate,
    shared_up,
):
    peers, tokens, width = blocks.shape
    bf16 = jnp.bfloat16
    return pl.pallas_call(
        expert_kernel,
        out_shape=VMEM((peers, 2 * tokens, width), bf16),
        in_specs=[in_vmem()] * 9,
        out_specs=in_vmem(),
        compiler_params=params(16),
        name="experts",
    )(
        blocks,
        norm_gain.reshape(peers, width),
        routes.T,
        route_scores.T,
        *(
            pltpu.with_memory_space_constraint(a, VMEM)
            for a in (expert_gate[0], expert_up[0], expert_down[0], shared_gate, shared_up)
        ),
    )


def combine_kernel(received_ref, stream_ref, down_ref, out_ref):
    peers, double, width = received_ref.shape
    tokens = double // 2
    units = down_ref.shape[0] // peers
    total = stream_ref[0].astype(jnp.float32)
    for p in range(peers):
        total = total + received_ref[p, :tokens, :].astype(jnp.float32)
    for p in range(peers):
        total = total + jnp.dot(
            received_ref[p, tokens:, :][:, :units],
            down_ref[p * units : (p + 1) * units, :],
            preferred_element_type=jnp.float32,
        )
    out_ref[...] = total.astype(jnp.bfloat16)


def combine(received, stream, shared_down):
    tokens, width = stream.shape[1:]
    bf16 = jnp.bfloat16
    return pl.pallas_call(
        combine_kernel,
        out_shape=jax.ShapeDtypeStruct((tokens, width), bf16),
        in_specs=[in_vmem()] * 3,
        out_specs=in_vmem(),
        compiler_params=params(4),
        name="combine",
    )(received, stream, shared_down)


def exchange(blocks):
    return lax.all_to_all(blocks, "ep", split_axis=0, concat_axis=0, tiled=True)


def kernel_device(
    queries,
    fresh_token_key,
    value_new,
    forget_logit,
    cache_keys,
    cache_values,
    cache_cumlog,
    lengths,
    residual,
    out_weight,
    norm_gain,
    expert_gate,
    expert_up,
    expert_down,
    shared_gate,
    shared_up,
    shared_down,
    routes,
    route_scores,
):
    peers = lax.axis_size("ep")
    _, heads, size = queries.shape
    _, key_heads, span, _ = cache_keys.shape
    tokens, width = residual.shape
    bf16 = jnp.bfloat16
    spread = attend(
        queries,
        fresh_token_key,
        value_new,
        forget_logit,
        cache_keys,
        cache_values,
        cache_cumlog,
        lengths,
    )
    rows = exchange(spread)
    stream = pl.pallas_call(
        projection_kernel,
        out_shape=VMEM((peers, tokens, width), bf16),
        in_specs=[in_vmem()] * 3,
        out_specs=in_vmem(),
        compiler_params=params(4),
        cost_estimate=pl.CostEstimate(flops=100000000000, bytes_accessed=0, transcendentals=0),
        name="projection",
    )(rows, out_weight, residual)
    blocks = exchange(stream)
    outgoing = run_experts(
        blocks,
        norm_gain,
        routes,
        route_scores,
        expert_gate,
        expert_up,
        expert_down,
        shared_gate,
        shared_up,
    )
    received = exchange(outgoing)
    return combine(received, stream, shared_down)


def on_device(*arrays):
    residual, expert_gate, shared_gate = arrays[8], arrays[11], arrays[14]
    queries, cache_keys = arrays[0], arrays[4]
    fits = (
        residual.shape[1] % 128 == 0
        and residual.shape[0] % 16 == 0
        and shared_gate.shape[0] % 8 == 0
        and shared_gate.shape[0] <= residual.shape[1]
        and expert_gate.shape[0] == 1
        and queries.shape[0] == 1
        and cache_keys.shape[2] % 2048 == 0
    )
    return kernel_device(*arrays) if fits else plain_device(*arrays)


def solution(mesh):
    placed = (
        P(("grp", "ep"), None, None),
        P(("grp", "ep"), None, None),
        P(("grp", "ep"), None, None),
        P(("grp", "ep"), None),
        P(("grp", "ep"), None, None, None),
        P(("grp", "ep"), None, None, None),
        P(("grp", "ep"), None, None),
        P(("grp", "ep")),
        P("grp", "ep"),
        P(None, "ep"),
        P(),
        P("ep", None, None),
        P("ep", None, None),
        P("ep", None, None),
        P("ep", None),
        P("ep", None),
        P(None, "ep"),
        P("grp", None),
        P("grp", None),
    )
    return jax.shard_map(
        on_device, mesh=mesh, in_specs=placed, out_specs=P("grp", "ep"), check_vma=False
    )
```

```python
import jax
import jax.numpy as jnp
from jax import lax
from jax.experimental import pallas as pl
from jax.experimental.pallas import tpu as pltpu
from jax.sharding import PartitionSpec as P

CAP = 12


norm_eps = 1e-06
routed_scale = 2.5
contract_last = (((1,), (1,)), ((), ()))


def expert_hidden(row_block, gate_matrix, up_matrix):
    gate_part = lax.dot_general(
        row_block, gate_matrix, contract_last, preferred_element_type=jnp.float32
    )
    up_part = lax.dot_general(
        row_block, up_matrix, contract_last, preferred_element_type=jnp.float32
    )
    return (jax.nn.silu(gate_part) * up_part).astype(jnp.bfloat16)


def attention(
    queries,
    fresh_token_key,
    value_new,
    forget_logit,
    cache_keys,
    cache_values,
    cache_cumlog,
    lengths,
):
    batch_rows, head_count, head_size = queries.shape
    key_heads = cache_keys.shape[1]
    cache_span = cache_keys.shape[2]
    groups = head_count // key_heads
    inv_root = head_size ** (-0.5)
    grouped_heads = queries.reshape(batch_rows, key_heads, groups, head_size)
    scores = (
        jnp.einsum(
            "bkgd,bkpd->bkgp", grouped_heads, cache_keys, preferred_element_type=jnp.float32
        ).reshape(batch_rows, head_count, cache_span)
        * inv_root
    )
    positions = lax.broadcasted_iota(jnp.int32, (1, 1, cache_span), 2)
    last_pos = (lengths - 1)[:, None, None]
    latest = jnp.sum(jnp.where(positions == last_pos, cache_cumlog, 0.0), axis=2)
    log_gate = jax.nn.log_sigmoid(forget_logit)
    scores = scores + (latest + log_gate)[:, :, None] - cache_cumlog
    visible = positions < lengths[:, None, None]
    scores = jnp.where(visible, scores, -jnp.inf)
    own_score = (
        jnp.einsum(
            "tiuh,tih->tiu", grouped_heads, fresh_token_key, preferred_element_type=jnp.float32
        ).reshape(batch_rows, head_count)
        * inv_root
    )
    top_score = jnp.maximum(jnp.max(scores, axis=2), own_score)
    weights = jnp.where(visible, jnp.exp(scores - top_score[:, :, None]), 0.0)
    own_weight = jnp.exp(own_score - top_score)
    denominator = jnp.sum(weights, axis=2) + own_weight
    weighted = jnp.einsum(
        "bkgp,bkpd->bkgd",
        weights.astype(jnp.bfloat16).reshape(batch_rows, key_heads, groups, cache_span),
        cache_values,
        preferred_element_type=jnp.float32,
    )
    own_rounded = lax.optimization_barrier(own_weight.astype(jnp.bfloat16)).astype(jnp.float32)
    own_value = jnp.repeat(value_new, groups, axis=1).astype(jnp.float32)
    numerator = (
        weighted.reshape(batch_rows, head_count, head_size) + own_rounded[:, :, None] * own_value
    )
    return (
        (numerator / denominator[:, :, None])
        .astype(jnp.bfloat16)
        .reshape(batch_rows, head_count * head_size)
    )


def plain_device(
    queries,
    fresh_token_key,
    value_new,
    forget_logit,
    cache_keys,
    cache_values,
    cache_cumlog,
    lengths,
    residual,
    out_weight,
    norm_gain,
    expert_gate,
    expert_up,
    expert_down,
    shared_gate,
    shared_up,
    shared_down,
    routes,
    route_scores,
):
    attended = attention(
        queries,
        fresh_token_key,
        value_new,
        forget_logit,
        cache_keys,
        cache_values,
        cache_cumlog,
        lengths,
    )
    mixed = jnp.dot(
        lax.all_gather(attended, "ep", axis=0, tiled=True),
        out_weight,
        preferred_element_type=jnp.float32,
    )
    stream = (residual.astype(jnp.float32) + mixed).astype(jnp.bfloat16)
    full_rows = lax.all_gather(stream, "ep", axis=1, tiled=True)
    rows_wide = full_rows.astype(jnp.float32)
    inv_rms = lax.rsqrt(jnp.mean(rows_wide * rows_wide, axis=1, keepdims=True) + norm_eps)
    normed = (rows_wide * inv_rms * norm_gain).astype(jnp.bfloat16)
    gate_weights = route_scores / jnp.sum(route_scores, axis=1, keepdims=True) * routed_scale
    shared_mid = expert_hidden(normed, shared_gate, shared_up)
    my_expert = lax.axis_index("ep")
    expert_hits = routes == my_expert
    is_member = jnp.sum(expert_hits.astype(jnp.int32), axis=1)
    slot_rank = jnp.cumsum(is_member) - 1
    slot_ids = lax.broadcasted_iota(jnp.int32, (CAP, 1), 0)
    selector = (is_member[None, :] == 1) & (slot_rank[None, :] == slot_ids)
    picked = jnp.dot(
        selector.astype(jnp.bfloat16), normed, preferred_element_type=jnp.float32
    ).astype(jnp.bfloat16)
    hidden = expert_hidden(picked, expert_gate[0], expert_up[0])
    expert_out = jnp.dot(hidden, expert_down[0], preferred_element_type=jnp.float32).astype(
        jnp.bfloat16
    )
    received = lax.all_to_all(expert_out[None], "ep", split_axis=2, concat_axis=0, tiled=True)
    expert_count = received.shape[0]
    expert_ids = lax.broadcasted_iota(jnp.int32, (1, 1, expert_count), 2)
    all_hits = routes[:, :, None] == expert_ids
    membership = jnp.sum(all_hits.astype(jnp.int32), axis=1)
    share_all = jnp.sum(jnp.where(all_hits, gate_weights[:, :, None], 0.0), axis=1)
    rank_all = jnp.cumsum(membership, axis=0) - 1
    slot_grid = lax.broadcasted_iota(jnp.int32, (1, 1, CAP), 2)
    slot_mask = (membership[:, :, None] == 1) & (rank_all[:, :, None] == slot_grid)
    combiner = jnp.where(slot_mask, share_all[:, :, None], 0.0).reshape(
        routes.shape[0], expert_count * CAP
    )
    flat_slots = received.reshape(expert_count * CAP, received.shape[2]).astype(jnp.float32)
    routed_part = jnp.dot(combiner, flat_slots, precision=lax.Precision.HIGHEST)
    shared_part = jnp.dot(
        lax.all_gather(shared_mid, "ep", axis=1, tiled=True),
        shared_down,
        preferred_element_type=jnp.float32,
    )
    return (stream.astype(jnp.float32) + routed_part + shared_part).astype(jnp.bfloat16)


VMEM = pltpu.VMEM
cuts = (0, 1, 4, 8)
ahead = 2


def in_vmem():
    return pl.BlockSpec(memory_space=VMEM)


def in_hbm():
    return pl.BlockSpec(memory_space=pltpu.HBM)


def held_in_hbm(*arrays):
    return [pltpu.with_memory_space_constraint(a, pltpu.HBM) for a in arrays]


def params(mib):
    return pltpu.CompilerParams(vmem_limit_bytes=mib * 1024 * 1024)


def attention_kernel(
    lengths_ref,
    queries_hbm,
    fresh_hbm,
    value_new_hbm,
    forget_hbm,
    keys_hbm,
    values_hbm,
    cumlog_hbm,
    out_ref,
    queries_ref,
    fresh_ref,
    value_new_ref,
    forget_ref,
    keys,
    values,
    scores,
    sems,
):
    heads, size = queries_ref.shape
    key_heads, span, _ = keys.shape
    groups = heads // key_heads
    inv_root = size ** (-0.5)
    first = 2 * len(cuts) - 2
    small_copies = [
        pltpu.make_async_copy(source, target, sems.at[first + i])
        for i, (source, target) in enumerate(
            (
                (cumlog_hbm.at[0], scores),
                (queries_hbm.at[0], queries_ref),
                (fresh_hbm.at[0], fresh_ref),
                (forget_hbm, forget_ref),
                (value_new_hbm.at[0], value_new_ref),
            )
        )
    ]

    def pieces(cuts):
        edges = [span * cut // cuts[-1] for cut in cuts]
        return list(zip(edges[:-1], edges[1:]))

    def copies(source, target, cuts, first):
        return [
            pltpu.make_async_copy(
                source.at[0, :, pl.ds(low, high - low), :],
                target.at[:, pl.ds(low, high - low), :],
                sems.at[first + i],
            )
            for i, (low, high) in enumerate(pieces(cuts))
        ]

    key_copies = copies(keys_hbm, keys, cuts, 0)
    value_copies = copies(values_hbm, values, cuts, len(cuts) - 1)
    for copy in small_copies + key_copies + value_copies:
        copy.start()

    def side_by_side(ref, low, high):
        return jnp.concatenate([ref[k, low:high, :] for k in range(key_heads)], axis=1)

    head_rows = lax.broadcasted_iota(jnp.int32, (heads, 1), 0)

    def per_head(ref):
        rows = ref[...].astype(jnp.float32)
        total = jnp.zeros((heads, size), jnp.float32)
        for k in range(key_heads):
            total = jnp.where(head_rows // groups == k, rows[k : k + 1, :], total)
        return total

    for copy in small_copies:
        copy.wait()
    length = lengths_ref[0]
    queries = queries_ref[...]
    wide = jnp.concatenate(
        [
            jnp.where(head_rows // groups == k, queries, jnp.zeros_like(queries))
            for k in range(key_heads)
        ],
        axis=1,
    )
    own_score = (
        jnp.sum(queries.astype(jnp.float32) * per_head(fresh_ref), axis=1, keepdims=True) * inv_root
    )
    logit_row = jnp.broadcast_to(forget_ref[...], (heads, heads))
    diagonal = lax.broadcasted_iota(jnp.int32, (heads, heads), 1) == head_rows
    logit = jnp.sum(jnp.where(diagonal, logit_row, 0.0), axis=1, keepdims=True)
    log_gate = jnp.minimum(logit, 0.0) - jnp.log1p(jnp.exp(-jnp.abs(logit)))
    positions = lax.broadcasted_iota(jnp.int32, (heads, span), 1)
    cumlog = scores[...]
    latest = jnp.sum(jnp.where(positions == length - 1, cumlog, 0.0), axis=1, keepdims=True)
    scores[...] = jnp.where(positions < length, latest + log_gate - cumlog, -jnp.inf)
    parts = pieces(cuts)

    def score(i):
        low, high = parts[i]
        raw = lax.dot_general(
            wide,
            side_by_side(keys, low, high),
            contract_last,
            preferred_element_type=jnp.float32,
        )
        return raw * inv_root + scores[:, low:high]

    def attend_to(weights, i):
        low, high = parts[i]
        return jnp.dot(weights, side_by_side(values, low, high), preferred_element_type=jnp.float32)

    count = len(parts)
    ready = [None] * count

    def fold(state, i):
        top, total, denominator = state
        new_top = jnp.maximum(top, jnp.max(ready[i], axis=1, keepdims=True))
        weights = jnp.exp(ready[i] - new_top)
        added = jnp.sum(weights, axis=1, keepdims=True)
        value_copies[i].wait()
        product = attend_to(weights.astype(jnp.bfloat16), i)
        if total is None:
            return new_top, product, added
        shrink = jnp.exp(top - new_top)
        return new_top, total * shrink + product, denominator * shrink + added

    state = own_score, None, None
    for i in range(count):
        key_copies[i].wait()
        ready[i] = score(i)
        if i >= ahead:
            state = fold(state, i - ahead)
    for i in range(max(count - ahead, 0), count):
        state = fold(state, i)
    top, total, denominator = state
    own_weight = jnp.exp(own_score - top)
    denominator = denominator + own_weight
    mine = own_weight.astype(jnp.bfloat16).astype(jnp.float32) * per_head(value_new_ref)
    for k in range(key_heads):
        mine = mine + jnp.where(
            head_rows // groups == k, total[:, k * size : (k + 1) * size], 0.0
        )
    attended = (mine / denominator).astype(jnp.bfloat16)
    out_ref[...] = attended


def spread_kernel(own_ref, out_ref):
    for peer in range(out_ref.shape[0]):
        out_ref[peer] = own_ref[...]


def attend(queries, fresh_token_key, value_new, forget_logit, cache_keys, cache_values, cache_cumlog, lengths):
    peers = lax.axis_size("ep")
    _, heads, size = queries.shape
    _, key_heads, span, _ = cache_keys.shape
    bf16 = jnp.bfloat16
    own = pl.pallas_call(
        attention_kernel,
        out_shape=VMEM((heads, size), bf16),
        in_specs=[pl.BlockSpec(memory_space=pltpu.SMEM)] + [in_hbm()] * 7,
        out_specs=in_vmem(),
        scratch_shapes=[
            VMEM((heads, size), bf16),
            VMEM((key_heads, size), bf16),
            VMEM((key_heads, size), bf16),
            VMEM((1, heads), jnp.float32),
            VMEM((key_heads, span, size), bf16),
            VMEM((key_heads, span, size), bf16),
            VMEM((heads, span), jnp.float32),
            pltpu.SemaphoreType.DMA((2 * len(cuts) + 3,)),
        ],
        compiler_params=params(12),
        name="attention",
    )(
        lengths,
        *held_in_hbm(
            queries,
            fresh_token_key,
            value_new,
            forget_logit,
            cache_keys,
            cache_values,
            cache_cumlog,
        ),
    )
    return pl.pallas_call(
        spread_kernel,
        out_shape=VMEM((peers, heads, size), bf16),
        in_specs=[in_vmem()],
        out_specs=in_vmem(),
        compiler_params=params(4),
        cost_estimate=pl.CostEstimate(
            flops=100000000000, bytes_accessed=0, transcendentals=0
        ),
        name="spread",
    )(own)


def projection_kernel(rows_ref, weight_ref, residual_ref, out_ref):
    tokens, heads, size = rows_ref.shape
    stacked = rows_ref[...].reshape(tokens * heads, size)
    which = lax.broadcasted_iota(jnp.int32, (tokens * heads, 1), 0) % heads
    wide = jnp.concatenate(
        [jnp.where(which == h, stacked, jnp.zeros_like(stacked)) for h in range(heads)], axis=1
    )
    product = jnp.dot(wide, weight_ref[...], preferred_element_type=jnp.float32)
    mixed = jnp.sum(product.reshape(tokens, heads, product.shape[1]), axis=1)
    stream = (residual_ref[...].astype(jnp.float32) + mixed).astype(jnp.bfloat16)
    for peer in range(out_ref.shape[0]):
        out_ref[peer] = stream


def silu_product(gate, up):
    return gate / (1.0 + jnp.exp(-gate)) * up


def expert_kernel(
    blocks_ref,
    gain_ref,
    routes_ref,
    scores_ref,
    gate_ref,
    up_ref,
    down_ref,
    shared_gate_ref,
    shared_up_ref,
    out_ref,
):
    peers, tokens, width = blocks_ref.shape
    wide = [blocks_ref[p].astype(jnp.float32) for p in range(peers)]
    squares = wide[0] * wide[0]
    for block in wide[1:]:
        squares = squares + block * block
    mean = jnp.sum(squares, axis=1, keepdims=True) / (peers * width)
    inv_rms = lax.rsqrt(mean + norm_eps)
    normed = jnp.concatenate(
        [
            (wide[p] * inv_rms * gain_ref[p : p + 1, :]).astype(jnp.bfloat16)
            for p in range(peers)
        ],
        axis=1,
    )
    scores = scores_ref[...]
    shares = scores / jnp.sum(scores, axis=0, keepdims=True) * routed_scale
    share = jnp.sum(
        jnp.where(routes_ref[...] == lax.axis_index("ep"), shares, 0.0), axis=0, keepdims=True
    )

    def against(matrix):
        return lax.dot_general(matrix, normed, contract_last, preferred_element_type=jnp.float32)

    units = shared_gate_ref.shape[0]
    spread = (
        lax.broadcasted_iota(jnp.int32, (units, width), 0)
        == lax.broadcasted_iota(jnp.int32, (units, width), 1)
    ).astype(jnp.bfloat16)
    contract_first = (((0,), (0,)), ((), ()))
    halves = (against(gate_ref[...]), against(up_ref[...]))
    shared_halves = (against(shared_gate_ref[...]), against(shared_up_ref[...]))
    hidden = (silu_product(*halves) * share).astype(jnp.bfloat16)
    result = lax.dot_general(
        hidden, down_ref[...], contract_first, preferred_element_type=jnp.float32
    ).astype(jnp.bfloat16)
    shared_hidden = silu_product(*shared_halves).astype(jnp.bfloat16)
    shared_rows = lax.dot_general(
        shared_hidden, spread, contract_first, preferred_element_type=jnp.float32
    ).astype(jnp.bfloat16)
    for p in range(peers):
        out_ref[p, :tokens, :] = result[:, p * width : (p + 1) * width]
        out_ref[p, tokens:, :] = shared_rows


def run_experts(
    blocks,
    norm_gain,
    routes,
    route_scores,
    expert_gate,
    expert_up,
    expert_down,
    shared_gate,
    shared_up,
):
    peers, tokens, width = blocks.shape
    bf16 = jnp.bfloat16
    return pl.pallas_call(
        expert_kernel,
        out_shape=VMEM((peers, 2 * tokens, width), bf16),
        in_specs=[in_vmem()] * 9,
        out_specs=in_vmem(),
        compiler_params=params(16),
        name="experts",
    )(
        blocks,
        norm_gain.reshape(peers, width),
        routes.T,
        route_scores.T,
        *(
            pltpu.with_memory_space_constraint(a, VMEM)
            for a in (expert_gate[0], expert_up[0], expert_down[0], shared_gate, shared_up)
        ),
    )


def combine_kernel(received_ref, stream_ref, down_ref, out_ref):
    peers, double, width = received_ref.shape
    tokens = double // 2
    units = down_ref.shape[0] // peers
    total = stream_ref[0].astype(jnp.float32)
    for p in range(peers):
        total = total + received_ref[p, :tokens, :].astype(jnp.float32)
    for p in range(peers):
        total = total + jnp.dot(
            received_ref[p, tokens:, :][:, :units],
            down_ref[p * units : (p + 1) * units, :],
            preferred_element_type=jnp.float32,
        )
    out_ref[...] = total.astype(jnp.bfloat16)


def combine(received, stream, shared_down):
    tokens, width = stream.shape[1:]
    bf16 = jnp.bfloat16
    return pl.pallas_call(
        combine_kernel,
        out_shape=jax.ShapeDtypeStruct((tokens, width), bf16),
        in_specs=[in_vmem()] * 3,
        out_specs=in_vmem(),
        compiler_params=params(4),
        name="combine",
    )(received, stream, shared_down)


def exchange(blocks):
    return lax.all_to_all(blocks, "ep", split_axis=0, concat_axis=0, tiled=True)


def kernel_device(
    queries,
    fresh_token_key,
    value_new,
    forget_logit,
    cache_keys,
    cache_values,
    cache_cumlog,
    lengths,
    residual,
    out_weight,
    norm_gain,
    expert_gate,
    expert_up,
    expert_down,
    shared_gate,
    shared_up,
    shared_down,
    routes,
    route_scores,
):
    peers = lax.axis_size("ep")
    _, heads, size = queries.shape
    _, key_heads, span, _ = cache_keys.shape
    tokens, width = residual.shape
    bf16 = jnp.bfloat16
    spread = attend(
        queries,
        fresh_token_key,
        value_new,
        forget_logit,
        cache_keys,
        cache_values,
        cache_cumlog,
        lengths,
    )
    rows = exchange(spread)
    stream = pl.pallas_call(
        projection_kernel,
        out_shape=VMEM((peers, tokens, width), bf16),
        in_specs=[in_vmem()] * 3,
        out_specs=in_vmem(),
        compiler_params=params(4),
        name="projection",
    )(rows, out_weight, residual)
    blocks = exchange(stream)
    outgoing = run_experts(
        blocks,
        norm_gain,
        routes,
        route_scores,
        expert_gate,
        expert_up,
        expert_down,
        shared_gate,
        shared_up,
    )
    received = exchange(outgoing)
    return combine(received, stream, shared_down)


def on_device(*arrays):
    residual, expert_gate, shared_gate = arrays[8], arrays[11], arrays[14]
    queries, cache_keys = arrays[0], arrays[4]
    fits = (
        residual.shape[1] % 128 == 0
        and residual.shape[0] % 16 == 0
        and shared_gate.shape[0] % 8 == 0
        and shared_gate.shape[0] <= residual.shape[1]
        and expert_gate.shape[0] == 1
        and queries.shape[0] == 1
        and cache_keys.shape[2] % 2048 == 0
    )
    return kernel_device(*arrays) if fits else plain_device(*arrays)


def solution(mesh):
    placed = (
        P(("grp", "ep"), None, None),
        P(("grp", "ep"), None, None),
        P(("grp", "ep"), None, None),
        P(("grp", "ep"), None),
        P(("grp", "ep"), None, None, None),
        P(("grp", "ep"), None, None, None),
        P(("grp", "ep"), None, None),
        P(("grp", "ep")),
        P("grp", "ep"),
        P(None, "ep"),
        P(),
        P("ep", None, None),
        P("ep", None, None),
        P("ep", None, None),
        P("ep", None),
        P("ep", None),
        P(None, "ep"),
        P("grp", None),
        P("grp", None),
    )
    return jax.shard_map(
        on_device, mesh=mesh, in_specs=placed, out_specs=P("grp", "ep"), check_vma=False
    )
```

```python
import jax
import jax.numpy as jnp
from jax import lax
from jax.experimental import pallas as pl
from jax.experimental.pallas import tpu as pltpu
from jax.sharding import PartitionSpec as P

CAP = 12


norm_eps = 1e-06
routed_scale = 2.5
contract_last = (((1,), (1,)), ((), ()))


def expert_hidden(row_block, gate_matrix, up_matrix):
    gate_part = lax.dot_general(
        row_block, gate_matrix, contract_last, preferred_element_type=jnp.float32
    )
    up_part = lax.dot_general(
        row_block, up_matrix, contract_last, preferred_element_type=jnp.float32
    )
    return (jax.nn.silu(gate_part) * up_part).astype(jnp.bfloat16)


def attention(
    queries,
    fresh_token_key,
    value_new,
    forget_logit,
    cache_keys,
    cache_values,
    cache_cumlog,
    lengths,
):
    batch_rows, head_count, head_size = queries.shape
    key_heads = cache_keys.shape[1]
    cache_span = cache_keys.shape[2]
    groups = head_count // key_heads
    inv_root = head_size ** (-0.5)
    grouped_heads = queries.reshape(batch_rows, key_heads, groups, head_size)
    scores = (
        jnp.einsum(
            "bkgd,bkpd->bkgp", grouped_heads, cache_keys, preferred_element_type=jnp.float32
        ).reshape(batch_rows, head_count, cache_span)
        * inv_root
    )
    positions = lax.broadcasted_iota(jnp.int32, (1, 1, cache_span), 2)
    last_pos = (lengths - 1)[:, None, None]
    latest = jnp.sum(jnp.where(positions == last_pos, cache_cumlog, 0.0), axis=2)
    log_gate = jax.nn.log_sigmoid(forget_logit)
    scores = scores + (latest + log_gate)[:, :, None] - cache_cumlog
    visible = positions < lengths[:, None, None]
    scores = jnp.where(visible, scores, -jnp.inf)
    own_score = (
        jnp.einsum(
            "tiuh,tih->tiu", grouped_heads, fresh_token_key, preferred_element_type=jnp.float32
        ).reshape(batch_rows, head_count)
        * inv_root
    )
    top_score = jnp.maximum(jnp.max(scores, axis=2), own_score)
    weights = jnp.where(visible, jnp.exp(scores - top_score[:, :, None]), 0.0)
    own_weight = jnp.exp(own_score - top_score)
    denominator = jnp.sum(weights, axis=2) + own_weight
    weighted = jnp.einsum(
        "bkgp,bkpd->bkgd",
        weights.astype(jnp.bfloat16).reshape(batch_rows, key_heads, groups, cache_span),
        cache_values,
        preferred_element_type=jnp.float32,
    )
    own_rounded = lax.optimization_barrier(own_weight.astype(jnp.bfloat16)).astype(jnp.float32)
    own_value = jnp.repeat(value_new, groups, axis=1).astype(jnp.float32)
    numerator = (
        weighted.reshape(batch_rows, head_count, head_size) + own_rounded[:, :, None] * own_value
    )
    return (
        (numerator / denominator[:, :, None])
        .astype(jnp.bfloat16)
        .reshape(batch_rows, head_count * head_size)
    )


def plain_device(
    queries,
    fresh_token_key,
    value_new,
    forget_logit,
    cache_keys,
    cache_values,
    cache_cumlog,
    lengths,
    residual,
    out_weight,
    norm_gain,
    expert_gate,
    expert_up,
    expert_down,
    shared_gate,
    shared_up,
    shared_down,
    routes,
    route_scores,
):
    attended = attention(
        queries,
        fresh_token_key,
        value_new,
        forget_logit,
        cache_keys,
        cache_values,
        cache_cumlog,
        lengths,
    )
    mixed = jnp.dot(
        lax.all_gather(attended, "ep", axis=0, tiled=True),
        out_weight,
        preferred_element_type=jnp.float32,
    )
    stream = (residual.astype(jnp.float32) + mixed).astype(jnp.bfloat16)
    full_rows = lax.all_gather(stream, "ep", axis=1, tiled=True)
    rows_wide = full_rows.astype(jnp.float32)
    inv_rms = lax.rsqrt(jnp.mean(rows_wide * rows_wide, axis=1, keepdims=True) + norm_eps)
    normed = (rows_wide * inv_rms * norm_gain).astype(jnp.bfloat16)
    gate_weights = route_scores / jnp.sum(route_scores, axis=1, keepdims=True) * routed_scale
    shared_mid = expert_hidden(normed, shared_gate, shared_up)
    my_expert = lax.axis_index("ep")
    expert_hits = routes == my_expert
    is_member = jnp.sum(expert_hits.astype(jnp.int32), axis=1)
    slot_rank = jnp.cumsum(is_member) - 1
    slot_ids = lax.broadcasted_iota(jnp.int32, (CAP, 1), 0)
    selector = (is_member[None, :] == 1) & (slot_rank[None, :] == slot_ids)
    picked = jnp.dot(
        selector.astype(jnp.bfloat16), normed, preferred_element_type=jnp.float32
    ).astype(jnp.bfloat16)
    hidden = expert_hidden(picked, expert_gate[0], expert_up[0])
    expert_out = jnp.dot(hidden, expert_down[0], preferred_element_type=jnp.float32).astype(
        jnp.bfloat16
    )
    received = lax.all_to_all(expert_out[None], "ep", split_axis=2, concat_axis=0, tiled=True)
    expert_count = received.shape[0]
    expert_ids = lax.broadcasted_iota(jnp.int32, (1, 1, expert_count), 2)
    all_hits = routes[:, :, None] == expert_ids
    membership = jnp.sum(all_hits.astype(jnp.int32), axis=1)
    share_all = jnp.sum(jnp.where(all_hits, gate_weights[:, :, None], 0.0), axis=1)
    rank_all = jnp.cumsum(membership, axis=0) - 1
    slot_grid = lax.broadcasted_iota(jnp.int32, (1, 1, CAP), 2)
    slot_mask = (membership[:, :, None] == 1) & (rank_all[:, :, None] == slot_grid)
    combiner = jnp.where(slot_mask, share_all[:, :, None], 0.0).reshape(
        routes.shape[0], expert_count * CAP
    )
    flat_slots = received.reshape(expert_count * CAP, received.shape[2]).astype(jnp.float32)
    routed_part = jnp.dot(combiner, flat_slots, precision=lax.Precision.HIGHEST)
    shared_part = jnp.dot(
        lax.all_gather(shared_mid, "ep", axis=1, tiled=True),
        shared_down,
        preferred_element_type=jnp.float32,
    )
    return (stream.astype(jnp.float32) + routed_part + shared_part).astype(jnp.bfloat16)


VMEM = pltpu.VMEM
cuts = (0, 1, 4, 8)
ahead = 2


def in_vmem():
    return pl.BlockSpec(memory_space=VMEM)


def in_hbm():
    return pl.BlockSpec(memory_space=pltpu.HBM)


def held_in_hbm(*arrays):
    return [pltpu.with_memory_space_constraint(a, pltpu.HBM) for a in arrays]


def params(mib):
    return pltpu.CompilerParams(vmem_limit_bytes=mib * 1024 * 1024)


def attention_kernel(
    lengths_ref,
    queries_hbm,
    fresh_hbm,
    value_new_hbm,
    forget_hbm,
    keys_hbm,
    values_hbm,
    cumlog_hbm,
    out_ref,
    queries_ref,
    fresh_ref,
    value_new_ref,
    forget_ref,
    keys,
    values,
    scores,
    sems,
):
    heads, size = queries_ref.shape
    key_heads, span, _ = keys.shape
    groups = heads // key_heads
    inv_root = size ** (-0.5)
    first = 2 * len(cuts) - 2
    small_copies = [
        pltpu.make_async_copy(source, target, sems.at[first + i])
        for i, (source, target) in enumerate(
            (
                (cumlog_hbm.at[0], scores),
                (queries_hbm.at[0], queries_ref),
                (fresh_hbm.at[0], fresh_ref),
                (forget_hbm, forget_ref),
                (value_new_hbm.at[0], value_new_ref),
            )
        )
    ]

    def pieces(cuts):
        edges = [span * cut // cuts[-1] for cut in cuts]
        return list(zip(edges[:-1], edges[1:]))

    def copies(source, target, cuts, first):
        return [
            pltpu.make_async_copy(
                source.at[0, :, pl.ds(low, high - low), :],
                target.at[:, pl.ds(low, high - low), :],
                sems.at[first + i],
            )
            for i, (low, high) in enumerate(pieces(cuts))
        ]

    key_copies = copies(keys_hbm, keys, cuts, 0)
    value_copies = copies(values_hbm, values, cuts, len(cuts) - 1)
    for copy in small_copies + key_copies + value_copies:
        copy.start()

    def side_by_side(ref, low, high):
        return jnp.concatenate([ref[k, low:high, :] for k in range(key_heads)], axis=1)

    head_rows = lax.broadcasted_iota(jnp.int32, (heads, 1), 0)

    def per_head(ref):
        rows = ref[...].astype(jnp.float32)
        total = jnp.zeros((heads, size), jnp.float32)
        for k in range(key_heads):
            total = jnp.where(head_rows // groups == k, rows[k : k + 1, :], total)
        return total

    for copy in small_copies:
        copy.wait()
    length = lengths_ref[0]
    queries = queries_ref[...]
    wide = jnp.concatenate(
        [
            jnp.where(head_rows // groups == k, queries, jnp.zeros_like(queries))
            for k in range(key_heads)
        ],
        axis=1,
    )
    own_score = (
        jnp.sum(queries.astype(jnp.float32) * per_head(fresh_ref), axis=1, keepdims=True) * inv_root
    )
    logit_row = jnp.broadcast_to(forget_ref[...], (heads, heads))
    diagonal = lax.broadcasted_iota(jnp.int32, (heads, heads), 1) == head_rows
    logit = jnp.sum(jnp.where(diagonal, logit_row, 0.0), axis=1, keepdims=True)
    log_gate = jnp.minimum(logit, 0.0) - jnp.log1p(jnp.exp(-jnp.abs(logit)))
    positions = lax.broadcasted_iota(jnp.int32, (heads, span), 1)
    cumlog = scores[...]
    latest = jnp.sum(jnp.where(positions == length - 1, cumlog, 0.0), axis=1, keepdims=True)
    scores[...] = jnp.where(positions < length, latest + log_gate - cumlog, -jnp.inf)
    parts = pieces(cuts)

    def score(i):
        low, high = parts[i]
        raw = lax.dot_general(
            wide,
            side_by_side(keys, low, high),
            contract_last,
            preferred_element_type=jnp.float32,
        )
        return raw * inv_root + scores[:, low:high]

    def attend_to(weights, i):
        low, high = parts[i]
        return jnp.dot(weights, side_by_side(values, low, high), preferred_element_type=jnp.float32)

    count = len(parts)
    ready = [None] * count

    def fold(state, i):
        top, total, denominator = state
        new_top = jnp.maximum(top, jnp.max(ready[i], axis=1, keepdims=True))
        weights = jnp.exp(ready[i] - new_top)
        added = jnp.sum(weights, axis=1, keepdims=True)
        value_copies[i].wait()
        product = attend_to(weights.astype(jnp.bfloat16), i)
        if total is None:
            return new_top, product, added
        shrink = jnp.exp(top - new_top)
        return new_top, total * shrink + product, denominator * shrink + added

    state = own_score, None, None
    for i in range(count):
        key_copies[i].wait()
        ready[i] = score(i)
        if i >= ahead:
            state = fold(state, i - ahead)
    for i in range(max(count - ahead, 0), count):
        state = fold(state, i)
    top, total, denominator = state
    own_weight = jnp.exp(own_score - top)
    denominator = denominator + own_weight
    mine = own_weight.astype(jnp.bfloat16).astype(jnp.float32) * per_head(value_new_ref)
    for k in range(key_heads):
        mine = mine + jnp.where(
            head_rows // groups == k, total[:, k * size : (k + 1) * size], 0.0
        )
    attended = (mine / denominator).astype(jnp.bfloat16)
    out_ref[...] = attended


def spread_kernel(own_ref, out_ref):
    for peer in range(out_ref.shape[0]):
        out_ref[peer] = own_ref[...]


def attend(queries, fresh_token_key, value_new, forget_logit, cache_keys, cache_values, cache_cumlog, lengths):
    peers = lax.axis_size("ep")
    _, heads, size = queries.shape
    _, key_heads, span, _ = cache_keys.shape
    bf16 = jnp.bfloat16
    own = pl.pallas_call(
        attention_kernel,
        out_shape=VMEM((heads, size), bf16),
        in_specs=[pl.BlockSpec(memory_space=pltpu.SMEM)] + [in_hbm()] * 7,
        out_specs=in_vmem(),
        scratch_shapes=[
            VMEM((heads, size), bf16),
            VMEM((key_heads, size), bf16),
            VMEM((key_heads, size), bf16),
            VMEM((1, heads), jnp.float32),
            VMEM((key_heads, span, size), bf16),
            VMEM((key_heads, span, size), bf16),
            VMEM((heads, span), jnp.float32),
            pltpu.SemaphoreType.DMA((2 * len(cuts) + 3,)),
        ],
        compiler_params=params(12),
        name="attention",
    )(
        lengths,
        *held_in_hbm(
            queries,
            fresh_token_key,
            value_new,
            forget_logit,
            cache_keys,
            cache_values,
            cache_cumlog,
        ),
    )
    return pl.pallas_call(
        spread_kernel,
        out_shape=VMEM((peers, heads, size), bf16),
        in_specs=[in_vmem()],
        out_specs=in_vmem(),
        compiler_params=params(4),
        cost_estimate=pl.CostEstimate(
            flops=100000000000, bytes_accessed=0, transcendentals=0
        ),
        name="spread",
    )(own)


def projection_kernel(rows_ref, weight_ref, residual_ref, out_ref):
    tokens, heads, size = rows_ref.shape
    stacked = rows_ref[...].reshape(tokens * heads, size)
    which = lax.broadcasted_iota(jnp.int32, (tokens * heads, 1), 0) % heads
    wide = jnp.concatenate(
        [jnp.where(which == h, stacked, jnp.zeros_like(stacked)) for h in range(heads)], axis=1
    )
    product = jnp.dot(wide, weight_ref[...], preferred_element_type=jnp.float32)
    mixed = jnp.sum(product.reshape(tokens, heads, product.shape[1]), axis=1)
    stream = (residual_ref[...].astype(jnp.float32) + mixed).astype(jnp.bfloat16)
    for peer in range(out_ref.shape[0]):
        out_ref[peer] = stream


def silu_product(gate, up):
    return gate / (1.0 + jnp.exp(-gate)) * up


def expert_kernel(
    blocks_ref,
    gain_ref,
    routes_ref,
    scores_ref,
    gate_ref,
    up_ref,
    down_ref,
    shared_gate_ref,
    shared_up_ref,
    out_ref,
):
    peers, tokens, width = blocks_ref.shape
    wide = [blocks_ref[p].astype(jnp.float32) for p in range(peers)]
    squares = wide[0] * wide[0]
    for block in wide[1:]:
        squares = squares + block * block
    mean = jnp.sum(squares, axis=1, keepdims=True) / (peers * width)
    inv_rms = lax.rsqrt(mean + norm_eps)
    normed = jnp.concatenate(
        [
            (wide[p] * inv_rms * gain_ref[p : p + 1, :]).astype(jnp.bfloat16)
            for p in range(peers)
        ],
        axis=1,
    )
    scores = scores_ref[...]
    shares = scores / jnp.sum(scores, axis=0, keepdims=True) * routed_scale
    share = jnp.sum(
        jnp.where(routes_ref[...] == lax.axis_index("ep"), shares, 0.0), axis=0, keepdims=True
    )

    def against(matrix):
        return lax.dot_general(matrix, normed, contract_last, preferred_element_type=jnp.float32)

    units = shared_gate_ref.shape[0]
    spread = (
        lax.broadcasted_iota(jnp.int32, (units, width), 0)
        == lax.broadcasted_iota(jnp.int32, (units, width), 1)
    ).astype(jnp.bfloat16)
    contract_first = (((0,), (0,)), ((), ()))
    halves = (against(gate_ref[...]), against(up_ref[...]))
    shared_halves = (against(shared_gate_ref[...]), against(shared_up_ref[...]))
    hidden = (silu_product(*halves) * share).astype(jnp.bfloat16)
    result = lax.dot_general(
        hidden, down_ref[...], contract_first, preferred_element_type=jnp.float32
    ).astype(jnp.bfloat16)
    shared_hidden = silu_product(*shared_halves).astype(jnp.bfloat16)
    shared_rows = lax.dot_general(
        shared_hidden, spread, contract_first, preferred_element_type=jnp.float32
    ).astype(jnp.bfloat16)
    for p in range(peers):
        out_ref[p, :tokens, :] = result[:, p * width : (p + 1) * width]
        out_ref[p, tokens:, :] = shared_rows


def run_experts(
    blocks,
    norm_gain,
    routes,
    route_scores,
    expert_gate,
    expert_up,
    expert_down,
    shared_gate,
    shared_up,
):
    peers, tokens, width = blocks.shape
    bf16 = jnp.bfloat16
    return pl.pallas_call(
        expert_kernel,
        out_shape=VMEM((peers, 2 * tokens, width), bf16),
        in_specs=[in_vmem()] * 9,
        out_specs=in_vmem(),
        compiler_params=params(16),
        name="experts",
    )(
        blocks,
        norm_gain.reshape(peers, width),
        routes.T,
        route_scores.T,
        *(
            pltpu.with_memory_space_constraint(a, VMEM)
            for a in (expert_gate[0], expert_up[0], expert_down[0], shared_gate, shared_up)
        ),
    )


def combine_kernel(received_ref, stream_ref, down_ref, out_ref):
    peers, double, width = received_ref.shape
    tokens = double // 2
    units = down_ref.shape[0] // peers
    total = stream_ref[0].astype(jnp.float32)
    for p in range(peers):
        total = total + received_ref[p, :tokens, :].astype(jnp.float32)
    for p in range(peers):
        total = total + jnp.dot(
            received_ref[p, tokens:, :][:, :units],
            down_ref[p * units : (p + 1) * units, :],
            preferred_element_type=jnp.float32,
        )
    out_ref[...] = total.astype(jnp.bfloat16)


def combine(received, stream, shared_down):
    tokens, width = stream.shape[1:]
    bf16 = jnp.bfloat16
    return pl.pallas_call(
        combine_kernel,
        out_shape=jax.ShapeDtypeStruct((tokens, width), bf16),
        in_specs=[in_vmem()] * 3,
        out_specs=in_vmem(),
        compiler_params=params(4),
        name="combine",
    )(received, stream, shared_down)


def exchange(blocks):
    return lax.all_to_all(blocks, "ep", split_axis=0, concat_axis=0, tiled=True)


def kernel_device(
    queries,
    fresh_token_key,
    value_new,
    forget_logit,
    cache_keys,
    cache_values,
    cache_cumlog,
    lengths,
    residual,
    out_weight,
    norm_gain,
    expert_gate,
    expert_up,
    expert_down,
    shared_gate,
    shared_up,
    shared_down,
    routes,
    route_scores,
):
    peers = lax.axis_size("ep")
    _, heads, size = queries.shape
    _, key_heads, span, _ = cache_keys.shape
    tokens, width = residual.shape
    bf16 = jnp.bfloat16
    spread = attend(
        queries,
        fresh_token_key,
        value_new,
        forget_logit,
        cache_keys,
        cache_values,
        cache_cumlog,
        lengths,
    )
    rows = exchange(spread)
    stream = pl.pallas_call(
        projection_kernel,
        out_shape=VMEM((peers, tokens, width), bf16),
        in_specs=[in_vmem()] * 3,
        out_specs=in_vmem(),
        compiler_params=params(4),
        cost_estimate=pl.CostEstimate(
            flops=2000000000, bytes_accessed=0, transcendentals=0
        ),
        name="projection",
    )(rows, out_weight, residual)
    blocks = exchange(stream)
    outgoing = run_experts(
        blocks,
        norm_gain,
        routes,
        route_scores,
        expert_gate,
        expert_up,
        expert_down,
        shared_gate,
        shared_up,
    )
    received = exchange(outgoing)
    return combine(received, stream, shared_down)


def on_device(*arrays):
    residual, expert_gate, shared_gate = arrays[8], arrays[11], arrays[14]
    queries, cache_keys = arrays[0], arrays[4]
    fits = (
        residual.shape[1] % 128 == 0
        and residual.shape[0] % 16 == 0
        and shared_gate.shape[0] % 8 == 0
        and shared_gate.shape[0] <= residual.shape[1]
        and expert_gate.shape[0] == 1
        and queries.shape[0] == 1
        and cache_keys.shape[2] % 2048 == 0
    )
    return kernel_device(*arrays) if fits else plain_device(*arrays)


def solution(mesh):
    placed = (
        P(("grp", "ep"), None, None),
        P(("grp", "ep"), None, None),
        P(("grp", "ep"), None, None),
        P(("grp", "ep"), None),
        P(("grp", "ep"), None, None, None),
        P(("grp", "ep"), None, None, None),
        P(("grp", "ep"), None, None),
        P(("grp", "ep")),
        P("grp", "ep"),
        P(None, "ep"),
        P(),
        P("ep", None, None),
        P("ep", None, None),
        P("ep", None, None),
        P("ep", None),
        P("ep", None),
        P(None, "ep"),
        P("grp", None),
        P("grp", None),
    )
    return jax.shard_map(
        on_device, mesh=mesh, in_specs=placed, out_specs=P("grp", "ep"), check_vma=False
    )
```

```python
import jax
import jax.numpy as jnp
from jax import lax
from jax.experimental import pallas as pl
from jax.experimental.pallas import tpu as pltpu
from jax.sharding import PartitionSpec as P

CAP = 12


norm_eps = 1e-06
routed_scale = 2.5
contract_last = (((1,), (1,)), ((), ()))


def expert_hidden(row_block, gate_matrix, up_matrix):
    gate_part = lax.dot_general(
        row_block, gate_matrix, contract_last, preferred_element_type=jnp.float32
    )
    up_part = lax.dot_general(
        row_block, up_matrix, contract_last, preferred_element_type=jnp.float32
    )
    return (jax.nn.silu(gate_part) * up_part).astype(jnp.bfloat16)


def attention(
    queries,
    fresh_token_key,
    value_new,
    forget_logit,
    cache_keys,
    cache_values,
    cache_cumlog,
    lengths,
):
    batch_rows, head_count, head_size = queries.shape
    key_heads = cache_keys.shape[1]
    cache_span = cache_keys.shape[2]
    groups = head_count // key_heads
    inv_root = head_size ** (-0.5)
    grouped_heads = queries.reshape(batch_rows, key_heads, groups, head_size)
    scores = (
        jnp.einsum(
            "bkgd,bkpd->bkgp", grouped_heads, cache_keys, preferred_element_type=jnp.float32
        ).reshape(batch_rows, head_count, cache_span)
        * inv_root
    )
    positions = lax.broadcasted_iota(jnp.int32, (1, 1, cache_span), 2)
    last_pos = (lengths - 1)[:, None, None]
    latest = jnp.sum(jnp.where(positions == last_pos, cache_cumlog, 0.0), axis=2)
    log_gate = jax.nn.log_sigmoid(forget_logit)
    scores = scores + (latest + log_gate)[:, :, None] - cache_cumlog
    visible = positions < lengths[:, None, None]
    scores = jnp.where(visible, scores, -jnp.inf)
    own_score = (
        jnp.einsum(
            "tiuh,tih->tiu", grouped_heads, fresh_token_key, preferred_element_type=jnp.float32
        ).reshape(batch_rows, head_count)
        * inv_root
    )
    top_score = jnp.maximum(jnp.max(scores, axis=2), own_score)
    weights = jnp.where(visible, jnp.exp(scores - top_score[:, :, None]), 0.0)
    own_weight = jnp.exp(own_score - top_score)
    denominator = jnp.sum(weights, axis=2) + own_weight
    weighted = jnp.einsum(
        "bkgp,bkpd->bkgd",
        weights.astype(jnp.bfloat16).reshape(batch_rows, key_heads, groups, cache_span),
        cache_values,
        preferred_element_type=jnp.float32,
    )
    own_rounded = lax.optimization_barrier(own_weight.astype(jnp.bfloat16)).astype(jnp.float32)
    own_value = jnp.repeat(value_new, groups, axis=1).astype(jnp.float32)
    numerator = (
        weighted.reshape(batch_rows, head_count, head_size) + own_rounded[:, :, None] * own_value
    )
    return (
        (numerator / denominator[:, :, None])
        .astype(jnp.bfloat16)
        .reshape(batch_rows, head_count * head_size)
    )


def plain_device(
    queries,
    fresh_token_key,
    value_new,
    forget_logit,
    cache_keys,
    cache_values,
    cache_cumlog,
    lengths,
    residual,
    out_weight,
    norm_gain,
    expert_gate,
    expert_up,
    expert_down,
    shared_gate,
    shared_up,
    shared_down,
    routes,
    route_scores,
):
    attended = attention(
        queries,
        fresh_token_key,
        value_new,
        forget_logit,
        cache_keys,
        cache_values,
        cache_cumlog,
        lengths,
    )
    mixed = jnp.dot(
        lax.all_gather(attended, "ep", axis=0, tiled=True),
        out_weight,
        preferred_element_type=jnp.float32,
    )
    stream = (residual.astype(jnp.float32) + mixed).astype(jnp.bfloat16)
    full_rows = lax.all_gather(stream, "ep", axis=1, tiled=True)
    rows_wide = full_rows.astype(jnp.float32)
    inv_rms = lax.rsqrt(jnp.mean(rows_wide * rows_wide, axis=1, keepdims=True) + norm_eps)
    normed = (rows_wide * inv_rms * norm_gain).astype(jnp.bfloat16)
    gate_weights = route_scores / jnp.sum(route_scores, axis=1, keepdims=True) * routed_scale
    shared_mid = expert_hidden(normed, shared_gate, shared_up)
    my_expert = lax.axis_index("ep")
    expert_hits = routes == my_expert
    is_member = jnp.sum(expert_hits.astype(jnp.int32), axis=1)
    slot_rank = jnp.cumsum(is_member) - 1
    slot_ids = lax.broadcasted_iota(jnp.int32, (CAP, 1), 0)
    selector = (is_member[None, :] == 1) & (slot_rank[None, :] == slot_ids)
    picked = jnp.dot(
        selector.astype(jnp.bfloat16), normed, preferred_element_type=jnp.float32
    ).astype(jnp.bfloat16)
    hidden = expert_hidden(picked, expert_gate[0], expert_up[0])
    expert_out = jnp.dot(hidden, expert_down[0], preferred_element_type=jnp.float32).astype(
        jnp.bfloat16
    )
    received = lax.all_to_all(expert_out[None], "ep", split_axis=2, concat_axis=0, tiled=True)
    expert_count = received.shape[0]
    expert_ids = lax.broadcasted_iota(jnp.int32, (1, 1, expert_count), 2)
    all_hits = routes[:, :, None] == expert_ids
    membership = jnp.sum(all_hits.astype(jnp.int32), axis=1)
    share_all = jnp.sum(jnp.where(all_hits, gate_weights[:, :, None], 0.0), axis=1)
    rank_all = jnp.cumsum(membership, axis=0) - 1
    slot_grid = lax.broadcasted_iota(jnp.int32, (1, 1, CAP), 2)
    slot_mask = (membership[:, :, None] == 1) & (rank_all[:, :, None] == slot_grid)
    combiner = jnp.where(slot_mask, share_all[:, :, None], 0.0).reshape(
        routes.shape[0], expert_count * CAP
    )
    flat_slots = received.reshape(expert_count * CAP, received.shape[2]).astype(jnp.float32)
    routed_part = jnp.dot(combiner, flat_slots, precision=lax.Precision.HIGHEST)
    shared_part = jnp.dot(
        lax.all_gather(shared_mid, "ep", axis=1, tiled=True),
        shared_down,
        preferred_element_type=jnp.float32,
    )
    return (stream.astype(jnp.float32) + routed_part + shared_part).astype(jnp.bfloat16)


VMEM = pltpu.VMEM
cuts = (0, 1, 4, 8)
ahead = 2
unit_step = 256


def in_vmem():
    return pl.BlockSpec(memory_space=VMEM)


def in_hbm():
    return pl.BlockSpec(memory_space=pltpu.HBM)


def held_in_hbm(*arrays):
    return [pltpu.with_memory_space_constraint(a, pltpu.HBM) for a in arrays]


def params(mib):
    return pltpu.CompilerParams(vmem_limit_bytes=mib * 1024 * 1024)


def attention_kernel(
    lengths_ref,
    queries_hbm,
    fresh_hbm,
    value_new_hbm,
    forget_hbm,
    keys_hbm,
    values_hbm,
    cumlog_hbm,
    out_ref,
    queries_ref,
    fresh_ref,
    value_new_ref,
    forget_ref,
    keys,
    values,
    scores,
    sems,
):
    heads, size = queries_ref.shape
    key_heads, span, _ = keys.shape
    groups = heads // key_heads
    inv_root = size ** (-0.5)
    first = 2 * len(cuts) - 2
    small_copies = [
        pltpu.make_async_copy(source, target, sems.at[first + i])
        for i, (source, target) in enumerate(
            (
                (cumlog_hbm.at[0], scores),
                (queries_hbm.at[0], queries_ref),
                (fresh_hbm.at[0], fresh_ref),
                (forget_hbm, forget_ref),
                (value_new_hbm.at[0], value_new_ref),
            )
        )
    ]

    def pieces(cuts):
        edges = [span * cut // cuts[-1] for cut in cuts]
        return list(zip(edges[:-1], edges[1:]))

    def copies(source, target, cuts, first):
        return [
            pltpu.make_async_copy(
                source.at[0, :, pl.ds(low, high - low), :],
                target.at[:, pl.ds(low, high - low), :],
                sems.at[first + i],
            )
            for i, (low, high) in enumerate(pieces(cuts))
        ]

    key_copies = copies(keys_hbm, keys, cuts, 0)
    value_copies = copies(values_hbm, values, cuts, len(cuts) - 1)
    for copy in small_copies + key_copies + value_copies:
        copy.start()

    def side_by_side(ref, low, high):
        return jnp.concatenate([ref[k, low:high, :] for k in range(key_heads)], axis=1)

    head_rows = lax.broadcasted_iota(jnp.int32, (heads, 1), 0)

    def per_head(ref):
        rows = ref[...].astype(jnp.float32)
        total = jnp.zeros((heads, size), jnp.float32)
        for k in range(key_heads):
            total = jnp.where(head_rows // groups == k, rows[k : k + 1, :], total)
        return total

    for copy in small_copies:
        copy.wait()
    length = lengths_ref[0]
    queries = queries_ref[...]
    wide = jnp.concatenate(
        [
            jnp.where(head_rows // groups == k, queries, jnp.zeros_like(queries))
            for k in range(key_heads)
        ],
        axis=1,
    )
    own_score = (
        jnp.sum(queries.astype(jnp.float32) * per_head(fresh_ref), axis=1, keepdims=True) * inv_root
    )
    logit_row = jnp.broadcast_to(forget_ref[...], (heads, heads))
    diagonal = lax.broadcasted_iota(jnp.int32, (heads, heads), 1) == head_rows
    logit = jnp.sum(jnp.where(diagonal, logit_row, 0.0), axis=1, keepdims=True)
    log_gate = jnp.minimum(logit, 0.0) - jnp.log1p(jnp.exp(-jnp.abs(logit)))
    positions = lax.broadcasted_iota(jnp.int32, (heads, span), 1)
    cumlog = scores[...]
    latest = jnp.sum(jnp.where(positions == length - 1, cumlog, 0.0), axis=1, keepdims=True)
    scores[...] = jnp.where(positions < length, latest + log_gate - cumlog, -jnp.inf)
    parts = pieces(cuts)

    def score(i):
        low, high = parts[i]
        raw = lax.dot_general(
            wide,
            side_by_side(keys, low, high),
            contract_last,
            preferred_element_type=jnp.float32,
        )
        return raw * inv_root + scores[:, low:high]

    def attend_to(weights, i):
        low, high = parts[i]
        return jnp.dot(weights, side_by_side(values, low, high), preferred_element_type=jnp.float32)

    count = len(parts)
    ready = [None] * count

    def fold(state, i):
        top, total, denominator = state
        new_top = jnp.maximum(top, jnp.max(ready[i], axis=1, keepdims=True))
        weights = jnp.exp(ready[i] - new_top)
        added = jnp.sum(weights, axis=1, keepdims=True)
        value_copies[i].wait()
        product = attend_to(weights.astype(jnp.bfloat16), i)
        if total is None:
            return new_top, product, added
        shrink = jnp.exp(top - new_top)
        return new_top, total * shrink + product, denominator * shrink + added

    state = own_score, None, None
    for i in range(count):
        key_copies[i].wait()
        ready[i] = score(i)
        if i >= ahead:
            state = fold(state, i - ahead)
    for i in range(max(count - ahead, 0), count):
        state = fold(state, i)
    top, total, denominator = state
    own_weight = jnp.exp(own_score - top)
    denominator = denominator + own_weight
    mine = own_weight.astype(jnp.bfloat16).astype(jnp.float32) * per_head(value_new_ref)
    for k in range(key_heads):
        mine = mine + jnp.where(
            head_rows // groups == k, total[:, k * size : (k + 1) * size], 0.0
        )
    attended = (mine / denominator).astype(jnp.bfloat16)
    out_ref[...] = attended


def spread_kernel(own_ref, out_ref):
    for peer in range(out_ref.shape[0]):
        out_ref[peer] = own_ref[...]


def attend(queries, fresh_token_key, value_new, forget_logit, cache_keys, cache_values, cache_cumlog, lengths):
    peers = lax.axis_size("ep")
    _, heads, size = queries.shape
    _, key_heads, span, _ = cache_keys.shape
    bf16 = jnp.bfloat16
    own = pl.pallas_call(
        attention_kernel,
        out_shape=VMEM((heads, size), bf16),
        in_specs=[pl.BlockSpec(memory_space=pltpu.SMEM)] + [in_hbm()] * 7,
        out_specs=in_vmem(),
        scratch_shapes=[
            VMEM((heads, size), bf16),
            VMEM((key_heads, size), bf16),
            VMEM((key_heads, size), bf16),
            VMEM((1, heads), jnp.float32),
            VMEM((key_heads, span, size), bf16),
            VMEM((key_heads, span, size), bf16),
            VMEM((heads, span), jnp.float32),
            pltpu.SemaphoreType.DMA((2 * len(cuts) + 3,)),
        ],
        compiler_params=params(12),
        name="attention",
    )(
        lengths,
        *held_in_hbm(
            queries,
            fresh_token_key,
            value_new,
            forget_logit,
            cache_keys,
            cache_values,
            cache_cumlog,
        ),
    )
    return pl.pallas_call(
        spread_kernel,
        out_shape=VMEM((peers, heads, size), bf16),
        in_specs=[in_vmem()],
        out_specs=in_vmem(),
        compiler_params=params(4),
        cost_estimate=pl.CostEstimate(
            flops=100000000000, bytes_accessed=0, transcendentals=0
        ),
        name="spread",
    )(own)


def projection_kernel(rows_ref, weight_ref, residual_ref, out_ref):
    tokens, heads, size = rows_ref.shape
    stacked = rows_ref[...].reshape(tokens * heads, size)
    which = lax.broadcasted_iota(jnp.int32, (tokens * heads, 1), 0) % heads
    wide = jnp.concatenate(
        [jnp.where(which == h, stacked, jnp.zeros_like(stacked)) for h in range(heads)], axis=1
    )
    product = jnp.dot(wide, weight_ref[...], preferred_element_type=jnp.float32)
    mixed = jnp.sum(product.reshape(tokens, heads, product.shape[1]), axis=1)
    stream = (residual_ref[...].astype(jnp.float32) + mixed).astype(jnp.bfloat16)
    for peer in range(out_ref.shape[0]):
        out_ref[peer] = stream


def silu_product(gate, up):
    return gate / (1.0 + jnp.exp(-gate)) * up


def expert_kernel(
    blocks_ref,
    gain_ref,
    routes_ref,
    scores_ref,
    gate_ref,
    up_ref,
    down_ref,
    shared_gate_ref,
    shared_up_ref,
    out_ref,
):
    peers, tokens, width = blocks_ref.shape
    wide = [blocks_ref[p].astype(jnp.float32) for p in range(peers)]
    squares = wide[0] * wide[0]
    for block in wide[1:]:
        squares = squares + block * block
    mean = jnp.sum(squares, axis=1, keepdims=True) / (peers * width)
    inv_rms = lax.rsqrt(mean + norm_eps)
    normed = jnp.concatenate(
        [
            (wide[p] * inv_rms * gain_ref[p : p + 1, :]).astype(jnp.bfloat16)
            for p in range(peers)
        ],
        axis=1,
    )
    scores = scores_ref[...]
    shares = scores / jnp.sum(scores, axis=0, keepdims=True) * routed_scale
    share = jnp.sum(
        jnp.where(routes_ref[...] == lax.axis_index("ep"), shares, 0.0), axis=0, keepdims=True
    )

    def against(matrix):
        return lax.dot_general(matrix, normed, contract_last, preferred_element_type=jnp.float32)


    tokens_eye = (
        lax.broadcasted_iota(jnp.int32, (tokens, tokens), 0)
        == lax.broadcasted_iota(jnp.int32, (tokens, tokens), 1)
    )
    share = jnp.sum(
        jnp.where(tokens_eye, jnp.broadcast_to(share, (tokens, tokens)), 0.0),
        axis=1,
        keepdims=True,
    )

    def across(matrix):
        return lax.dot_general(normed, matrix, contract_last, preferred_element_type=jnp.float32)

    total = gate_ref.shape[0]
    edges = list(range(0, total, unit_step)) + [total]
    pairs = []
    for low, high in zip(edges[:-1], edges[1:]):
        pairs.append((against(gate_ref[low:high, :]), across(up_ref[low:high, :])))
    shared_g = against(shared_gate_ref[...]).T
    shared_u = across(shared_up_ref[...])

    hidden = jnp.concatenate([(silu_product(g.T, u) * share).astype(jnp.bfloat16) for g, u in pairs], axis=1)
    result = jnp.dot(hidden, down_ref[...], preferred_element_type=jnp.float32).astype(jnp.bfloat16)
    shared_hidden = silu_product(shared_g, shared_u).astype(jnp.bfloat16)
    units = shared_hidden.shape[1]
    shared_rows = jnp.concatenate(
        [shared_hidden, jnp.zeros((tokens, width - units), jnp.bfloat16)], axis=1
    )
    for p in range(peers):
        out_ref[p, :tokens, :] = result[:, p * width : (p + 1) * width]
        out_ref[p, tokens:, :] = shared_rows


def run_experts(
    blocks,
    norm_gain,
    routes,
    route_scores,
    expert_gate,
    expert_up,
    expert_down,
    shared_gate,
    shared_up,
):
    peers, tokens, width = blocks.shape
    bf16 = jnp.bfloat16
    return pl.pallas_call(
        expert_kernel,
        out_shape=VMEM((peers, 2 * tokens, width), bf16),
        in_specs=[in_vmem()] * 9,
        out_specs=in_vmem(),
        compiler_params=params(16),
        name="experts",
    )(
        blocks,
        norm_gain.reshape(peers, width),
        routes.T,
        route_scores.T,
        *(
            pltpu.with_memory_space_constraint(a, VMEM)
            for a in (expert_gate[0], expert_up[0], expert_down[0], shared_gate, shared_up)
        ),
    )


def combine_kernel(received_ref, stream_ref, down_ref, out_ref):
    peers, double, width = received_ref.shape
    tokens = double // 2
    units = down_ref.shape[0] // peers
    total = stream_ref[0].astype(jnp.float32)
    for p in range(peers):
        total = total + received_ref[p, :tokens, :].astype(jnp.float32)
    for p in range(peers):
        total = total + jnp.dot(
            received_ref[p, tokens:, :][:, :units],
            down_ref[p * units : (p + 1) * units, :],
            preferred_element_type=jnp.float32,
        )
    out_ref[...] = total.astype(jnp.bfloat16)


def combine(received, stream, shared_down):
    tokens, width = stream.shape[1:]
    bf16 = jnp.bfloat16
    return pl.pallas_call(
        combine_kernel,
        out_shape=jax.ShapeDtypeStruct((tokens, width), bf16),
        in_specs=[in_vmem()] * 3,
        out_specs=in_vmem(),
        compiler_params=params(4),
        name="combine",
    )(received, stream, shared_down)


def exchange(blocks):
    return lax.all_to_all(blocks, "ep", split_axis=0, concat_axis=0, tiled=True)


def kernel_device(
    queries,
    fresh_token_key,
    value_new,
    forget_logit,
    cache_keys,
    cache_values,
    cache_cumlog,
    lengths,
    residual,
    out_weight,
    norm_gain,
    expert_gate,
    expert_up,
    expert_down,
    shared_gate,
    shared_up,
    shared_down,
    routes,
    route_scores,
):
    peers = lax.axis_size("ep")
    _, heads, size = queries.shape
    _, key_heads, span, _ = cache_keys.shape
    tokens, width = residual.shape
    bf16 = jnp.bfloat16
    spread = attend(
        queries,
        fresh_token_key,
        value_new,
        forget_logit,
        cache_keys,
        cache_values,
        cache_cumlog,
        lengths,
    )
    rows = exchange(spread)
    stream = pl.pallas_call(
        projection_kernel,
        out_shape=VMEM((peers, tokens, width), bf16),
        in_specs=[in_vmem()] * 3,
        out_specs=in_vmem(),
        compiler_params=params(4),
        name="projection",
    )(rows, out_weight, residual)
    blocks = exchange(stream)
    outgoing = run_experts(
        blocks,
        norm_gain,
        routes,
        route_scores,
        expert_gate,
        expert_up,
        expert_down,
        shared_gate,
        shared_up,
    )
    received = exchange(outgoing)
    return combine(received, stream, shared_down)


def on_device(*arrays):
    residual, expert_gate, shared_gate = arrays[8], arrays[11], arrays[14]
    queries, cache_keys = arrays[0], arrays[4]
    fits = (
        residual.shape[1] % 128 == 0
        and residual.shape[0] % 16 == 0
        and shared_gate.shape[0] % 8 == 0
        and shared_gate.shape[0] <= residual.shape[1]
        and expert_gate.shape[0] == 1
        and queries.shape[0] == 1
        and cache_keys.shape[2] % 2048 == 0
    )
    return kernel_device(*arrays) if fits else plain_device(*arrays)


def solution(mesh):
    placed = (
        P(("grp", "ep"), None, None),
        P(("grp", "ep"), None, None),
        P(("grp", "ep"), None, None),
        P(("grp", "ep"), None),
        P(("grp", "ep"), None, None, None),
        P(("grp", "ep"), None, None, None),
        P(("grp", "ep"), None, None),
        P(("grp", "ep")),
        P("grp", "ep"),
        P(None, "ep"),
        P(),
        P("ep", None, None),
        P("ep", None, None),
        P("ep", None, None),
        P("ep", None),
        P("ep", None),
        P(None, "ep"),
        P("grp", None),
        P("grp", None),
    )
    return jax.shard_map(
        on_device, mesh=mesh, in_specs=placed, out_specs=P("grp", "ep"), check_vma=False
    )
```

```python
import jax
import jax.numpy as jnp
from jax import lax
from jax.experimental import pallas as pl
from jax.experimental.pallas import tpu as pltpu
from jax.sharding import PartitionSpec as P

CAP = 12


norm_eps = 1e-06
routed_scale = 2.5
contract_last = (((1,), (1,)), ((), ()))


def expert_hidden(row_block, gate_matrix, up_matrix):
    gate_part = lax.dot_general(
        row_block, gate_matrix, contract_last, preferred_element_type=jnp.float32
    )
    up_part = lax.dot_general(
        row_block, up_matrix, contract_last, preferred_element_type=jnp.float32
    )
    return (jax.nn.silu(gate_part) * up_part).astype(jnp.bfloat16)


def attention(
    queries,
    fresh_token_key,
    value_new,
    forget_logit,
    cache_keys,
    cache_values,
    cache_cumlog,
    lengths,
):
    batch_rows, head_count, head_size = queries.shape
    key_heads = cache_keys.shape[1]
    cache_span = cache_keys.shape[2]
    groups = head_count // key_heads
    inv_root = head_size ** (-0.5)
    grouped_heads = queries.reshape(batch_rows, key_heads, groups, head_size)
    scores = (
        jnp.einsum(
            "bkgd,bkpd->bkgp", grouped_heads, cache_keys, preferred_element_type=jnp.float32
        ).reshape(batch_rows, head_count, cache_span)
        * inv_root
    )
    positions = lax.broadcasted_iota(jnp.int32, (1, 1, cache_span), 2)
    last_pos = (lengths - 1)[:, None, None]
    latest = jnp.sum(jnp.where(positions == last_pos, cache_cumlog, 0.0), axis=2)
    log_gate = jax.nn.log_sigmoid(forget_logit)
    scores = scores + (latest + log_gate)[:, :, None] - cache_cumlog
    visible = positions < lengths[:, None, None]
    scores = jnp.where(visible, scores, -jnp.inf)
    own_score = (
        jnp.einsum(
            "tiuh,tih->tiu", grouped_heads, fresh_token_key, preferred_element_type=jnp.float32
        ).reshape(batch_rows, head_count)
        * inv_root
    )
    top_score = jnp.maximum(jnp.max(scores, axis=2), own_score)
    weights = jnp.where(visible, jnp.exp(scores - top_score[:, :, None]), 0.0)
    own_weight = jnp.exp(own_score - top_score)
    denominator = jnp.sum(weights, axis=2) + own_weight
    weighted = jnp.einsum(
        "bkgp,bkpd->bkgd",
        weights.astype(jnp.bfloat16).reshape(batch_rows, key_heads, groups, cache_span),
        cache_values,
        preferred_element_type=jnp.float32,
    )
    own_rounded = lax.optimization_barrier(own_weight.astype(jnp.bfloat16)).astype(jnp.float32)
    own_value = jnp.repeat(value_new, groups, axis=1).astype(jnp.float32)
    numerator = (
        weighted.reshape(batch_rows, head_count, head_size) + own_rounded[:, :, None] * own_value
    )
    return (
        (numerator / denominator[:, :, None])
        .astype(jnp.bfloat16)
        .reshape(batch_rows, head_count * head_size)
    )


def plain_device(
    queries,
    fresh_token_key,
    value_new,
    forget_logit,
    cache_keys,
    cache_values,
    cache_cumlog,
    lengths,
    residual,
    out_weight,
    norm_gain,
    expert_gate,
    expert_up,
    expert_down,
    shared_gate,
    shared_up,
    shared_down,
    routes,
    route_scores,
):
    attended = attention(
        queries,
        fresh_token_key,
        value_new,
        forget_logit,
        cache_keys,
        cache_values,
        cache_cumlog,
        lengths,
    )
    mixed = jnp.dot(
        lax.all_gather(attended, "ep", axis=0, tiled=True),
        out_weight,
        preferred_element_type=jnp.float32,
    )
    stream = (residual.astype(jnp.float32) + mixed).astype(jnp.bfloat16)
    full_rows = lax.all_gather(stream, "ep", axis=1, tiled=True)
    rows_wide = full_rows.astype(jnp.float32)
    inv_rms = lax.rsqrt(jnp.mean(rows_wide * rows_wide, axis=1, keepdims=True) + norm_eps)
    normed = (rows_wide * inv_rms * norm_gain).astype(jnp.bfloat16)
    gate_weights = route_scores / jnp.sum(route_scores, axis=1, keepdims=True) * routed_scale
    shared_mid = expert_hidden(normed, shared_gate, shared_up)
    my_expert = lax.axis_index("ep")
    expert_hits = routes == my_expert
    is_member = jnp.sum(expert_hits.astype(jnp.int32), axis=1)
    slot_rank = jnp.cumsum(is_member) - 1
    slot_ids = lax.broadcasted_iota(jnp.int32, (CAP, 1), 0)
    selector = (is_member[None, :] == 1) & (slot_rank[None, :] == slot_ids)
    picked = jnp.dot(
        selector.astype(jnp.bfloat16), normed, preferred_element_type=jnp.float32
    ).astype(jnp.bfloat16)
    hidden = expert_hidden(picked, expert_gate[0], expert_up[0])
    expert_out = jnp.dot(hidden, expert_down[0], preferred_element_type=jnp.float32).astype(
        jnp.bfloat16
    )
    received = lax.all_to_all(expert_out[None], "ep", split_axis=2, concat_axis=0, tiled=True)
    expert_count = received.shape[0]
    expert_ids = lax.broadcasted_iota(jnp.int32, (1, 1, expert_count), 2)
    all_hits = routes[:, :, None] == expert_ids
    membership = jnp.sum(all_hits.astype(jnp.int32), axis=1)
    share_all = jnp.sum(jnp.where(all_hits, gate_weights[:, :, None], 0.0), axis=1)
    rank_all = jnp.cumsum(membership, axis=0) - 1
    slot_grid = lax.broadcasted_iota(jnp.int32, (1, 1, CAP), 2)
    slot_mask = (membership[:, :, None] == 1) & (rank_all[:, :, None] == slot_grid)
    combiner = jnp.where(slot_mask, share_all[:, :, None], 0.0).reshape(
        routes.shape[0], expert_count * CAP
    )
    flat_slots = received.reshape(expert_count * CAP, received.shape[2]).astype(jnp.float32)
    routed_part = jnp.dot(combiner, flat_slots, precision=lax.Precision.HIGHEST)
    shared_part = jnp.dot(
        lax.all_gather(shared_mid, "ep", axis=1, tiled=True),
        shared_down,
        preferred_element_type=jnp.float32,
    )
    return (stream.astype(jnp.float32) + routed_part + shared_part).astype(jnp.bfloat16)


VMEM = pltpu.VMEM
cuts = (0, 1, 4, 8)
ahead = 2
unit_step = 256


def in_vmem():
    return pl.BlockSpec(memory_space=VMEM)


def in_hbm():
    return pl.BlockSpec(memory_space=pltpu.HBM)


def held_in_hbm(*arrays):
    return [pltpu.with_memory_space_constraint(a, pltpu.HBM) for a in arrays]


def params(mib):
    return pltpu.CompilerParams(vmem_limit_bytes=mib * 1024 * 1024)


def attention_kernel(
    lengths_ref,
    queries_hbm,
    fresh_hbm,
    value_new_hbm,
    forget_hbm,
    keys_hbm,
    values_hbm,
    cumlog_hbm,
    *rest,
):
    extra = (len(rest) - 9) // 2
    side_hbm, (out_ref, *side_refs) = rest[:extra], rest[extra : 2 * extra + 1]
    queries_ref, fresh_ref, value_new_ref, forget_ref, keys, values, scores, sems = rest[
        2 * extra + 1 :
    ]
    heads, size = queries_ref.shape
    key_heads, span, _ = keys.shape
    groups = heads // key_heads
    inv_root = size ** (-0.5)
    first = 2 * len(cuts) - 2
    small_copies = [
        pltpu.make_async_copy(source, target, sems.at[first + i])
        for i, (source, target) in enumerate(
            (
                (cumlog_hbm.at[0], scores),
                (queries_hbm.at[0], queries_ref),
                (fresh_hbm.at[0], fresh_ref),
                (forget_hbm, forget_ref),
                (value_new_hbm.at[0], value_new_ref),
            )
        )
    ]

    def pieces(cuts):
        edges = [span * cut // cuts[-1] for cut in cuts]
        return list(zip(edges[:-1], edges[1:]))

    def copies(source, target, cuts, first):
        return [
            pltpu.make_async_copy(
                source.at[0, :, pl.ds(low, high - low), :],
                target.at[:, pl.ds(low, high - low), :],
                sems.at[first + i],
            )
            for i, (low, high) in enumerate(pieces(cuts))
        ]

    key_copies = copies(keys_hbm, keys, cuts, 0)
    value_copies = copies(values_hbm, values, cuts, len(cuts) - 1)
    side_copies = [
        pltpu.make_async_copy(source, target, sems.at[first + len(small_copies) + i])
        for i, (source, target) in enumerate(zip(side_hbm, side_refs))
    ]
    for copy in small_copies + key_copies + value_copies + side_copies:
        copy.start()

    def side_by_side(ref, low, high):
        return jnp.concatenate([ref[k, low:high, :] for k in range(key_heads)], axis=1)

    head_rows = lax.broadcasted_iota(jnp.int32, (heads, 1), 0)

    def per_head(ref):
        rows = ref[...].astype(jnp.float32)
        total = jnp.zeros((heads, size), jnp.float32)
        for k in range(key_heads):
            total = jnp.where(head_rows // groups == k, rows[k : k + 1, :], total)
        return total

    for copy in small_copies:
        copy.wait()
    length = lengths_ref[0]
    queries = queries_ref[...]
    wide = jnp.concatenate(
        [
            jnp.where(head_rows // groups == k, queries, jnp.zeros_like(queries))
            for k in range(key_heads)
        ],
        axis=1,
    )
    own_score = (
        jnp.sum(queries.astype(jnp.float32) * per_head(fresh_ref), axis=1, keepdims=True) * inv_root
    )
    logit_row = jnp.broadcast_to(forget_ref[...], (heads, heads))
    diagonal = lax.broadcasted_iota(jnp.int32, (heads, heads), 1) == head_rows
    logit = jnp.sum(jnp.where(diagonal, logit_row, 0.0), axis=1, keepdims=True)
    log_gate = jnp.minimum(logit, 0.0) - jnp.log1p(jnp.exp(-jnp.abs(logit)))
    positions = lax.broadcasted_iota(jnp.int32, (heads, span), 1)
    cumlog = scores[...]
    latest = jnp.sum(jnp.where(positions == length - 1, cumlog, 0.0), axis=1, keepdims=True)
    scores[...] = jnp.where(positions < length, latest + log_gate - cumlog, -jnp.inf)
    parts = pieces(cuts)

    def score(i):
        low, high = parts[i]
        raw = lax.dot_general(
            wide,
            side_by_side(keys, low, high),
            contract_last,
            preferred_element_type=jnp.float32,
        )
        return raw * inv_root + scores[:, low:high]

    def attend_to(weights, i):
        low, high = parts[i]
        return jnp.dot(weights, side_by_side(values, low, high), preferred_element_type=jnp.float32)

    count = len(parts)
    ready = [None] * count

    def fold(state, i):
        top, total, denominator = state
        new_top = jnp.maximum(top, jnp.max(ready[i], axis=1, keepdims=True))
        weights = jnp.exp(ready[i] - new_top)
        added = jnp.sum(weights, axis=1, keepdims=True)
        value_copies[i].wait()
        product = attend_to(weights.astype(jnp.bfloat16), i)
        if total is None:
            return new_top, product, added
        shrink = jnp.exp(top - new_top)
        return new_top, total * shrink + product, denominator * shrink + added

    state = own_score, None, None
    for i in range(count):
        key_copies[i].wait()
        ready[i] = score(i)
        if i >= ahead:
            state = fold(state, i - ahead)
    for i in range(max(count - ahead, 0), count):
        state = fold(state, i)
    top, total, denominator = state
    own_weight = jnp.exp(own_score - top)
    denominator = denominator + own_weight
    mine = own_weight.astype(jnp.bfloat16).astype(jnp.float32) * per_head(value_new_ref)
    for k in range(key_heads):
        mine = mine + jnp.where(
            head_rows // groups == k, total[:, k * size : (k + 1) * size], 0.0
        )
    out_ref[...] = (mine / denominator).astype(jnp.bfloat16)
    for copy in side_copies:
        copy.wait()


def spread_kernel(own_ref, out_ref):
    for peer in range(out_ref.shape[0]):
        out_ref[peer] = own_ref[...]


def attend(
    queries,
    fresh_token_key,
    value_new,
    forget_logit,
    cache_keys,
    cache_values,
    cache_cumlog,
    lengths,
    *side,
):
    peers = lax.axis_size("ep")
    _, heads, size = queries.shape
    _, key_heads, span, _ = cache_keys.shape
    bf16 = jnp.bfloat16
    own, *fetched = pl.pallas_call(
        attention_kernel,
        out_shape=[VMEM((heads, size), bf16)] + [VMEM(a.shape, a.dtype) for a in side],
        in_specs=[pl.BlockSpec(memory_space=pltpu.SMEM)] + [in_hbm()] * (7 + len(side)),
        out_specs=[in_vmem()] * (1 + len(side)),
        scratch_shapes=[
            VMEM((heads, size), bf16),
            VMEM((key_heads, size), bf16),
            VMEM((key_heads, size), bf16),
            VMEM((1, heads), jnp.float32),
            VMEM((key_heads, span, size), bf16),
            VMEM((key_heads, span, size), bf16),
            VMEM((heads, span), jnp.float32),
            pltpu.SemaphoreType.DMA((2 * len(cuts) + 3 + len(side),)),
        ],
        compiler_params=params(12),
        name="attention",
    )(
        lengths,
        *held_in_hbm(
            queries,
            fresh_token_key,
            value_new,
            forget_logit,
            cache_keys,
            cache_values,
            cache_cumlog,
            *side,
        ),
    )
    spread = pl.pallas_call(
        spread_kernel,
        out_shape=VMEM((peers, heads, size), bf16),
        in_specs=[in_vmem()],
        out_specs=in_vmem(),
        compiler_params=params(4),
        cost_estimate=pl.CostEstimate(
            flops=100000000000, bytes_accessed=0, transcendentals=0
        ),
        name="spread",
    )(own)
    return spread, fetched


def projection_kernel(rows_ref, weight_ref, residual_ref, out_ref):
    tokens, heads, size = rows_ref.shape
    stacked = rows_ref[...].reshape(tokens * heads, size)
    which = lax.broadcasted_iota(jnp.int32, (tokens * heads, 1), 0) % heads
    wide = jnp.concatenate(
        [jnp.where(which == h, stacked, jnp.zeros_like(stacked)) for h in range(heads)], axis=1
    )
    product = jnp.dot(wide, weight_ref[...], preferred_element_type=jnp.float32)
    mixed = jnp.sum(product.reshape(tokens, heads, product.shape[1]), axis=1)
    stream = (residual_ref[...].astype(jnp.float32) + mixed).astype(jnp.bfloat16)
    for peer in range(out_ref.shape[0]):
        out_ref[peer] = stream


def silu_product(gate, up):
    return gate / (1.0 + jnp.exp(-gate)) * up


def expert_kernel(
    blocks_ref,
    gain_ref,
    routes_ref,
    scores_ref,
    gate_ref,
    up_ref,
    down_ref,
    shared_gate_ref,
    shared_up_ref,
    out_ref,
):
    peers, tokens, width = blocks_ref.shape
    wide = [blocks_ref[p].astype(jnp.float32) for p in range(peers)]
    squares = wide[0] * wide[0]
    for block in wide[1:]:
        squares = squares + block * block
    mean = jnp.sum(squares, axis=1, keepdims=True) / (peers * width)
    inv_rms = lax.rsqrt(mean + norm_eps)
    normed = jnp.concatenate(
        [
            (wide[p] * inv_rms * gain_ref[p : p + 1, :]).astype(jnp.bfloat16)
            for p in range(peers)
        ],
        axis=1,
    )
    scores = scores_ref[...]
    shares = scores / jnp.sum(scores, axis=0, keepdims=True) * routed_scale
    share = jnp.sum(
        jnp.where(routes_ref[...] == lax.axis_index("ep"), shares, 0.0), axis=0, keepdims=True
    )

    def against(matrix):
        return lax.dot_general(matrix, normed, contract_last, preferred_element_type=jnp.float32)


    tokens_eye = (
        lax.broadcasted_iota(jnp.int32, (tokens, tokens), 0)
        == lax.broadcasted_iota(jnp.int32, (tokens, tokens), 1)
    )
    share = jnp.sum(
        jnp.where(tokens_eye, jnp.broadcast_to(share, (tokens, tokens)), 0.0),
        axis=1,
        keepdims=True,
    )

    def across(matrix):
        return lax.dot_general(normed, matrix, contract_last, preferred_element_type=jnp.float32)

    total = gate_ref.shape[0]
    edges = list(range(0, total, unit_step)) + [total]
    pairs = []
    for low, high in zip(edges[:-1], edges[1:]):
        pairs.append((against(gate_ref[low:high, :]), across(up_ref[low:high, :])))
    shared_g = against(shared_gate_ref[...]).T
    shared_u = across(shared_up_ref[...])

    hidden = jnp.concatenate([(silu_product(g.T, u) * share).astype(jnp.bfloat16) for g, u in pairs], axis=1)
    result = jnp.dot(hidden, down_ref[...], preferred_element_type=jnp.float32).astype(jnp.bfloat16)
    shared_hidden = silu_product(shared_g, shared_u).astype(jnp.bfloat16)
    units = shared_hidden.shape[1]
    shared_rows = jnp.concatenate(
        [shared_hidden, jnp.zeros((tokens, width - units), jnp.bfloat16)], axis=1
    )
    for p in range(peers):
        out_ref[p, :tokens, :] = result[:, p * width : (p + 1) * width]
        out_ref[p, tokens:, :] = shared_rows


def run_experts(blocks, fetched, expert_gate, expert_up, expert_down):
    peers, tokens, width = blocks.shape
    bf16 = jnp.bfloat16
    return pl.pallas_call(
        expert_kernel,
        out_shape=VMEM((peers, 2 * tokens, width), bf16),
        in_specs=[in_vmem()] * 9,
        out_specs=in_vmem(),
        compiler_params=params(16),
        name="experts",
    )(
        blocks,
        *(
            pltpu.with_memory_space_constraint(a, VMEM)
            for a in (
                *fetched[:3],
                expert_gate[0],
                expert_up[0],
                expert_down[0],
                *fetched[3:],
            )
        ),
    )


def combine_kernel(received_ref, stream_ref, down_ref, out_ref):
    peers, double, width = received_ref.shape
    tokens = double // 2
    units = down_ref.shape[0] // peers
    total = stream_ref[0].astype(jnp.float32)
    for p in range(peers):
        total = total + received_ref[p, :tokens, :].astype(jnp.float32)
    for p in range(peers):
        total = total + jnp.dot(
            received_ref[p, tokens:, :][:, :units],
            down_ref[p * units : (p + 1) * units, :],
            preferred_element_type=jnp.float32,
        )
    out_ref[...] = total.astype(jnp.bfloat16)


def combine(received, stream, shared_down):
    tokens, width = stream.shape[1:]
    bf16 = jnp.bfloat16
    return pl.pallas_call(
        combine_kernel,
        out_shape=jax.ShapeDtypeStruct((tokens, width), bf16),
        in_specs=[in_vmem()] * 3,
        out_specs=in_vmem(),
        compiler_params=params(4),
        name="combine",
    )(received, stream, shared_down)


def exchange(blocks):
    return lax.all_to_all(blocks, "ep", split_axis=0, concat_axis=0, tiled=True)


def kernel_device(
    queries,
    fresh_token_key,
    value_new,
    forget_logit,
    cache_keys,
    cache_values,
    cache_cumlog,
    lengths,
    residual,
    out_weight,
    norm_gain,
    expert_gate,
    expert_up,
    expert_down,
    shared_gate,
    shared_up,
    shared_down,
    routes,
    route_scores,
):
    peers = lax.axis_size("ep")
    _, heads, size = queries.shape
    _, key_heads, span, _ = cache_keys.shape
    tokens, width = residual.shape
    bf16 = jnp.bfloat16
    spread, fetched = attend(
        queries,
        fresh_token_key,
        value_new,
        forget_logit,
        cache_keys,
        cache_values,
        cache_cumlog,
        lengths,
        norm_gain.reshape(peers, width),
        routes.T,
        route_scores.T,
        shared_gate,
        shared_up,
    )
    rows = exchange(spread)
    stream = pl.pallas_call(
        projection_kernel,
        out_shape=VMEM((peers, tokens, width), bf16),
        in_specs=[in_vmem()] * 3,
        out_specs=in_vmem(),
        compiler_params=params(4),
        name="projection",
    )(rows, out_weight, residual)
    blocks = exchange(stream)
    outgoing = run_experts(blocks, fetched, expert_gate, expert_up, expert_down)
    received = exchange(outgoing)
    return combine(received, stream, shared_down)


def on_device(*arrays):
    residual, expert_gate, shared_gate = arrays[8], arrays[11], arrays[14]
    queries, cache_keys = arrays[0], arrays[4]
    fits = (
        residual.shape[1] % 128 == 0
        and residual.shape[0] % 16 == 0
        and shared_gate.shape[0] % 8 == 0
        and shared_gate.shape[0] <= residual.shape[1]
        and expert_gate.shape[0] == 1
        and queries.shape[0] == 1
        and cache_keys.shape[2] % 2048 == 0
    )
    return kernel_device(*arrays) if fits else plain_device(*arrays)


def solution(mesh):
    placed = (
        P(("grp", "ep"), None, None),
        P(("grp", "ep"), None, None),
        P(("grp", "ep"), None, None),
        P(("grp", "ep"), None),
        P(("grp", "ep"), None, None, None),
        P(("grp", "ep"), None, None, None),
        P(("grp", "ep"), None, None),
        P(("grp", "ep")),
        P("grp", "ep"),
        P(None, "ep"),
        P(),
        P("ep", None, None),
        P("ep", None, None),
        P("ep", None, None),
        P("ep", None),
        P("ep", None),
        P(None, "ep"),
        P("grp", None),
        P("grp", None),
    )
    return jax.shard_map(
        on_device, mesh=mesh, in_specs=placed, out_specs=P("grp", "ep"), check_vma=False
    )
```

```python
import jax
import jax.numpy as jnp
from jax import lax
from jax.experimental import pallas as pl
from jax.experimental.pallas import tpu as pltpu
from jax.sharding import PartitionSpec as P

CAP = 12


norm_eps = 1e-06
routed_scale = 2.5
contract_last = (((1,), (1,)), ((), ()))


def expert_hidden(row_block, gate_matrix, up_matrix):
    gate_part = lax.dot_general(
        row_block, gate_matrix, contract_last, preferred_element_type=jnp.float32
    )
    up_part = lax.dot_general(
        row_block, up_matrix, contract_last, preferred_element_type=jnp.float32
    )
    return (jax.nn.silu(gate_part) * up_part).astype(jnp.bfloat16)


def attention(
    queries,
    fresh_token_key,
    value_new,
    forget_logit,
    cache_keys,
    cache_values,
    cache_cumlog,
    lengths,
):
    batch_rows, head_count, head_size = queries.shape
    key_heads = cache_keys.shape[1]
    cache_span = cache_keys.shape[2]
    groups = head_count // key_heads
    inv_root = head_size ** (-0.5)
    grouped_heads = queries.reshape(batch_rows, key_heads, groups, head_size)
    scores = (
        jnp.einsum(
            "bkgd,bkpd->bkgp", grouped_heads, cache_keys, preferred_element_type=jnp.float32
        ).reshape(batch_rows, head_count, cache_span)
        * inv_root
    )
    positions = lax.broadcasted_iota(jnp.int32, (1, 1, cache_span), 2)
    last_pos = (lengths - 1)[:, None, None]
    latest = jnp.sum(jnp.where(positions == last_pos, cache_cumlog, 0.0), axis=2)
    log_gate = jax.nn.log_sigmoid(forget_logit)
    scores = scores + (latest + log_gate)[:, :, None] - cache_cumlog
    visible = positions < lengths[:, None, None]
    scores = jnp.where(visible, scores, -jnp.inf)
    own_score = (
        jnp.einsum(
            "tiuh,tih->tiu", grouped_heads, fresh_token_key, preferred_element_type=jnp.float32
        ).reshape(batch_rows, head_count)
        * inv_root
    )
    top_score = jnp.maximum(jnp.max(scores, axis=2), own_score)
    weights = jnp.where(visible, jnp.exp(scores - top_score[:, :, None]), 0.0)
    own_weight = jnp.exp(own_score - top_score)
    denominator = jnp.sum(weights, axis=2) + own_weight
    weighted = jnp.einsum(
        "bkgp,bkpd->bkgd",
        weights.astype(jnp.bfloat16).reshape(batch_rows, key_heads, groups, cache_span),
        cache_values,
        preferred_element_type=jnp.float32,
    )
    own_rounded = lax.optimization_barrier(own_weight.astype(jnp.bfloat16)).astype(jnp.float32)
    own_value = jnp.repeat(value_new, groups, axis=1).astype(jnp.float32)
    numerator = (
        weighted.reshape(batch_rows, head_count, head_size) + own_rounded[:, :, None] * own_value
    )
    return (
        (numerator / denominator[:, :, None])
        .astype(jnp.bfloat16)
        .reshape(batch_rows, head_count * head_size)
    )


def plain_device(
    queries,
    fresh_token_key,
    value_new,
    forget_logit,
    cache_keys,
    cache_values,
    cache_cumlog,
    lengths,
    residual,
    out_weight,
    norm_gain,
    expert_gate,
    expert_up,
    expert_down,
    shared_gate,
    shared_up,
    shared_down,
    routes,
    route_scores,
):
    attended = attention(
        queries,
        fresh_token_key,
        value_new,
        forget_logit,
        cache_keys,
        cache_values,
        cache_cumlog,
        lengths,
    )
    mixed = jnp.dot(
        lax.all_gather(attended, "ep", axis=0, tiled=True),
        out_weight,
        preferred_element_type=jnp.float32,
    )
    stream = (residual.astype(jnp.float32) + mixed).astype(jnp.bfloat16)
    full_rows = lax.all_gather(stream, "ep", axis=1, tiled=True)
    rows_wide = full_rows.astype(jnp.float32)
    inv_rms = lax.rsqrt(jnp.mean(rows_wide * rows_wide, axis=1, keepdims=True) + norm_eps)
    normed = (rows_wide * inv_rms * norm_gain).astype(jnp.bfloat16)
    gate_weights = route_scores / jnp.sum(route_scores, axis=1, keepdims=True) * routed_scale
    shared_mid = expert_hidden(normed, shared_gate, shared_up)
    my_expert = lax.axis_index("ep")
    expert_hits = routes == my_expert
    is_member = jnp.sum(expert_hits.astype(jnp.int32), axis=1)
    slot_rank = jnp.cumsum(is_member) - 1
    slot_ids = lax.broadcasted_iota(jnp.int32, (CAP, 1), 0)
    selector = (is_member[None, :] == 1) & (slot_rank[None, :] == slot_ids)
    picked = jnp.dot(
        selector.astype(jnp.bfloat16), normed, preferred_element_type=jnp.float32
    ).astype(jnp.bfloat16)
    hidden = expert_hidden(picked, expert_gate[0], expert_up[0])
    expert_out = jnp.dot(hidden, expert_down[0], preferred_element_type=jnp.float32).astype(
        jnp.bfloat16
    )
    received = lax.all_to_all(expert_out[None], "ep", split_axis=2, concat_axis=0, tiled=True)
    expert_count = received.shape[0]
    expert_ids = lax.broadcasted_iota(jnp.int32, (1, 1, expert_count), 2)
    all_hits = routes[:, :, None] == expert_ids
    membership = jnp.sum(all_hits.astype(jnp.int32), axis=1)
    share_all = jnp.sum(jnp.where(all_hits, gate_weights[:, :, None], 0.0), axis=1)
    rank_all = jnp.cumsum(membership, axis=0) - 1
    slot_grid = lax.broadcasted_iota(jnp.int32, (1, 1, CAP), 2)
    slot_mask = (membership[:, :, None] == 1) & (rank_all[:, :, None] == slot_grid)
    combiner = jnp.where(slot_mask, share_all[:, :, None], 0.0).reshape(
        routes.shape[0], expert_count * CAP
    )
    flat_slots = received.reshape(expert_count * CAP, received.shape[2]).astype(jnp.float32)
    routed_part = jnp.dot(combiner, flat_slots, precision=lax.Precision.HIGHEST)
    shared_part = jnp.dot(
        lax.all_gather(shared_mid, "ep", axis=1, tiled=True),
        shared_down,
        preferred_element_type=jnp.float32,
    )
    return (stream.astype(jnp.float32) + routed_part + shared_part).astype(jnp.bfloat16)


VMEM = pltpu.VMEM
cuts = (0, 1, 4, 8)
ahead = 2
unit_step = 256


def in_vmem():
    return pl.BlockSpec(memory_space=VMEM)


def in_hbm():
    return pl.BlockSpec(memory_space=pltpu.HBM)


def held_in_hbm(*arrays):
    return [pltpu.with_memory_space_constraint(a, pltpu.HBM) for a in arrays]


def params(mib):
    return pltpu.CompilerParams(vmem_limit_bytes=mib * 1024 * 1024)


def attention_kernel(
    lengths_ref,
    queries_hbm,
    fresh_hbm,
    value_new_hbm,
    forget_hbm,
    keys_hbm,
    values_hbm,
    cumlog_hbm,
    *rest,
):
    extra = (len(rest) - 9) // 2
    side_hbm, (out_ref, *side_refs) = rest[:extra], rest[extra : 2 * extra + 1]
    queries_ref, fresh_ref, value_new_ref, forget_ref, keys, values, scores, sems = rest[
        2 * extra + 1 :
    ]
    heads, size = queries_ref.shape
    key_heads, span, _ = keys.shape
    groups = heads // key_heads
    inv_root = size ** (-0.5)
    first = 2 * len(cuts) - 2
    small_copies = [
        pltpu.make_async_copy(source, target, sems.at[first + i])
        for i, (source, target) in enumerate(
            (
                (cumlog_hbm.at[0], scores),
                (queries_hbm.at[0], queries_ref),
                (fresh_hbm.at[0], fresh_ref),
                (forget_hbm, forget_ref),
                (value_new_hbm.at[0], value_new_ref),
            )
        )
    ]

    def pieces(cuts):
        edges = [span * cut // cuts[-1] for cut in cuts]
        return list(zip(edges[:-1], edges[1:]))

    def copies(source, target, cuts, first):
        return [
            pltpu.make_async_copy(
                source.at[0, :, pl.ds(low, high - low), :],
                target.at[:, pl.ds(low, high - low), :],
                sems.at[first + i],
            )
            for i, (low, high) in enumerate(pieces(cuts))
        ]

    key_copies = copies(keys_hbm, keys, cuts, 0)
    value_copies = copies(values_hbm, values, cuts, len(cuts) - 1)
    side_copies = [
        pltpu.make_async_copy(source, target, sems.at[first + len(small_copies) + i])
        for i, (source, target) in enumerate(zip(side_hbm, side_refs))
    ]
    for copy in small_copies + key_copies + value_copies + side_copies:
        copy.start()

    def side_by_side(ref, low, high):
        return jnp.concatenate([ref[k, low:high, :] for k in range(key_heads)], axis=1)

    head_rows = lax.broadcasted_iota(jnp.int32, (heads, 1), 0)

    def per_head(ref):
        rows = ref[...].astype(jnp.float32)
        total = jnp.zeros((heads, size), jnp.float32)
        for k in range(key_heads):
            total = jnp.where(head_rows // groups == k, rows[k : k + 1, :], total)
        return total

    for copy in small_copies:
        copy.wait()
    length = lengths_ref[0]
    queries = queries_ref[...]
    wide = jnp.concatenate(
        [
            jnp.where(head_rows // groups == k, queries, jnp.zeros_like(queries))
            for k in range(key_heads)
        ],
        axis=1,
    )
    own_score = (
        jnp.sum(queries.astype(jnp.float32) * per_head(fresh_ref), axis=1, keepdims=True) * inv_root
    )
    logit_row = jnp.broadcast_to(forget_ref[...], (heads, heads))
    diagonal = lax.broadcasted_iota(jnp.int32, (heads, heads), 1) == head_rows
    logit = jnp.sum(jnp.where(diagonal, logit_row, 0.0), axis=1, keepdims=True)
    log_gate = jnp.minimum(logit, 0.0) - jnp.log1p(jnp.exp(-jnp.abs(logit)))
    positions = lax.broadcasted_iota(jnp.int32, (heads, span), 1)
    cumlog = scores[...]
    latest = jnp.sum(jnp.where(positions == length - 1, cumlog, 0.0), axis=1, keepdims=True)
    scores[...] = jnp.where(positions < length, latest + log_gate - cumlog, -jnp.inf)
    parts = pieces(cuts)

    def score(i):
        low, high = parts[i]
        raw = lax.dot_general(
            wide,
            side_by_side(keys, low, high),
            contract_last,
            preferred_element_type=jnp.float32,
        )
        return raw * inv_root + scores[:, low:high]

    def attend_to(weights, i):
        low, high = parts[i]
        return jnp.dot(weights, side_by_side(values, low, high), preferred_element_type=jnp.float32)

    count = len(parts)
    ready = [None] * count

    def fold(state, i):
        top, total, denominator = state
        new_top = jnp.maximum(top, jnp.max(ready[i], axis=1, keepdims=True))
        weights = jnp.exp(ready[i] - new_top)
        added = jnp.sum(weights, axis=1, keepdims=True)
        value_copies[i].wait()
        product = attend_to(weights.astype(jnp.bfloat16), i)
        if total is None:
            return new_top, product, added
        shrink = jnp.exp(top - new_top)
        return new_top, total * shrink + product, denominator * shrink + added

    state = own_score, None, None
    for i in range(count):
        key_copies[i].wait()
        ready[i] = score(i)
        if i >= ahead:
            state = fold(state, i - ahead)
    for i in range(max(count - ahead, 0), count):
        state = fold(state, i)
    top, total, denominator = state
    own_weight = jnp.exp(own_score - top)
    denominator = denominator + own_weight
    mine = own_weight.astype(jnp.bfloat16).astype(jnp.float32) * per_head(value_new_ref)
    for k in range(key_heads):
        mine = mine + jnp.where(
            head_rows // groups == k, total[:, k * size : (k + 1) * size], 0.0
        )
    out_ref[...] = (mine / denominator).astype(jnp.bfloat16)
    for copy in side_copies:
        copy.wait()


def spread_kernel(own_ref, out_ref):
    for peer in range(out_ref.shape[0]):
        out_ref[peer] = own_ref[...]


def attend(
    queries,
    fresh_token_key,
    value_new,
    forget_logit,
    cache_keys,
    cache_values,
    cache_cumlog,
    lengths,
    *side,
):
    peers = lax.axis_size("ep")
    _, heads, size = queries.shape
    _, key_heads, span, _ = cache_keys.shape
    bf16 = jnp.bfloat16
    own, *fetched = pl.pallas_call(
        attention_kernel,
        out_shape=[VMEM((heads, size), bf16)] + [VMEM(a.shape, a.dtype) for a in side],
        in_specs=[pl.BlockSpec(memory_space=pltpu.SMEM)] + [in_hbm()] * (7 + len(side)),
        out_specs=[in_vmem()] * (1 + len(side)),
        scratch_shapes=[
            VMEM((heads, size), bf16),
            VMEM((key_heads, size), bf16),
            VMEM((key_heads, size), bf16),
            VMEM((1, heads), jnp.float32),
            VMEM((key_heads, span, size), bf16),
            VMEM((key_heads, span, size), bf16),
            VMEM((heads, span), jnp.float32),
            pltpu.SemaphoreType.DMA((2 * len(cuts) + 3 + len(side),)),
        ],
        compiler_params=params(12),
        name="attention",
    )(
        lengths,
        *held_in_hbm(
            queries,
            fresh_token_key,
            value_new,
            forget_logit,
            cache_keys,
            cache_values,
            cache_cumlog,
            *side,
        ),
    )
    spread = pl.pallas_call(
        spread_kernel,
        out_shape=VMEM((peers, heads, size), bf16),
        in_specs=[in_vmem()],
        out_specs=in_vmem(),
        compiler_params=params(4),
        cost_estimate=pl.CostEstimate(
            flops=100000000000, bytes_accessed=0, transcendentals=0
        ),
        name="spread",
    )(own)
    return spread, fetched


def projection_kernel(rows_ref, weight_ref, residual_ref, out_ref):
    tokens, heads, size = rows_ref.shape
    stacked = rows_ref[...].reshape(tokens * heads, size)
    which = lax.broadcasted_iota(jnp.int32, (tokens * heads, 1), 0) % heads
    wide = jnp.concatenate(
        [jnp.where(which == h, stacked, jnp.zeros_like(stacked)) for h in range(heads)], axis=1
    )
    product = jnp.dot(wide, weight_ref[...], preferred_element_type=jnp.float32)
    mixed = jnp.sum(product.reshape(tokens, heads, product.shape[1]), axis=1)
    stream = (residual_ref[...].astype(jnp.float32) + mixed).astype(jnp.bfloat16)
    for peer in range(out_ref.shape[0]):
        out_ref[peer] = stream


def silu_product(gate, up):
    return gate / (1.0 + jnp.exp(-gate)) * up


def expert_kernel(
    blocks_ref,
    gain_ref,
    routes_ref,
    scores_ref,
    gate_ref,
    up_ref,
    down_ref,
    shared_gate_ref,
    shared_up_ref,
    out_ref,
):
    peers, tokens, width = blocks_ref.shape
    wide = [blocks_ref[p].astype(jnp.float32) for p in range(peers)]
    squares = wide[0] * wide[0]
    for block in wide[1:]:
        squares = squares + block * block
    mean = jnp.sum(squares, axis=1, keepdims=True) / (peers * width)
    inv_rms = lax.rsqrt(mean + norm_eps)
    normed = jnp.concatenate(
        [
            (wide[p] * inv_rms * gain_ref[p : p + 1, :]).astype(jnp.bfloat16)
            for p in range(peers)
        ],
        axis=1,
    )
    scores = scores_ref[...]
    shares = scores / jnp.sum(scores, axis=0, keepdims=True) * routed_scale
    share = jnp.sum(
        jnp.where(routes_ref[...] == lax.axis_index("ep"), shares, 0.0), axis=0, keepdims=True
    )

    def against(matrix):
        return lax.dot_general(matrix, normed, contract_last, preferred_element_type=jnp.float32)


    tokens_eye = (
        lax.broadcasted_iota(jnp.int32, (tokens, tokens), 0)
        == lax.broadcasted_iota(jnp.int32, (tokens, tokens), 1)
    )
    share = jnp.sum(
        jnp.where(tokens_eye, jnp.broadcast_to(share, (tokens, tokens)), 0.0),
        axis=1,
        keepdims=True,
    )

    def across(matrix):
        return lax.dot_general(normed, matrix, contract_last, preferred_element_type=jnp.float32)

    total = gate_ref.shape[0]
    edges = list(range(0, total, unit_step)) + [total]
    pairs = []
    for low, high in zip(edges[:-1], edges[1:]):
        pairs.append((against(gate_ref[low:high, :]), across(up_ref[low:high, :])))
    shared_g = against(shared_gate_ref[...]).T
    shared_u = across(shared_up_ref[...])

    hidden = jnp.concatenate([(silu_product(g.T, u) * share).astype(jnp.bfloat16) for g, u in pairs], axis=1)
    result = jnp.dot(hidden, down_ref[...], preferred_element_type=jnp.float32).astype(jnp.bfloat16)
    shared_hidden = silu_product(shared_g, shared_u).astype(jnp.bfloat16)
    units = shared_hidden.shape[1]
    shared_rows = jnp.concatenate(
        [shared_hidden, jnp.zeros((tokens, width - units), jnp.bfloat16)], axis=1
    )
    for p in range(peers):
        out_ref[p, :tokens, :] = result[:, p * width : (p + 1) * width]
        out_ref[p, tokens:, :] = shared_rows


def run_experts(
    blocks, fetched, expert_gate, expert_up, expert_down, shared_gate, shared_up
):
    peers, tokens, width = blocks.shape
    bf16 = jnp.bfloat16
    return pl.pallas_call(
        expert_kernel,
        out_shape=VMEM((peers, 2 * tokens, width), bf16),
        in_specs=[in_vmem()] * 9,
        out_specs=in_vmem(),
        compiler_params=params(16),
        name="experts",
    )(
        blocks,
        *(
            pltpu.with_memory_space_constraint(a, VMEM)
            for a in (
                *fetched,
                expert_gate[0],
                expert_up[0],
                expert_down[0],
                shared_gate,
                shared_up,
            )
        ),
    )


def combine_kernel(received_ref, stream_ref, down_ref, out_ref):
    peers, double, width = received_ref.shape
    tokens = double // 2
    units = down_ref.shape[0] // peers
    total = stream_ref[0].astype(jnp.float32)
    for p in range(peers):
        total = total + received_ref[p, :tokens, :].astype(jnp.float32)
    for p in range(peers):
        total = total + jnp.dot(
            received_ref[p, tokens:, :][:, :units],
            down_ref[p * units : (p + 1) * units, :],
            preferred_element_type=jnp.float32,
        )
    out_ref[...] = total.astype(jnp.bfloat16)


def combine(received, stream, shared_down):
    tokens, width = stream.shape[1:]
    bf16 = jnp.bfloat16
    return pl.pallas_call(
        combine_kernel,
        out_shape=jax.ShapeDtypeStruct((tokens, width), bf16),
        in_specs=[in_vmem()] * 3,
        out_specs=in_vmem(),
        compiler_params=params(4),
        name="combine",
    )(received, stream, shared_down)


def exchange(blocks):
    return lax.all_to_all(blocks, "ep", split_axis=0, concat_axis=0, tiled=True)


def kernel_device(
    queries,
    fresh_token_key,
    value_new,
    forget_logit,
    cache_keys,
    cache_values,
    cache_cumlog,
    lengths,
    residual,
    out_weight,
    norm_gain,
    expert_gate,
    expert_up,
    expert_down,
    shared_gate,
    shared_up,
    shared_down,
    routes,
    route_scores,
):
    peers = lax.axis_size("ep")
    _, heads, size = queries.shape
    _, key_heads, span, _ = cache_keys.shape
    tokens, width = residual.shape
    bf16 = jnp.bfloat16
    spread, fetched = attend(
        queries,
        fresh_token_key,
        value_new,
        forget_logit,
        cache_keys,
        cache_values,
        cache_cumlog,
        lengths,
        norm_gain.reshape(peers, width),
        routes.T,
        route_scores.T,
    )
    rows = exchange(spread)
    stream = pl.pallas_call(
        projection_kernel,
        out_shape=VMEM((peers, tokens, width), bf16),
        in_specs=[in_vmem()] * 3,
        out_specs=in_vmem(),
        compiler_params=params(4),
        name="projection",
    )(rows, out_weight, residual)
    blocks = exchange(stream)
    outgoing = run_experts(
        blocks, fetched, expert_gate, expert_up, expert_down, shared_gate, shared_up
    )
    received = exchange(outgoing)
    return combine(received, stream, shared_down)


def on_device(*arrays):
    residual, expert_gate, shared_gate = arrays[8], arrays[11], arrays[14]
    queries, cache_keys = arrays[0], arrays[4]
    fits = (
        residual.shape[1] % 128 == 0
        and residual.shape[0] % 16 == 0
        and shared_gate.shape[0] % 8 == 0
        and shared_gate.shape[0] <= residual.shape[1]
        and expert_gate.shape[0] == 1
        and queries.shape[0] == 1
        and cache_keys.shape[2] % 2048 == 0
    )
    return kernel_device(*arrays) if fits else plain_device(*arrays)


def solution(mesh):
    placed = (
        P(("grp", "ep"), None, None),
        P(("grp", "ep"), None, None),
        P(("grp", "ep"), None, None),
        P(("grp", "ep"), None),
        P(("grp", "ep"), None, None, None),
        P(("grp", "ep"), None, None, None),
        P(("grp", "ep"), None, None),
        P(("grp", "ep")),
        P("grp", "ep"),
        P(None, "ep"),
        P(),
        P("ep", None, None),
        P("ep", None, None),
        P("ep", None, None),
        P("ep", None),
        P("ep", None),
        P(None, "ep"),
        P("grp", None),
        P("grp", None),
    )
    return jax.shard_map(
        on_device, mesh=mesh, in_specs=placed, out_specs=P("grp", "ep"), check_vma=False
    )
```
